512 devices in a mesh: sp: 32 (over z, x), dp: 16 (over y, core).
Axes of the slice: x: 4, y: 8, z: 8, core: 2. Of those that a mesh axis runs over, the one named last changes fastest.
Arguments:
- hidden_in: bfloat16 [16384, 2048], P('sp'), may hold values from -6 to 6
- content_weight: bfloat16 [2048, 2048], P('sp', 'dp'), may hold values from -0.125 to 0.125
- gating_weight: bfloat16 [2048, 2048], P('sp', 'dp'), may hold values from -2 to 2
- norm_gain: float32 [2048], P('dp'), may hold values from 0.1 to 1.9
- mixing_weight: bfloat16 [16, 128, 128], P('dp'), may hold values from -0.5 to 0.5
- mixing_bias: float32 [16, 128], P('dp'), may hold values from 0.1 to 1.9
- out_grad: bfloat16 [16384, 2048], P('sp', 'dp'), may hold values from -13 to 13
Outputs:
- input_grad: bfloat16 [16384, 2048], P('sp', 'dp')
- content_grad: float32 [2048, 2048], P('sp', 'dp')
- gating_grad: float32 [2048, 2048], P('sp', 'dp')
- mixing_grad: float32 [16, 128, 128], P('dp')
The draws below stay inside these ranges and needn't reach their ends.
All inputs are finite; a program needn't handle non-finite values.
Results may differ from the reference program's by a relative error of at most 0.019.
Values may be sent and summed in bfloat16 or wider, within the bound.
No kernel may reach another device: no remote copies, remote signals or barrier semaphores. Data moves between devices by JAX's collectives and lax.ppermute only.
A program may use at most 64 MiB of HBM per device.

```python
import math
import jax
import jax.numpy as jnp
from jax import lax

D = 2048
G = 16
GROUP_DIM = 128
BLOCK = 128
F = 2048
TOKENS = 16384
N_DP = 16


def column_scales(key):
    group_of = (jnp.arange(F) // GROUP_DIM).astype(jnp.float32)
    rising = group_of / (G - 1)
    jitter = jax.random.uniform(key, (F,), jnp.float32)
    exponent = 0.5 * rising + 0.5 * jitter
    return 10.0 ** (exponent - 0.5)


def draw_gating_weight(key, part):
    entries = jax.random.truncated_normal(jax.random.fold_in(key, 11), -4.0, 4.0, (D, F), jnp.float32)
    scales = column_scales(jax.random.fold_in(key, 12))
    return (entries * scales[None, :] * D ** (-0.5)).astype(jnp.bfloat16)


def draw_out_grad(key, part):
    entries = jax.random.truncated_normal(jax.random.fold_in(key, 21), -4.0, 4.0, (TOKENS, F), jnp.float32)
    scales = column_scales(jax.random.fold_in(key, 22))
    return (entries * scales[None, :]).astype(jnp.bfloat16)


def level_of(stream_key, extent, cuts, low, top_value):
    gain = 1.0
    for axis_at, blocks in cuts:
        draws = jax.random.uniform(jax.random.fold_in(jax.random.fold_in(stream_key, 6), axis_at), (blocks,), jnp.float32, low / len(cuts), top_value / len(cuts))
        gain = gain * jnp.repeat(jnp.exp(draws), extent[axis_at] // blocks).reshape((-1,) + (1,) * (len(extent) - 1 - axis_at))
    return gain


def bell_draw(own_key, extent, scale, limit, pieces=(), kind=jnp.bfloat16):
    result = jax.random.normal(own_key, extent, jnp.float32) * scale
    if len(pieces) > 0:
        result = level_of(own_key, extent, pieces, -0.22, 0.18) * result
    return jnp.clip(result, min=-limit, max=limit).astype(kind)


def setup_inputs(seed: int = 0) -> dict:
    seeds = jax.random.split(jax.random.key(seed), 8)
    hidden_in = bell_draw(seeds[0], (TOKENS, D), 1.0, 6.0, ((0, 32),))
    content_weight = bell_draw(seeds[1], (D, F), D ** -0.5, 0.125, ((0, 32), (1, 16)))
    gating_weight = draw_gating_weight(jax.random.fold_in(seeds[7], 71), 0)
    norm_gain = jnp.clip(1.0 + 0.18 * jax.random.normal(seeds[3], (F,), jnp.float32), 0.1, 1.9)
    mixing_weight = bell_draw(seeds[4], (G, BLOCK, BLOCK), BLOCK ** -0.5, 0.5, ((0, 16),))
    mixing_bias = jnp.clip(1.0 + 0.18 * jax.random.normal(seeds[5], (G, BLOCK), jnp.float32), 0.1, 1.9)
    out_grad = draw_out_grad(jax.random.fold_in(seeds[7], 71), 0)
    return dict(hidden_in=hidden_in, content_weight=content_weight, gating_weight=gating_weight, norm_gain=norm_gain, mixing_weight=mixing_weight, mixing_bias=mixing_bias, out_grad=out_grad)


norm_eps = 1e-05

def gelu_slope(values):
    cumulative = 0.5 * (1.0 + lax.erf(values * (1.0 / math.sqrt(2.0))))
    density = jnp.exp(-0.5 * values * values) * (1.0 / math.sqrt(2.0 * math.pi))
    return cumulative + values * density

def stored(values):
    return lax.optimization_barrier(values.astype(jnp.bfloat16))

def causal_table(weights):
    row_ids = lax.broadcasted_iota(jnp.int32, (BLOCK, BLOCK), 0)
    col_ids = lax.broadcasted_iota(jnp.int32, (BLOCK, BLOCK), 1)
    keeper = (col_ids <= row_ids)[None]
    return (jnp.where(keeper, weights, jnp.zeros_like(weights)), keeper)

def reference(hidden_in, content_weight, gating_weight, norm_gain, mixing_weight, mixing_bias, out_grad):
    tokens = hidden_in.shape[0]
    width = content_weight.shape[1]
    groups = width // GROUP_DIM
    blocks = tokens // BLOCK
    grad_scale = 1.0 / math.sqrt(tokens)
    pre_content = stored(jnp.dot(hidden_in, content_weight, preferred_element_type=jnp.float32)).astype(jnp.float32)
    pre_gating = stored(jnp.dot(hidden_in, gating_weight, preferred_element_type=jnp.float32)).astype(jnp.float32)
    content = jax.nn.gelu(pre_content, approximate=False)
    gating = jax.nn.gelu(pre_gating, approximate=False)
    row_mean = lax.optimization_barrier(jnp.mean(gating, axis=1, keepdims=True))
    row_var = lax.optimization_barrier(jnp.mean(gating * gating, axis=1, keepdims=True)) - row_mean * row_mean
    inv_std = lax.rsqrt(row_var + norm_eps)
    centred = (gating - row_mean) * inv_std
    normed = (centred * norm_gain[None, :]).astype(jnp.bfloat16)
    spatial, keeper = causal_table(mixing_weight)
    spatial_wide = spatial.astype(jnp.float32)
    normed_blocks = normed.astype(jnp.float32).reshape(blocks, BLOCK, groups, GROUP_DIM)
    mixed = jnp.einsum('gts,bsgc->btgc', spatial_wide, normed_blocks)
    mixed = mixed + jnp.transpose(mixing_bias)[None, :, :, None]
    mixed = mixed.reshape(tokens, width)
    grad_wide = out_grad.astype(jnp.float32)
    content_pre_grad = (grad_wide * mixed * gelu_slope(pre_content)).astype(jnp.bfloat16)
    mixed_grad = (grad_wide * content).astype(jnp.bfloat16)
    mixed_blocks = mixed_grad.astype(jnp.float32).reshape(blocks, BLOCK, groups, GROUP_DIM)
    mixing_grad = jnp.where(keeper, jnp.einsum('btgc,bsgc->gts', mixed_blocks, normed_blocks), 0.0) * grad_scale
    normed_grad = jnp.einsum('gts,btgc->bsgc', spatial_wide, mixed_blocks).reshape(tokens, width)
    centred_grad = normed_grad * norm_gain[None, :]
    first_moment = lax.optimization_barrier(jnp.mean(centred_grad, axis=1, keepdims=True))
    second_moment = lax.optimization_barrier(jnp.mean(centred_grad * centred, axis=1, keepdims=True))
    gating_back = inv_std * (centred_grad - first_moment - centred * second_moment)
    gating_pre_grad = (gating_back * gelu_slope(pre_gating)).astype(jnp.bfloat16)
    shard_cols = width // N_DP
    dims = (((1,), (1,)), ((), ()))

    def add_shard(running, shard_index):
        col_start = shard_index * shard_cols
        part_content = lax.dynamic_slice_in_dim(content_pre_grad, col_start, shard_cols, 1)
        part_gating = lax.dynamic_slice_in_dim(gating_pre_grad, col_start, shard_cols, 1)
        weight_content = lax.dynamic_slice_in_dim(content_weight, col_start, shard_cols, 1)
        weight_gating = lax.dynamic_slice_in_dim(gating_weight, col_start, shard_cols, 1)
        term = lax.dot_general(part_content, weight_content, dims, preferred_element_type=jnp.float32)
        term = term + lax.dot_general(part_gating, weight_gating, dims, preferred_element_type=jnp.float32)
        return (running + stored(term).astype(jnp.float32), None)
    input_sum, unused = lax.scan(add_shard, jnp.zeros((tokens, D), jnp.float32), jnp.arange(N_DP, dtype=jnp.int32))
    token_dims = (((0,), (0,)), ((), ()))
    content_grad = lax.dot_general(hidden_in, content_pre_grad, token_dims, preferred_element_type=jnp.float32) * grad_scale
    gating_grad = lax.dot_general(hidden_in, gating_pre_grad, token_dims, preferred_element_type=jnp.float32) * grad_scale
    return (input_sum.astype(jnp.bfloat16), content_grad, gating_grad, mixing_grad)
```

```python
import math

import jax
import jax.numpy as jnp
from jax import lax
from jax.sharding import Mesh
from jax.sharding import PartitionSpec as P

GROUP_DIM = 128
BLOCK = 128
SP = ("sp_0", "sp_1")
DP = ("dp_0", "dp_1")


norm_eps = 1e-05


def exchange(array, axis):
    return lax.all_to_all(array, axis, split_axis=0, concat_axis=0, tiled=True)


def sent_to_all(array, axis):
    return exchange(jnp.broadcast_to(array, (lax.axis_size(axis), *array.shape)), axis)


def shifted(array, axis, step):
    n = lax.axis_size(axis)
    return lax.ppermute(array, axis, [(i, (i + step) % n) for i in range(n)])


def gelu_slope(values):
    cumulative = 0.5 * (1.0 + lax.erf(values * (1.0 / math.sqrt(2.0))))
    density = jnp.exp(-0.5 * values * values) * (1.0 / math.sqrt(2.0 * math.pi))
    return cumulative + values * density


def causal_table(weights):
    row_ids = lax.broadcasted_iota(jnp.int32, (BLOCK, BLOCK), 0)
    col_ids = lax.broadcasted_iota(jnp.int32, (BLOCK, BLOCK), 1)
    keeper = (col_ids <= row_ids)[None]
    return (jnp.where(keeper, weights, jnp.zeros_like(weights)), keeper)


def local(
    hidden_in, content_weight, gating_weight, norm_gain, mixing_weight, mixing_bias, out_grad
):
    bf16, f32 = jnp.bfloat16, jnp.float32
    tok_rows, width = hidden_in.shape
    local_width = content_weight.shape[1]
    groups_here = local_width // GROUP_DIM
    blocks = tok_rows // BLOCK
    n_sp, n_dp = lax.axis_size(SP), lax.axis_size(DP)
    ring, cores = lax.axis_size("dp_0"), lax.axis_size("dp_1")
    full_width = local_width * n_dp
    out_cols = width // n_dp
    grad_scale = 1.0 / math.sqrt(tok_rows * n_sp)
    here, core = lax.axis_index("dp_0"), lax.axis_index("dp_1")

    shard = jnp.concatenate([content_weight, gating_weight], axis=1)
    weight = sent_to_all(shard, SP).reshape(width, 2 * local_width)

    by_owner = weight.reshape(ring, cores, out_cols, 2 * local_width)
    mine = lax.dynamic_index_in_dim(by_owner, core, axis=1, keepdims=False)
    theirs = lax.dynamic_index_in_dim(by_owner, 1 - core, axis=1, keepdims=False)
    pair_weight = jnp.concatenate([mine, shifted(theirs, "dp_1", 1)], axis=2)
    pair_weight = lax.dynamic_slice_in_dim(
        jnp.concatenate([pair_weight, pair_weight], axis=0), here, ring, axis=0
    )

    pre_both = jnp.dot(hidden_in, weight, preferred_element_type=f32).astype(bf16)
    pre_content = pre_both[:, :local_width].astype(f32)
    pre_gating = pre_both[:, local_width:].astype(f32)
    content = jax.nn.gelu(pre_content, approximate=False)
    gating = jax.nn.gelu(pre_gating, approximate=False)
    spatial, keeper = causal_table(mixing_weight)
    grad_wide = out_grad.astype(f32)
    mixed_grad = (grad_wide * content).astype(bf16)
    mixed_blocks = mixed_grad.reshape(blocks, BLOCK, groups_here, GROUP_DIM)
    normed_grad = jnp.einsum("gts,btgc->bsgc", spatial, mixed_blocks, preferred_element_type=f32)
    centred_grad = normed_grad.reshape(tok_rows, local_width) * norm_gain[None, :]
    sums = jnp.stack(
        [
            jnp.sum(gating, axis=1),
            jnp.sum(gating * gating, axis=1),
            jnp.sum(centred_grad, axis=1),
            jnp.sum(centred_grad * gating, axis=1),
        ]
    )
    sums = sent_to_all(sums.reshape(-1, 128), DP).sum(axis=0).reshape(4, tok_rows) / full_width
    row_mean = sums[0][:, None]
    row_var = sums[1][:, None] - row_mean * row_mean
    inv_std = lax.rsqrt(row_var + norm_eps)
    centred = (gating - row_mean) * inv_std
    first_moment = sums[2][:, None]
    second_moment = inv_std * (sums[3][:, None] - row_mean * first_moment)
    normed = (centred * norm_gain[None, :]).astype(bf16)
    normed_blocks = normed.reshape(blocks, BLOCK, groups_here, GROUP_DIM)
    mixed = jnp.einsum("gts,bsgc->btgc", spatial, normed_blocks, preferred_element_type=f32)
    mixed = (mixed + jnp.transpose(mixing_bias)[None, :, :, None]).reshape(tok_rows, local_width)
    content_pre_grad = (grad_wide * mixed * gelu_slope(pre_content)).astype(bf16)
    local_mixing = jnp.einsum(
        "btgc,bsgc->gts", mixed_blocks, normed_blocks, preferred_element_type=f32
    )
    local_mixing = jnp.where(keeper, local_mixing, 0.0).astype(bf16)
    gating_back = inv_std * (centred_grad - first_moment - centred * second_moment)
    gating_pre_grad = (gating_back * gelu_slope(pre_gating)).astype(bf16)
    joined_grad = jnp.concatenate([content_pre_grad, gating_pre_grad], axis=1)

    partner_grad = shifted(joined_grad, "dp_1", 1)

    weight_terms = lax.dot_general(
        hidden_in, joined_grad, (((0,), (0,)), ((), ())), preferred_element_type=f32
    ).astype(bf16)
    weight_terms = weight_terms.reshape(n_sp, width // n_sp, 2 * local_width)
    mixing_terms = local_mixing.reshape(1, -1, 2 * local_width)
    mixing_terms = jnp.broadcast_to(mixing_terms, (n_sp, *mixing_terms.shape[1:]))
    arrived = exchange(jnp.concatenate([weight_terms, mixing_terms], axis=1), SP)

    pair_grad = jnp.concatenate([joined_grad, partner_grad], axis=1)

    def part_for(step):
        return lax.dot_general(
            pair_grad, pair_weight[step], (((1,), (1,)), ((), ())), preferred_element_type=f32
        )

    parts = []
    for far in range(ring // 2, 0, -1):
        for step in sorted({far, ring - far}):
            parts.append(shifted(part_for(step).astype(bf16), "dp_0", step))
    total = part_for(0)
    for part in parts:
        total = total + part.astype(f32)
    input_grad = total.astype(bf16)

    arrived = arrived.astype(f32).sum(axis=0) * grad_scale
    rows = width // n_sp
    content_grad = arrived[:rows, :local_width]
    gating_grad = arrived[:rows, local_width:]
    mixing_grad = arrived[rows:].reshape(mixing_weight.shape)
    return (input_grad, content_grad, gating_grad, mixing_grad)


def solution(mesh):
    split = Mesh(mesh.devices.reshape(8, 4, 8, 2), (*SP, *DP))
    in_specs = (
        P(SP, None),
        P(SP, DP),
        P(SP, DP),
        P(DP),
        P(DP, None, None),
        P(DP, None),
        P(SP, DP),
    )
    out_specs = (P(SP, DP), P(SP, DP), P(SP, DP), P(DP, None, None))
    return jax.shard_map(local, mesh=split, in_specs=in_specs, out_specs=out_specs, check_vma=False)
```

```python
import functools
import math

import jax
import jax.numpy as jnp
from jax import lax
from jax.experimental import pallas as pl
from jax.experimental.pallas import tpu as pltpu
from jax.sharding import Mesh
from jax.sharding import PartitionSpec as P


BLOCK = 128
SP = ("sp_0", "sp_1")
DP = ("dp_0", "dp_1")


norm_eps = 1e-05
f32, bf16 = jnp.float32, jnp.bfloat16


def exchange(array, axis):
    return lax.all_to_all(array, axis, split_axis=0, concat_axis=0, tiled=True)


def swapped(array):
    return lax.ppermute(array, "dp_1", [(0, 1), (1, 0)])


def sent_apart(array, step):
    ring = lax.axis_size("dp_0")
    moves = []
    for y in range(ring):
        moves.append((2 * y, 2 * ((y + step) % ring)))
        moves.append((2 * y + 1, 2 * ((y - step) % ring) + 1))
    return lax.ppermute(array, DP, moves)


def normal_below(values):
    return 0.5 * (1.0 + lax.erf(values * (1.0 / math.sqrt(2.0))))


def gelu_slope(values):
    density = jnp.exp(-0.5 * values * values) * (1.0 / math.sqrt(2.0 * math.pi))
    return normal_below(values) + values * density


def causal(weights):
    rows = lax.broadcasted_iota(jnp.int32, (BLOCK, BLOCK), 0)
    cols = lax.broadcasted_iota(jnp.int32, (BLOCK, BLOCK), 1)
    return jnp.where(cols <= rows, weights, jnp.zeros_like(weights))


def nt(a, b, **kw):
    return lax.dot_general(a, b, (((1,), (1,)), ((), ())), preferred_element_type=f32, **kw)


def nn(a, b):
    return jnp.dot(a, b, preferred_element_type=f32)


def call(body, outs, scalars=False):
    def run(*args):
        inside = [pltpu.VMEM] * len(args)
        if scalars:
            inside[0] = pltpu.SMEM
        args = [
            a if m is pltpu.SMEM else pltpu.with_memory_space_constraint(a, m)
            for a, m in zip(args, inside)
        ]
        specs = [pl.BlockSpec(memory_space=m) for m in inside]
        limit = pltpu.CompilerParams(vmem_limit_bytes=20 * 1024 * 1024)
        made = pl.pallas_call(body, out_shape=outs, in_specs=specs, compiler_params=limit)
        return made(*args)

    return run


def like(shape, dtype):
    return pltpu.VMEM(shape, dtype)


def outside(shape, dtype):
    return jax.ShapeDtypeStruct(shape, dtype)


def project_body(hidden, weight, mixing, gain, grad, pre_out, gating_out, mixed_out, back_out, sums_out):
    n_x, n_z, rows, both = weight.shape
    slab = n_x * rows
    width = both // 2
    pre = None
    for z in range(n_z):
        term = nn(hidden[:, z * slab : (z + 1) * slab], weight[:, z].reshape(slab, both))
        pre = term if pre is None else pre + term
    pre = pre.astype(bf16)
    pre_out[...] = pre
    pre_content = pre[:, :width].astype(f32)
    pre_gating = pre[:, width:].astype(f32)
    gating = pre_gating * normal_below(pre_gating)
    gating_out[...] = gating
    mixed_grad = (grad[...].astype(f32) * (pre_content * normal_below(pre_content))).astype(bf16)
    mixed_out[...] = mixed_grad
    table = causal(mixing[0].astype(f32)).T.astype(bf16)
    pieces = []
    for at in range(0, mixed_grad.shape[0], BLOCK):
        pieces.append(nn(table, mixed_grad[at : at + BLOCK]) * gain[...])
    back = jnp.concatenate(pieces, axis=0)
    back_out[...] = back
    row = lax.broadcasted_iota(jnp.int32, (8, width), 0)
    sums = None
    for at, values in enumerate((gating, gating * gating, back, back * gating)):
        pick = jnp.where(row == at, 1.0, 0.0).astype(f32)
        term = nt(pick, values, precision=lax.Precision.HIGHEST)
        sums = term if sums is None else sums + term
    for peer in range(sums_out.shape[0]):
        sums_out[peer] = sums[:4]


def join_body(content, gating, out):
    both = jnp.concatenate([content[...], gating[...]], axis=1)
    for peer in range(out.shape[0]):
        out[peer] = both


def spread_body(arrived, out):
    for peer in range(out.shape[0]):
        out[peer] = arrived[...]


def flip_body(array, out):
    step = 256
    for at in range(0, array.shape[1], step):
        out[at : at + step] = array[:, at : at + step].T


def slopes_body(pre, grad, content_out, gating_out):
    width = grad.shape[1]
    content_out[...] = grad[...].astype(f32) * gelu_slope(pre[:, :width].astype(f32))
    gating_out[...] = gelu_slope(pre[:, width:].astype(f32))


def norm_body(full_width, sums, gating, mixed_grad, back, content_slope, gating_slope, mixing, bias, gain, joined_out, mixing_out):
    total = jnp.sum(sums[...], axis=0) * (1.0 / full_width)
    row_mean = total[0:1]
    row_var = total[1:2] - row_mean * row_mean
    inv_std = lax.rsqrt(row_var + norm_eps)
    first = total[2:3]
    second = inv_std * (total[3:4] - row_mean * first)
    columns = jnp.concatenate([row_mean, inv_std, first, second] * 2, axis=0).T
    row_mean, inv_std, first, second = [columns[:, i : i + 1] for i in range(4)]
    centred = (gating[...] - row_mean) * inv_std
    normed = (centred * gain[...]).astype(bf16)
    table = causal(mixing[0].astype(f32)).astype(bf16)
    shift = jnp.broadcast_to(bias[...], (8, BLOCK)).T[:, 0:1]
    width = normed.shape[1]
    mixing_grad = None
    for at in range(0, normed.shape[0], BLOCK):
        rows = slice(at, at + BLOCK)
        mixed = nn(table, normed[rows]) + shift
        joined_out[rows, :width] = (mixed * content_slope[rows]).astype(bf16)
        term = nt(mixed_grad[rows], normed[rows])
        mixing_grad = term if mixing_grad is None else mixing_grad + term
    gating_back = inv_std * (back[...] - first - centred * second)
    joined_out[:, width:] = (gating_back * gating_slope[...]).astype(bf16)
    mixing_grad = causal(mixing_grad).astype(bf16)
    half = BLOCK // 2
    mixing_out[...] = jnp.concatenate([mixing_grad[:half], mixing_grad[half:]], axis=1)


def weight_terms_body(hidden_t, joined, mixing_term, out):
    n_x, n_all, rows, _ = out.shape
    n_z = n_all - 1
    slab = n_x * rows
    for z in range(n_z):
        term = nn(hidden_t[z * slab : (z + 1) * slab], joined[...]).astype(bf16)
        for x in range(n_x):
            out[x, z] = term[x * rows : (x + 1) * rows]
    for x in range(n_x):
        out[x, n_z] = mixing_term[...]


def input_terms_body(where, joined, joined_far, weight, weight_far, one, two, three, four, own):
    n_x, _, rows, both = weight.shape

    def term(x_from, n, z):
        near = weight[pl.ds(x_from, n), pl.ds(z, 1)].reshape(n * rows, both)
        far = weight_far[pl.ds(x_from, n), pl.ds(z, 1)].reshape(n * rows, both)
        return nt(joined[...], near) + nt(joined_far[...], far)

    three[...] = term(0, n_x, where[3]).astype(bf16)
    two[...] = term(0, n_x, where[2]).astype(bf16)
    one[...] = term(0, n_x, where[1]).astype(bf16)
    half = n_x // 2
    four[...] = term(where[5] * half, half, where[4]).astype(bf16)
    own[...] = term(where[5] * half, half, where[0])


def regroup_body(arrived, out):
    n_z = out.shape[0]
    total = arrived[0].astype(f32)
    for x in range(1, arrived.shape[0]):
        total = total + arrived[x].astype(f32)
    total = total.astype(bf16)
    for z in range(n_z):
        out[z, 0] = total[z]
        out[z, 1] = total[n_z]


def finish_body(scale, arrived, content_out, gating_out, mixing_out):
    total = arrived[0].astype(f32)
    for z in range(1, arrived.shape[0]):
        total = total + arrived[z].astype(f32)
    total = total * scale
    half = content_out.shape[1]
    content_out[...] = total[0][:, :half]
    gating_out[...] = total[0][:, half:]
    mixing_out[0, : BLOCK // 2] = total[1][:, :half]
    mixing_out[0, BLOCK // 2 :] = total[1][:, half:]


def gather_body(where, one, two, three, four, own, keep_out, send_out):
    half = own.shape[1]
    total = one[...].astype(f32) + two[...].astype(f32) + three[...].astype(f32)
    first = where[5] == 0
    left, right = total[:, :half], total[:, half:]
    keep_out[...] = own[...] + four[...].astype(f32) + jnp.where(first, left, right)
    send_out[...] = jnp.where(first, right, left).astype(bf16)


def step(
    hidden_in, content_weight, gating_weight, norm_gain, mixing_weight, mixing_bias, out_grad
):
    tok_rows, width = hidden_in.shape
    shard_rows, local_width = content_weight.shape
    both = 2 * local_width
    n_z, n_x = lax.axis_size("sp_0"), lax.axis_size("sp_1")
    n_sp, n_dp = n_z * n_x, lax.axis_size(DP)
    ring = lax.axis_size("dp_0")
    full_width = local_width * n_dp
    out_cols = width // n_dp
    grad_scale = 1.0 / math.sqrt(tok_rows * n_sp)
    here, core = lax.axis_index("dp_0"), lax.axis_index("dp_1")
    side = 1 - 2 * core
    where = jnp.stack([(here + side * k + ring) % ring for k in range(5)] + [core]).astype(jnp.int32)
    gain = norm_gain[None, :]

    hidden_t = call(flip_body, like((width, tok_rows), bf16))(hidden_in)
    shards = call(join_body, like((n_z, shard_rows, both), bf16))(content_weight, gating_weight)
    along_z = exchange(shards, "sp_0")
    spread = call(spread_body, like((n_x, n_z, shard_rows, both), bf16))(along_z)
    weight = exchange(spread, "sp_1")
    weight_far = swapped(weight)

    tile, wide = (tok_rows, local_width), (tok_rows, both)
    pre, gating, mixed_grad, back, sums = call(
        project_body,
        (like(wide, bf16), like(tile, f32), like(tile, bf16), like(tile, f32), like((n_dp, 4, tok_rows), f32)),
    )(hidden_in, weight, mixing_weight, gain, out_grad)
    sums = exchange(sums, DP)
    content_slope, gating_slope = call(
        slopes_body, (like(tile, f32), like(tile, f32))
    )(pre, out_grad)
    joined, mixing_term = call(
        functools.partial(norm_body, full_width), (like(wide, bf16), like((BLOCK // 2, both), bf16))
    )(sums, gating, mixed_grad, back, content_slope, gating_slope, mixing_weight, mixing_bias, gain)

    joined_far = swapped(joined)
    terms = call(
        weight_terms_body, like((n_x, n_z + 1, shard_rows, both), bf16)
    )(hidden_t, joined, mixing_term)
    along_x = exchange(terms, "sp_1")

    pair, single = (tok_rows, 2 * out_cols), (tok_rows, out_cols)
    one, two, three, four, own = call(
        input_terms_body,
        (like(pair, bf16), like(pair, bf16), like(pair, bf16), like(single, bf16), like(single, f32)),
        scalars=True,
    )(where, joined, joined_far, weight, weight_far)
    three = sent_apart(three, 3)
    four = sent_apart(four, 4)
    two = sent_apart(two, 2)
    one = sent_apart(one, 1)

    regrouped = call(regroup_body, like((n_z, 2, shard_rows, both), bf16))(along_x)
    arrived = exchange(regrouped, "sp_0")

    keep, send = call(
        gather_body, (like(single, f32), like(single, bf16)), scalars=True
    )(where, one, two, three, four, own)
    input_grad = (keep + swapped(send).astype(f32)).astype(bf16)

    content_grad, gating_grad, mixing_grad = call(
        functools.partial(finish_body, grad_scale),
        (
            outside((shard_rows, local_width), f32),
            outside((shard_rows, local_width), f32),
            outside(mixing_weight.shape, f32),
        ),
    )(arrived)
    return (input_grad, content_grad, gating_grad, mixing_grad)


def solution(mesh):
    split = Mesh(mesh.devices.reshape(8, 4, 8, 2), (*SP, *DP))
    in_specs = (
        P(SP, None),
        P(SP, DP),
        P(SP, DP),
        P(DP),
        P(DP, None, None),
        P(DP, None),
        P(SP, DP),
    )
    out_specs = (P(SP, DP), P(SP, DP), P(SP, DP), P(DP, None, None))
    return jax.shard_map(step, mesh=split, in_specs=in_specs, out_specs=out_specs, check_vma=False)
```

```python
import functools
import math

import jax
import jax.numpy as jnp
from jax import lax
from jax.experimental import pallas as pl
from jax.experimental.pallas import tpu as pltpu
from jax.sharding import Mesh
from jax.sharding import PartitionSpec as P


BLOCK = 128
SP = ("sp_0", "sp_1")
DP = ("dp_0", "dp_1")


norm_eps = 1e-05
f32, bf16 = jnp.float32, jnp.bfloat16


def exchange(array, axis):
    return lax.all_to_all(array, axis, split_axis=0, concat_axis=0, tiled=True)


def swapped(array):
    return lax.ppermute(array, "dp_1", [(0, 1), (1, 0)])


def sent_apart(array, step):
    ring = lax.axis_size("dp_0")
    moves = []
    for y in range(ring):
        moves.append((2 * y, 2 * ((y + step) % ring)))
        moves.append((2 * y + 1, 2 * ((y - step) % ring) + 1))
    return lax.ppermute(array, DP, moves)


def normal_below(values):
    return 0.5 * (1.0 + lax.erf(values * (1.0 / math.sqrt(2.0))))


def gelu_slope(values):
    density = jnp.exp(-0.5 * values * values) * (1.0 / math.sqrt(2.0 * math.pi))
    return normal_below(values) + values * density


def causal(weights):
    rows = lax.broadcasted_iota(jnp.int32, (BLOCK, BLOCK), 0)
    cols = lax.broadcasted_iota(jnp.int32, (BLOCK, BLOCK), 1)
    return jnp.where(cols <= rows, weights, jnp.zeros_like(weights))


def nt(a, b, **kw):
    return lax.dot_general(a, b, (((1,), (1,)), ((), ())), preferred_element_type=f32, **kw)


def nn(a, b):
    return jnp.dot(a, b, preferred_element_type=f32)


def call(body, outs, scalars=False, cold=(), free=()):
    def run(*args):
        specs, operands = [], []
        for at, array in enumerate(args):
            if scalars and at == 0:
                specs.append(pl.BlockSpec(memory_space=pltpu.SMEM))
            elif at in free:
                specs.append(pl.BlockSpec())
            elif at in cold:
                specs.append(pl.BlockSpec())
                array = pltpu.with_memory_space_constraint(array, pltpu.HBM)
            else:
                specs.append(pl.BlockSpec(memory_space=pltpu.VMEM))
                array = pltpu.with_memory_space_constraint(array, pltpu.VMEM)
            operands.append(array)
        limit = pltpu.CompilerParams(vmem_limit_bytes=20 * 1024 * 1024)
        made = pl.pallas_call(body, out_shape=outs, in_specs=specs, compiler_params=limit)
        return made(*operands)

    return run


def like(shape, dtype):
    return pltpu.VMEM(shape, dtype)


def stored(shape, dtype):
    return pltpu.HBM(shape, dtype)


def outside(shape, dtype):
    return jax.ShapeDtypeStruct(shape, dtype)


def project_body(hidden, weight, mixing, gain, grad, pre_out, sums_out):
    n_x, n_z, rows, both = weight.shape
    slab = n_x * rows
    width = both // 2
    pre = None
    for z in range(n_z):
        term = nn(hidden[:, z * slab : (z + 1) * slab], weight[:, z].reshape(slab, both))
        pre = term if pre is None else pre + term
    pre = pre.astype(bf16)
    pre_out[...] = pre
    gating, _, back, _ = branches(pre, grad[...], mixing[0], gain[...])
    row = lax.broadcasted_iota(jnp.int32, (8, width), 0)
    sums = None
    for at, values in enumerate((gating, gating * gating, back, back * gating)):
        pick = jnp.where(row == at, 1.0, 0.0).astype(f32)
        term = nt(pick, values, precision=lax.Precision.HIGHEST)
        sums = term if sums is None else sums + term
    for peer in range(sums_out.shape[0]):
        sums_out[peer] = sums[:4]


def branches(pre, grad, mixing, gain):
    width = grad.shape[1]
    pre_content = pre[:, :width].astype(f32)
    pre_gating = pre[:, width:].astype(f32)
    gating = pre_gating * normal_below(pre_gating)
    content = pre_content * normal_below(pre_content)
    mixed_grad = (grad.astype(f32) * content).astype(bf16)
    table = causal(mixing.astype(f32)).T.astype(bf16)
    pieces = []
    for at in range(0, mixed_grad.shape[0], BLOCK):
        pieces.append(nn(table, mixed_grad[at : at + BLOCK]) * gain)
    return gating, mixed_grad, jnp.concatenate(pieces, axis=0), (pre_content, pre_gating)


def join_body(content, gating, out):
    both = jnp.concatenate([content[...], gating[...]], axis=1)
    for peer in range(out.shape[0]):
        out[peer] = both


def spread_body(arrived, out):
    for peer in range(out.shape[0]):
        out[peer] = arrived[...]


def flip_body(array, out):
    step = 256
    for at in range(0, array.shape[1], step):
        out[at : at + step] = array[:, at : at + step].T


def norm_body(full_width, sums, pre, grad, mixing, bias, gain, joined_out, mixing_out):
    gating, mixed_grad, back, (pre_content, pre_gating) = branches(
        pre[...], grad[...], mixing[0], gain[...]
    )
    content_slope = grad[...].astype(f32) * gelu_slope(pre_content)
    total = jnp.sum(sums[...], axis=0) * (1.0 / full_width)
    row_mean = total[0:1]
    row_var = total[1:2] - row_mean * row_mean
    inv_std = lax.rsqrt(row_var + norm_eps)
    first = total[2:3]
    second = inv_std * (total[3:4] - row_mean * first)
    columns = jnp.concatenate([row_mean, inv_std, first, second] * 2, axis=0).T
    row_mean, inv_std, first, second = [columns[:, i : i + 1] for i in range(4)]
    centred = (gating - row_mean) * inv_std
    normed = (centred * gain[...]).astype(bf16)
    table = causal(mixing[0].astype(f32)).astype(bf16)
    shift = jnp.broadcast_to(bias[...], (8, BLOCK)).T[:, 0:1]
    width = normed.shape[1]
    mixing_grad = None
    for at in range(0, normed.shape[0], BLOCK):
        rows = slice(at, at + BLOCK)
        mixed = nn(table, normed[rows]) + shift
        joined_out[rows, :width] = (mixed * content_slope[rows]).astype(bf16)
        term = nt(mixed_grad[rows], normed[rows])
        mixing_grad = term if mixing_grad is None else mixing_grad + term
    gating_back = inv_std * (back - first - centred * second)
    joined_out[:, width:] = (gating_back * gelu_slope(pre_gating)).astype(bf16)
    mixing_grad = causal(mixing_grad).astype(bf16)
    half = BLOCK // 2
    mixing_out[...] = jnp.concatenate([mixing_grad[:half], mixing_grad[half:]], axis=1)


def weight_terms_body(hidden_t, joined, mixing_term, out):
    n_x, n_all, rows, _ = out.shape
    n_z = n_all - 1
    slab = n_x * rows
    for z in range(n_z):
        term = nn(hidden_t[z * slab : (z + 1) * slab], joined[...]).astype(bf16)
        for x in range(n_x):
            out[x, z] = term[x * rows : (x + 1) * rows]
    for x in range(n_x):
        out[x, n_z] = mixing_term[...]


def term_for(joined, joined_far, weight, weight_far, x_from, n, z):
    _, _, rows, both = weight.shape
    near = weight[pl.ds(x_from, n), pl.ds(z, 1)].reshape(n * rows, both)
    far = weight_far[pl.ds(x_from, n), pl.ds(z, 1)].reshape(n * rows, both)
    return nt(joined[...], near) + nt(joined_far[...], far)


def far_terms_body(where, joined, joined_far, weight, weight_far, three, four):
    n_x = weight.shape[0]
    half = n_x // 2
    sources = (joined, joined_far, weight, weight_far)
    four[...] = term_for(*sources, where[5] * half, half, where[4]).astype(bf16)
    three[...] = term_for(*sources, 0, n_x, where[3]).astype(bf16)


def near_terms_body(where, joined, joined_far, weight, weight_far, one, two, own):
    n_x = weight.shape[0]
    half = n_x // 2
    sources = (joined, joined_far, weight, weight_far)
    one[...] = term_for(*sources, 0, n_x, where[1]).astype(bf16)
    two[...] = term_for(*sources, 0, n_x, where[2])
    own[...] = term_for(*sources, where[5] * half, half, where[0])


def merge_body(where, two, three, four, out):
    half = four.shape[1]
    first = where[5] == 0
    extra = four[...].astype(f32)
    none = jnp.zeros_like(extra)
    left = two[:, :half] + three[:, :half].astype(f32) + jnp.where(first, extra, none)
    right = two[:, half:] + three[:, half:].astype(f32) + jnp.where(first, none, extra)
    out[:, :half] = left.astype(bf16)
    out[:, half:] = right.astype(bf16)


def regroup_body(arrived, out):
    n_z = out.shape[0]
    total = arrived[0].astype(f32)
    for x in range(1, arrived.shape[0]):
        total = total + arrived[x].astype(f32)
    total = total.astype(bf16)
    for z in range(n_z):
        out[z, 0] = total[z]
        out[z, 1] = total[n_z]


def finish_body(scale, arrived, content_out, gating_out, mixing_out):
    total = arrived[0].astype(f32)
    for z in range(1, arrived.shape[0]):
        total = total + arrived[z].astype(f32)
    total = total * scale
    half = content_out.shape[1]
    content_out[...] = total[0][:, :half]
    gating_out[...] = total[0][:, half:]
    mixing_out[0, : BLOCK // 2] = total[1][:, :half]
    mixing_out[0, BLOCK // 2 :] = total[1][:, half:]


def gather_body(where, one, two, own, keep_out, send_out):
    half = own.shape[1]
    total = one[...].astype(f32) + two[...].astype(f32)
    first = where[5] == 0
    left, right = total[:, :half], total[:, half:]
    keep_out[...] = own[...] + jnp.where(first, left, right)
    send_out[...] = jnp.where(first, right, left).astype(bf16)


def step(
    hidden_in, content_weight, gating_weight, norm_gain, mixing_weight, mixing_bias, out_grad
):
    tok_rows, width = hidden_in.shape
    shard_rows, local_width = content_weight.shape
    both = 2 * local_width
    n_z, n_x = lax.axis_size("sp_0"), lax.axis_size("sp_1")
    n_sp, n_dp = n_z * n_x, lax.axis_size(DP)
    ring = lax.axis_size("dp_0")
    full_width = local_width * n_dp
    out_cols = width // n_dp
    grad_scale = 1.0 / math.sqrt(tok_rows * n_sp)
    here, core = lax.axis_index("dp_0"), lax.axis_index("dp_1")
    side = 1 - 2 * core
    where = jnp.stack([(here + side * k + ring) % ring for k in range(5)] + [core]).astype(jnp.int32)
    gain = norm_gain[None, :]

    hidden_t = call(flip_body, like((width, tok_rows), bf16))(hidden_in)
    shards = call(join_body, stored((n_z, shard_rows, both), bf16), cold=(0, 1))(
        content_weight, gating_weight
    )
    along_z = exchange(shards, "sp_0")
    spread = call(spread_body, like((n_x, n_z, shard_rows, both), bf16))(along_z)
    weight = exchange(spread, "sp_1")
    weight_far = swapped(weight)

    wide = (tok_rows, both)
    pre, sums = call(
        project_body, (stored(wide, bf16), stored((n_dp, 4, tok_rows), f32)), cold=(2,)
    )(hidden_in, weight, mixing_weight, gain, out_grad)
    sums = exchange(sums, DP)
    joined, mixing_term = call(
        functools.partial(norm_body, full_width),
        (like(wide, bf16), like((BLOCK // 2, both), bf16)),
        cold=(0, 1, 3, 4, 5),
    )(sums, pre, out_grad, mixing_weight, mixing_bias, gain)

    joined_far = swapped(joined)
    terms = call(
        weight_terms_body, stored((n_x, n_z + 1, shard_rows, both), bf16)
    )(hidden_t, joined, mixing_term)
    along_x = exchange(terms, "sp_1")

    pair, single = (tok_rows, 2 * out_cols), (tok_rows, out_cols)
    sources = (where, joined, joined_far, weight, weight_far)
    three, four = call(
        far_terms_body, (like(pair, bf16), like(single, bf16)), scalars=True
    )(*sources)
    four = sent_apart(four, 2)
    three = sent_apart(three, 1)
    one, two, own = call(
        near_terms_body, (like(pair, bf16), like(pair, f32), like(single, f32)), scalars=True
    )(*sources)
    one = sent_apart(one, 1)
    two = call(merge_body, like(pair, bf16), scalars=True)(where, two, three, four)
    two = sent_apart(two, 2)

    regrouped = call(regroup_body, stored((n_z, 2, shard_rows, both), bf16))(along_x)
    arrived = exchange(regrouped, "sp_0")

    keep, send = call(
        gather_body, (like(single, f32), like(single, bf16)), scalars=True
    )(where, one, two, own)
    input_grad = (keep + swapped(send).astype(f32)).astype(bf16)

    content_grad, gating_grad, mixing_grad = call(
        functools.partial(finish_body, grad_scale),
        (
            outside((shard_rows, local_width), f32),
            outside((shard_rows, local_width), f32),
            outside(mixing_weight.shape, f32),
        ),
    )(arrived)
    return (input_grad, content_grad, gating_grad, mixing_grad)


def solution(mesh):
    split = Mesh(mesh.devices.reshape(8, 4, 8, 2), (*SP, *DP))
    in_specs = (
        P(SP, None),
        P(SP, DP),
        P(SP, DP),
        P(DP),
        P(DP, None, None),
        P(DP, None),
        P(SP, DP),
    )
    out_specs = (P(SP, DP), P(SP, DP), P(SP, DP), P(DP, None, None))
    return jax.shard_map(step, mesh=split, in_specs=in_specs, out_specs=out_specs, check_vma=False)
```

```python
import functools
import math

import jax
import jax.numpy as jnp
from jax import lax
from jax.experimental import pallas as pl
from jax.experimental.pallas import tpu as pltpu
from jax.sharding import Mesh
from jax.sharding import PartitionSpec as P


BLOCK = 128
SP = ("sp_0", "sp_1")
DP = ("dp_0", "dp_1")


norm_eps = 1e-05
f32, bf16 = jnp.float32, jnp.bfloat16


def exchange(array, axis):
    return lax.all_to_all(array, axis, split_axis=0, concat_axis=0, tiled=True)


def swapped(array):
    return lax.ppermute(array, "dp_1", [(0, 1), (1, 0)])


def sent_apart(array, step):
    ring = lax.axis_size("dp_0")
    moves = []
    for y in range(ring):
        moves.append((2 * y, 2 * ((y + step) % ring)))
        moves.append((2 * y + 1, 2 * ((y - step) % ring) + 1))
    return lax.ppermute(array, DP, moves)


def normal_below(values):
    return 0.5 * (1.0 + lax.erf(values * (1.0 / math.sqrt(2.0))))


def gelu_slope(values):
    density = jnp.exp(-0.5 * values * values) * (1.0 / math.sqrt(2.0 * math.pi))
    return normal_below(values) + values * density


def causal(weights):
    rows = lax.broadcasted_iota(jnp.int32, (BLOCK, BLOCK), 0)
    cols = lax.broadcasted_iota(jnp.int32, (BLOCK, BLOCK), 1)
    return jnp.where(cols <= rows, weights, jnp.zeros_like(weights))


def nt(a, b, **kw):
    return lax.dot_general(a, b, (((1,), (1,)), ((), ())), preferred_element_type=f32, **kw)


def nn(a, b):
    return jnp.dot(a, b, preferred_element_type=f32)


def call(body, outs, scalars=False, cold=(), free=()):
    def run(*args):
        specs, operands = [], []
        for at, array in enumerate(args):
            if scalars and at == 0:
                specs.append(pl.BlockSpec(memory_space=pltpu.SMEM))
            elif at in free:
                specs.append(pl.BlockSpec())
            elif at in cold:
                specs.append(pl.BlockSpec())
                array = pltpu.with_memory_space_constraint(array, pltpu.HBM)
            else:
                specs.append(pl.BlockSpec(memory_space=pltpu.VMEM))
                array = pltpu.with_memory_space_constraint(array, pltpu.VMEM)
            operands.append(array)
        limit = pltpu.CompilerParams(vmem_limit_bytes=20 * 1024 * 1024)
        made = pl.pallas_call(body, out_shape=outs, in_specs=specs, compiler_params=limit)
        return made(*operands)

    return run


def like(shape, dtype):
    return pltpu.VMEM(shape, dtype)


def stored(shape, dtype):
    return pltpu.HBM(shape, dtype)


def outside(shape, dtype):
    return jax.ShapeDtypeStruct(shape, dtype)


def project_body(hidden, weight, mixing, gain, grad, pre_out, sums_out):
    n_x, n_z, rows, both = weight.shape
    slab = n_x * rows
    width = both // 2
    pre = None
    for z in range(n_z):
        term = nn(hidden[:, z * slab : (z + 1) * slab], weight[:, z].reshape(slab, both))
        pre = term if pre is None else pre + term
    pre = pre.astype(bf16)
    pre_out[...] = pre
    gating, _, back, _ = branches(pre, grad[...], mixing[0], gain[...])
    row = lax.broadcasted_iota(jnp.int32, (8, width), 0)
    sums = None
    for at, values in enumerate((gating, gating * gating, back, back * gating)):
        pick = jnp.where(row == at, 1.0, 0.0).astype(f32)
        term = nt(pick, values, precision=lax.Precision.HIGHEST)
        sums = term if sums is None else sums + term
    for peer in range(sums_out.shape[0]):
        sums_out[peer] = sums[:4]


def branches(pre, grad, mixing, gain):
    width = grad.shape[1]
    pre_content = pre[:, :width].astype(f32)
    pre_gating = pre[:, width:].astype(f32)
    gating = pre_gating * normal_below(pre_gating)
    content = pre_content * normal_below(pre_content)
    mixed_grad = (grad.astype(f32) * content).astype(bf16)
    table = causal(mixing.astype(f32)).T.astype(bf16)
    pieces = []
    for at in range(0, mixed_grad.shape[0], BLOCK):
        pieces.append(nn(table, mixed_grad[at : at + BLOCK]) * gain)
    return gating, mixed_grad, jnp.concatenate(pieces, axis=0), (pre_content, pre_gating)


def join_body(content, gating, out):
    both = jnp.concatenate([content[...], gating[...]], axis=1)
    for peer in range(out.shape[0]):
        out[peer] = both


def spread_body(arrived, out):
    for peer in range(out.shape[0]):
        out[peer] = arrived[...]


def flip_body(array, out):
    step = 256
    for at in range(0, array.shape[1], step):
        out[at : at + step] = array[:, at : at + step].T


def norm_body(full_width, sums, pre, grad, mixing, bias, gain, joined_out, mixing_out):
    gating, mixed_grad, back, (pre_content, pre_gating) = branches(
        pre[...], grad[...], mixing[0], gain[...]
    )
    content_slope = grad[...].astype(f32) * gelu_slope(pre_content)
    total = jnp.sum(sums[...], axis=0) * (1.0 / full_width)
    row_mean = total[0:1]
    row_var = total[1:2] - row_mean * row_mean
    inv_std = lax.rsqrt(row_var + norm_eps)
    first = total[2:3]
    second = inv_std * (total[3:4] - row_mean * first)
    columns = jnp.concatenate([row_mean, inv_std, first, second] * 2, axis=0).T
    row_mean, inv_std, first, second = [columns[:, i : i + 1] for i in range(4)]
    centred = (gating - row_mean) * inv_std
    normed = (centred * gain[...]).astype(bf16)
    table = causal(mixing[0].astype(f32)).astype(bf16)
    shift = jnp.broadcast_to(bias[...], (8, BLOCK)).T[:, 0:1]
    width = normed.shape[1]
    mixing_grad = None
    for at in range(0, normed.shape[0], BLOCK):
        rows = slice(at, at + BLOCK)
        mixed = nn(table, normed[rows]) + shift
        joined_out[rows, :width] = (mixed * content_slope[rows]).astype(bf16)
        term = nt(mixed_grad[rows], normed[rows])
        mixing_grad = term if mixing_grad is None else mixing_grad + term
    gating_back = inv_std * (back - first - centred * second)
    joined_out[:, width:] = (gating_back * gelu_slope(pre_gating)).astype(bf16)
    mixing_grad = causal(mixing_grad).astype(bf16)
    half = BLOCK // 2
    mixing_out[...] = jnp.concatenate([mixing_grad[:half], mixing_grad[half:]], axis=1)


def weight_terms_body(hidden_t, joined, mixing_term, out):
    n_x, n_all, rows, _ = out.shape
    n_z = n_all - 1
    slab = n_x * rows
    for z in range(n_z):
        term = nn(hidden_t[z * slab : (z + 1) * slab], joined[...]).astype(bf16)
        for x in range(n_x):
            out[x, z] = term[x * rows : (x + 1) * rows]
    for x in range(n_x):
        out[x, n_z] = mixing_term[...]


def term_for(joined, joined_far, weight, weight_far, x_from, n, z):
    _, _, rows, both = weight.shape
    near = weight[pl.ds(x_from, n), pl.ds(z, 1)].reshape(n * rows, both)
    far = weight_far[pl.ds(x_from, n), pl.ds(z, 1)].reshape(n * rows, both)
    return nt(joined[...], near) + nt(joined_far[...], far)


def input_terms_body(where, joined, joined_far, weight, weight_far, four, odd, two, own):
    n_x = weight.shape[0]
    half = n_x // 2
    width = two.shape[1]
    sources = (joined, joined_far, weight, weight_far)
    four[...] = term_for(*sources, where[5] * half, half, where[4]).astype(bf16)
    odd[:, :width] = term_for(*sources, 0, n_x, where[3]).astype(bf16)
    odd[:, width:] = term_for(*sources, 0, n_x, where[1]).astype(bf16)
    two[...] = term_for(*sources, 0, n_x, where[2])
    own[...] = term_for(*sources, where[5] * half, half, where[0])


def merge_body(where, two, odd, four, out):
    half = four.shape[1]
    first = where[5] == 0
    extra = four[...].astype(f32)
    none = jnp.zeros_like(extra)
    left = two[:, :half] + odd[:, :half].astype(f32) + jnp.where(first, extra, none)
    right = two[:, half:] + odd[:, half : 2 * half].astype(f32) + jnp.where(first, none, extra)
    out[:, :half] = left.astype(bf16)
    out[:, half:] = right.astype(bf16)


def regroup_body(arrived, out):
    n_z = out.shape[0]
    total = arrived[0].astype(f32)
    for x in range(1, arrived.shape[0]):
        total = total + arrived[x].astype(f32)
    total = total.astype(bf16)
    for z in range(n_z):
        out[z, 0] = total[z]
        out[z, 1] = total[n_z]


def finish_body(scale, arrived, content_out, gating_out, mixing_out):
    total = arrived[0].astype(f32)
    for z in range(1, arrived.shape[0]):
        total = total + arrived[z].astype(f32)
    total = total * scale
    half = content_out.shape[1]
    content_out[...] = total[0][:, :half]
    gating_out[...] = total[0][:, half:]
    mixing_out[0, : BLOCK // 2] = total[1][:, :half]
    mixing_out[0, BLOCK // 2 :] = total[1][:, half:]


def gather_body(where, odd, two, own, keep_out, send_out):
    half = own.shape[1]
    total = odd[:, 2 * half :].astype(f32) + two[...].astype(f32)
    first = where[5] == 0
    left, right = total[:, :half], total[:, half:]
    keep_out[...] = own[...] + jnp.where(first, left, right)
    send_out[...] = jnp.where(first, right, left).astype(bf16)


def step(
    hidden_in, content_weight, gating_weight, norm_gain, mixing_weight, mixing_bias, out_grad
):
    tok_rows, width = hidden_in.shape
    shard_rows, local_width = content_weight.shape
    both = 2 * local_width
    n_z, n_x = lax.axis_size("sp_0"), lax.axis_size("sp_1")
    n_sp, n_dp = n_z * n_x, lax.axis_size(DP)
    ring = lax.axis_size("dp_0")
    full_width = local_width * n_dp
    out_cols = width // n_dp
    grad_scale = 1.0 / math.sqrt(tok_rows * n_sp)
    here, core = lax.axis_index("dp_0"), lax.axis_index("dp_1")
    side = 1 - 2 * core
    where = jnp.stack([(here + side * k + ring) % ring for k in range(5)] + [core]).astype(jnp.int32)
    gain = norm_gain[None, :]

    hidden_t = call(flip_body, like((width, tok_rows), bf16))(hidden_in)
    shards = call(join_body, stored((n_z, shard_rows, both), bf16), cold=(0, 1))(
        content_weight, gating_weight
    )
    along_z = exchange(shards, "sp_0")
    spread = call(spread_body, like((n_x, n_z, shard_rows, both), bf16))(along_z)
    weight = exchange(spread, "sp_1")
    weight_far = swapped(weight)

    wide = (tok_rows, both)
    pre, sums = call(
        project_body, (stored(wide, bf16), stored((n_dp, 4, tok_rows), f32)), cold=(2,)
    )(hidden_in, weight, mixing_weight, gain, out_grad)
    sums = exchange(sums, DP)
    joined, mixing_term = call(
        functools.partial(norm_body, full_width),
        (like(wide, bf16), like((BLOCK // 2, both), bf16)),
        cold=(0, 1, 3, 4, 5),
    )(sums, pre, out_grad, mixing_weight, mixing_bias, gain)

    joined_far = swapped(joined)
    terms = call(
        weight_terms_body, stored((n_x, n_z + 1, shard_rows, both), bf16)
    )(hidden_t, joined, mixing_term)
    along_x = exchange(terms, "sp_1")

    single, pair = (tok_rows, out_cols), (tok_rows, 2 * out_cols)
    wide_pair = (tok_rows, 4 * out_cols)
    sources = (where, joined, joined_far, weight, weight_far)
    four, odd, two, own = call(
        input_terms_body,
        (like(single, bf16), like(wide_pair, bf16), like(pair, f32), like(single, f32)),
        scalars=True,
    )(*sources)
    four = sent_apart(four, 2)
    odd = sent_apart(odd, 1)
    two = call(merge_body, like(pair, bf16), scalars=True)(where, two, odd, four)
    two = sent_apart(two, 2)

    regrouped = call(regroup_body, stored((n_z, 2, shard_rows, both), bf16))(along_x)
    arrived = exchange(regrouped, "sp_0")

    keep, send = call(
        gather_body, (like(single, f32), like(single, bf16)), scalars=True
    )(where, odd, two, own)
    input_grad = (keep + swapped(send).astype(f32)).astype(bf16)

    content_grad, gating_grad, mixing_grad = call(
        functools.partial(finish_body, grad_scale),
        (
            outside((shard_rows, local_width), f32),
            outside((shard_rows, local_width), f32),
            outside(mixing_weight.shape, f32),
        ),
    )(arrived)
    return (input_grad, content_grad, gating_grad, mixing_grad)


def solution(mesh):
    split = Mesh(mesh.devices.reshape(8, 4, 8, 2), (*SP, *DP))
    in_specs = (
        P(SP, None),
        P(SP, DP),
        P(SP, DP),
        P(DP),
        P(DP, None, None),
        P(DP, None),
        P(SP, DP),
    )
    out_specs = (P(SP, DP), P(SP, DP), P(SP, DP), P(DP, None, None))
    return jax.shard_map(step, mesh=split, in_specs=in_specs, out_specs=out_specs, check_vma=False)
```

```python
import functools
import math

import jax
import jax.numpy as jnp
from jax import lax
from jax.experimental import pallas as pl
from jax.experimental.pallas import tpu as pltpu
from jax.sharding import Mesh
from jax.sharding import PartitionSpec as P


BLOCK = 128
SP = ("sp_0", "sp_1")
DP = ("dp_0", "dp_1")


norm_eps = 1e-05
f32, bf16 = jnp.float32, jnp.bfloat16


def exchange(array, axis):
    return lax.all_to_all(array, axis, split_axis=0, concat_axis=0, tiled=True)


def swapped(array):
    return lax.ppermute(array, "dp_1", [(0, 1), (1, 0)])


def sent_apart(array, step):
    ring = lax.axis_size("dp_0")
    moves = []
    for y in range(ring):
        moves.append((2 * y, 2 * ((y + step) % ring)))
        moves.append((2 * y + 1, 2 * ((y - step) % ring) + 1))
    return lax.ppermute(array, DP, moves)


def normal_below(values):
    return 0.5 * (1.0 + lax.erf(values * (1.0 / math.sqrt(2.0))))


def gelu_slope(values):
    density = jnp.exp(-0.5 * values * values) * (1.0 / math.sqrt(2.0 * math.pi))
    return normal_below(values) + values * density


def causal(weights):
    rows = lax.broadcasted_iota(jnp.int32, (BLOCK, BLOCK), 0)
    cols = lax.broadcasted_iota(jnp.int32, (BLOCK, BLOCK), 1)
    return jnp.where(cols <= rows, weights, jnp.zeros_like(weights))


def nt(a, b, **kw):
    return lax.dot_general(a, b, (((1,), (1,)), ((), ())), preferred_element_type=f32, **kw)


def nn(a, b):
    return jnp.dot(a, b, preferred_element_type=f32)


def call(body, outs, scalars=False, cold=(), free=()):
    def run(*args):
        specs, operands = [], []
        for at, array in enumerate(args):
            if scalars and at == 0:
                specs.append(pl.BlockSpec(memory_space=pltpu.SMEM))
            elif at in free:
                specs.append(pl.BlockSpec())
            elif at in cold:
                specs.append(pl.BlockSpec())
                array = pltpu.with_memory_space_constraint(array, pltpu.HBM)
            else:
                specs.append(pl.BlockSpec(memory_space=pltpu.VMEM))
                array = pltpu.with_memory_space_constraint(array, pltpu.VMEM)
            operands.append(array)
        limit = pltpu.CompilerParams(vmem_limit_bytes=20 * 1024 * 1024)
        made = pl.pallas_call(body, out_shape=outs, in_specs=specs, compiler_params=limit)
        return made(*operands)

    return run


def like(shape, dtype):
    return pltpu.VMEM(shape, dtype)


def stored(shape, dtype):
    return pltpu.HBM(shape, dtype)


def outside(shape, dtype):
    return jax.ShapeDtypeStruct(shape, dtype)


def project_body(hidden, weight, mixing, gain, grad, pre_out, sums_out):
    n_x, n_z, rows, both = weight.shape
    slab = n_x * rows
    pre = None
    for z in range(n_z):
        term = nn(hidden[:, z * slab : (z + 1) * slab], weight[:, z].reshape(slab, both))
        pre = term if pre is None else pre + term
    pre = pre.astype(bf16)
    pre_out[...] = pre
    flipped = causal(mixing[0].astype(f32)).T.astype(bf16)
    gating, _, back, _ = branches(pre, grad[...], flipped, gain[...])
    lane = lax.broadcasted_iota(jnp.int32, gating.shape, 1)
    sums = jnp.zeros_like(gating)
    for at, values in enumerate((gating, gating * gating, back, back * gating)):
        sums = jnp.where(lane == at, jnp.sum(values, axis=1, keepdims=True), sums)
    sums = sums.T
    for peer in range(sums_out.shape[0]):
        sums_out[peer] = sums[:4]


def branches(pre, grad, flipped, gain):
    width = grad.shape[1]
    pre_content = pre[:, :width].astype(f32)
    pre_gating = pre[:, width:].astype(f32)
    gating = pre_gating * normal_below(pre_gating)
    content = pre_content * normal_below(pre_content)
    mixed_grad = (grad.astype(f32) * content).astype(bf16)
    pieces = []
    for at in range(0, mixed_grad.shape[0], BLOCK):
        pieces.append(nn(flipped, mixed_grad[at : at + BLOCK]) * gain)
    return gating, mixed_grad, jnp.concatenate(pieces, axis=0), (pre_content, pre_gating)


def join_body(content, gating, out):
    both = jnp.concatenate([content[...], gating[...]], axis=1)
    for peer in range(out.shape[0]):
        out[peer] = both


def spread_body(arrived, out):
    for peer in range(out.shape[0]):
        out[peer] = arrived[...]


def flip_body(array, out):
    step = 256
    for at in range(0, array.shape[1], step):
        out[at : at + step] = array[:, at : at + step].T


def norm_body(full_width, sums, pre, grad, table, flipped, bias, gain, joined_out, mixing_out):
    gating, mixed_grad, back, (pre_content, pre_gating) = branches(
        pre[...], grad[...], flipped[...], gain[...]
    )
    content_slope = grad[...].astype(f32) * gelu_slope(pre_content)
    total = jnp.sum(sums[...], axis=0) * (1.0 / full_width)
    row_mean = total[0:1]
    row_var = total[1:2] - row_mean * row_mean
    inv_std = lax.rsqrt(row_var + norm_eps)
    first = total[2:3]
    second = inv_std * (total[3:4] - row_mean * first)
    columns = jnp.concatenate([row_mean, inv_std, first, second] * 2, axis=0).T
    row_mean, inv_std, first, second = [columns[:, i : i + 1] for i in range(4)]
    centred = (gating - row_mean) * inv_std
    normed = (centred * gain[...]).astype(bf16)
    shift = jnp.broadcast_to(bias[...], (8, BLOCK)).T[:, 0:1]
    width = normed.shape[1]
    mixing_grad = None
    for at in range(0, normed.shape[0], BLOCK):
        rows = slice(at, at + BLOCK)
        mixed = nn(table[...], normed[rows]) + shift
        joined_out[rows, :width] = (mixed * content_slope[rows]).astype(bf16)
        term = nt(mixed_grad[rows], normed[rows])
        mixing_grad = term if mixing_grad is None else mixing_grad + term
    gating_back = inv_std * (back - first - centred * second)
    joined_out[:, width:] = (gating_back * gelu_slope(pre_gating)).astype(bf16)
    mixing_grad = causal(mixing_grad).astype(bf16)
    half = BLOCK // 2
    mixing_out[...] = jnp.concatenate([mixing_grad[:half], mixing_grad[half:]], axis=1)


def weight_terms_body(hidden_t, joined, mixing_term, out):
    n_x, _, rows, _ = out.shape
    step, last = pl.program_id(0), pl.num_programs(0) - 1

    @pl.when(step < last)
    def _():
        term = nn(hidden_t[...], joined[...]).astype(bf16)
        for x in range(n_x):
            out[x, 0] = term[x * rows : (x + 1) * rows]

    @pl.when(step == last)
    def _():
        for x in range(n_x):
            out[x, 0] = mixing_term[...]


def weight_terms(hidden_t, joined, mixing_term, n_x, n_z):
    tokens, both = joined.shape
    slab = hidden_t.shape[0] // n_z
    inside = pl.BlockSpec(memory_space=pltpu.VMEM)
    return pl.pallas_call(
        weight_terms_body,
        grid=(n_z + 1,),
        out_shape=stored((n_x, n_z + 1, slab // n_x, both), bf16),
        in_specs=[
            pl.BlockSpec((slab, tokens), lambda z: (jnp.minimum(z, n_z - 1), 0)),
            inside,
            inside,
        ],
        out_specs=pl.BlockSpec((n_x, 1, slab // n_x, both), lambda z: (0, z, 0, 0)),
        compiler_params=pltpu.CompilerParams(vmem_limit_bytes=20 * 1024 * 1024),
        name="weight_terms",
    )(
        pltpu.with_memory_space_constraint(hidden_t, pltpu.HBM),
        pltpu.with_memory_space_constraint(joined, pltpu.VMEM),
        pltpu.with_memory_space_constraint(mixing_term, pltpu.VMEM),
    )


def pick_body(where, weight, mixing, mine_out, theirs_out, table_out, flipped_out):
    table = causal(mixing[0].astype(f32))
    table_out[...] = table.astype(bf16)
    flipped_out[...] = table.T.astype(bf16)
    n_x, _, rows, both = weight.shape
    half = n_x // 2
    for out, base, core in ((mine_out, 0, where[10]), (theirs_out, 5, 1 - where[10])):
        at = 0
        for step in (3, 1, 2):
            block = weight[:, pl.ds(where[base + step], 1)].reshape(n_x * rows, both)
            out[at : at + n_x * rows] = block
            at += n_x * rows
        for step in (4, 0):
            block = weight[pl.ds(core * half, half), pl.ds(where[base + step], 1)]
            out[at : at + half * rows] = block.reshape(half * rows, both)
            at += half * rows


def input_terms_body(joined, joined_far, mine, far, odd, two, four, own):
    def term(at, n):
        rows = slice(at, at + n)
        return nt(joined[...], mine[rows]) + nt(joined_far[...], far[rows])

    single, pair = own.shape[1], two.shape[1]
    odd[...] = term(0, 2 * pair).astype(bf16)
    four[...] = term(3 * pair, single).astype(bf16)
    two[...] = term(2 * pair, pair)
    own[...] = term(3 * pair + single, single)


def merge_body(where, two, odd, four, out):
    half = four.shape[1]
    first = where[10] == 0
    extra = four[...].astype(f32)
    none = jnp.zeros_like(extra)
    left = two[:, :half] + odd[:, :half].astype(f32) + jnp.where(first, extra, none)
    right = two[:, half:] + odd[:, half : 2 * half].astype(f32) + jnp.where(first, none, extra)
    out[:, :half] = left.astype(bf16)
    out[:, half:] = right.astype(bf16)


def regroup_body(arrived, out):
    n_z = out.shape[0]
    total = arrived[0].astype(f32)
    for x in range(1, arrived.shape[0]):
        total = total + arrived[x].astype(f32)
    total = total.astype(bf16)
    for z in range(n_z):
        out[z, 0] = total[z]
        out[z, 1] = total[n_z]


def finish_body(scale, arrived, content_out, gating_out, mixing_out):
    total = arrived[0].astype(f32)
    for z in range(1, arrived.shape[0]):
        total = total + arrived[z].astype(f32)
    total = total * scale
    half = content_out.shape[1]
    content_out[...] = total[0][:, :half]
    gating_out[...] = total[0][:, half:]
    mixing_out[0, : BLOCK // 2] = total[1][:, :half]
    mixing_out[0, BLOCK // 2 :] = total[1][:, half:]


def gather_body(where, odd, two, own, keep_out, send_out):
    half = own.shape[1]
    total = odd[:, 2 * half :].astype(f32) + two[...].astype(f32)
    first = where[10] == 0
    left, right = total[:, :half], total[:, half:]
    keep_out[...] = own[...] + jnp.where(first, left, right)
    send_out[...] = jnp.where(first, right, left).astype(bf16)


def step(
    hidden_in, content_weight, gating_weight, norm_gain, mixing_weight, mixing_bias, out_grad
):
    tok_rows, width = hidden_in.shape
    shard_rows, local_width = content_weight.shape
    both = 2 * local_width
    n_z, n_x = lax.axis_size("sp_0"), lax.axis_size("sp_1")
    n_sp, n_dp = n_z * n_x, lax.axis_size(DP)
    ring = lax.axis_size("dp_0")
    full_width = local_width * n_dp
    out_cols = width // n_dp
    grad_scale = 1.0 / math.sqrt(tok_rows * n_sp)
    here, core = lax.axis_index("dp_0"), lax.axis_index("dp_1")
    side = 1 - 2 * core
    ahead = [(here + side * k + ring) % ring for k in range(5)]
    behind = [(here - side * k + ring) % ring for k in range(5)]
    where = jnp.stack(ahead + behind + [core]).astype(jnp.int32)
    gain = norm_gain[None, :]

    hidden_t = call(flip_body, stored((width, tok_rows), bf16))(hidden_in)
    shards = call(join_body, stored((n_z, shard_rows, both), bf16), cold=(0, 1))(
        content_weight, gating_weight
    )
    along_z = exchange(shards, "sp_0")
    spread = call(spread_body, like((n_x, n_z, shard_rows, both), bf16))(along_z)
    weight = exchange(spread, "sp_1")
    single, pair = (tok_rows, out_cols), (tok_rows, 2 * out_cols)
    wide_pair, picked = (tok_rows, 4 * out_cols), (width // 2, both)
    square = like((BLOCK, BLOCK), bf16)
    mine, theirs, table, flipped = call(
        pick_body, (like(picked, bf16), like(picked, bf16), square, square), scalars=True, cold=(2,)
    )(where, weight, mixing_weight)
    far = swapped(theirs)

    wide = (tok_rows, both)
    pre, sums = call(
        project_body, (like(wide, bf16), stored((n_dp, 4, tok_rows), f32))
    )(hidden_in, weight, mixing_weight, gain, out_grad)
    sums = exchange(sums, DP)
    joined, mixing_term = call(
        functools.partial(norm_body, full_width), (like(wide, bf16), like((BLOCK // 2, both), bf16))
    )(sums, pre, out_grad, table, flipped, mixing_bias, gain)

    joined_far = swapped(joined)
    terms = weight_terms(hidden_t, joined, mixing_term, n_x, n_z)
    along_x = exchange(terms, "sp_1")

    odd, two, four, own = call(
        input_terms_body,
        (like(wide_pair, bf16), like(pair, f32), like(single, bf16), like(single, f32)),
    )(joined, joined_far, mine, far)
    four = sent_apart(four, 2)
    odd = sent_apart(odd, 1)
    two = call(merge_body, like(pair, bf16), scalars=True)(where, two, odd, four)
    two = sent_apart(two, 2)

    regrouped = call(regroup_body, stored((n_z, 2, shard_rows, both), bf16))(along_x)
    arrived = exchange(regrouped, "sp_0")

    keep, send = call(
        gather_body, (like(single, f32), like(single, bf16)), scalars=True
    )(where, odd, two, own)
    input_grad = (keep + swapped(send).astype(f32)).astype(bf16)

    content_grad, gating_grad, mixing_grad = call(
        functools.partial(finish_body, grad_scale),
        (
            outside((shard_rows, local_width), f32),
            outside((shard_rows, local_width), f32),
            outside(mixing_weight.shape, f32),
        ),
    )(arrived)
    return (input_grad, content_grad, gating_grad, mixing_grad)


def solution(mesh):
    split = Mesh(mesh.devices.reshape(8, 4, 8, 2), (*SP, *DP))
    in_specs = (
        P(SP, None),
        P(SP, DP),
        P(SP, DP),
        P(DP),
        P(DP, None, None),
        P(DP, None),
        P(SP, DP),
    )
    out_specs = (P(SP, DP), P(SP, DP), P(SP, DP), P(DP, None, None))
    return jax.shard_map(step, mesh=split, in_specs=in_specs, out_specs=out_specs, check_vma=False)
```

```python
import functools
import math

import jax
import jax.numpy as jnp
from jax import lax
from jax.experimental import pallas as pl
from jax.experimental.pallas import tpu as pltpu
from jax.sharding import Mesh
from jax.sharding import PartitionSpec as P


BLOCK = 128
SP = ("sp_0", "sp_1")
DP = ("dp_0", "dp_1")


norm_eps = 1e-05
f32, bf16 = jnp.float32, jnp.bfloat16


def exchange(array, axis):
    return lax.all_to_all(array, axis, split_axis=0, concat_axis=0, tiled=True)


def swapped(array):
    return lax.ppermute(array, "dp_1", [(0, 1), (1, 0)])


def sent_apart(array, step):
    ring = lax.axis_size("dp_0")
    moves = []
    for y in range(ring):
        moves.append((2 * y, 2 * ((y + step) % ring)))
        moves.append((2 * y + 1, 2 * ((y - step) % ring) + 1))
    return lax.ppermute(array, DP, moves)


def normal_below(values):
    return 0.5 * (1.0 + lax.erf(values * (1.0 / math.sqrt(2.0))))


def gelu_slope(values):
    density = jnp.exp(-0.5 * values * values) * (1.0 / math.sqrt(2.0 * math.pi))
    return normal_below(values) + values * density


def causal(weights):
    rows = lax.broadcasted_iota(jnp.int32, (BLOCK, BLOCK), 0)
    cols = lax.broadcasted_iota(jnp.int32, (BLOCK, BLOCK), 1)
    return jnp.where(cols <= rows, weights, jnp.zeros_like(weights))


def nt(a, b, **kw):
    return lax.dot_general(a, b, (((1,), (1,)), ((), ())), preferred_element_type=f32, **kw)


def nn(a, b):
    return jnp.dot(a, b, preferred_element_type=f32)


def call(body, outs, scalars=False, cold=(), free=()):
    def run(*args):
        specs, operands = [], []
        for at, array in enumerate(args):
            if scalars and at == 0:
                specs.append(pl.BlockSpec(memory_space=pltpu.SMEM))
            elif at in free:
                specs.append(pl.BlockSpec())
            elif at in cold:
                specs.append(pl.BlockSpec())
                array = pltpu.with_memory_space_constraint(array, pltpu.HBM)
            else:
                specs.append(pl.BlockSpec(memory_space=pltpu.VMEM))
                array = pltpu.with_memory_space_constraint(array, pltpu.VMEM)
            operands.append(array)
        limit = pltpu.CompilerParams(vmem_limit_bytes=20 * 1024 * 1024)
        made = pl.pallas_call(body, out_shape=outs, in_specs=specs, compiler_params=limit)
        return made(*operands)

    return run


def like(shape, dtype):
    return pltpu.VMEM(shape, dtype)


def stored(shape, dtype):
    return pltpu.HBM(shape, dtype)


def outside(shape, dtype):
    return jax.ShapeDtypeStruct(shape, dtype)


def project_body(hidden, weight, mixing, gain, grad, pre_out, sums_out):
    n_x, n_z, rows, both = weight.shape
    slab = n_x * rows
    pre = None
    for z in range(n_z):
        term = nn(hidden[:, z * slab : (z + 1) * slab], weight[:, z].reshape(slab, both))
        pre = term if pre is None else pre + term
    pre = pre.astype(bf16)
    pre_out[...] = pre
    flipped = causal(mixing[0].astype(f32)).T.astype(bf16)
    gating, _, back, _ = branches(pre, grad[...], flipped, gain[...])
    lane = lax.broadcasted_iota(jnp.int32, gating.shape, 1)
    sums = jnp.zeros_like(gating)
    for at, values in enumerate((gating, gating * gating, back, back * gating)):
        sums = jnp.where(lane == at, jnp.sum(values, axis=1, keepdims=True), sums)
    sums = sums.T
    for peer in range(sums_out.shape[0]):
        sums_out[peer] = sums[:4]


def branches(pre, grad, flipped, gain):
    width = grad.shape[1]
    pre_content = pre[:, :width].astype(f32)
    pre_gating = pre[:, width:].astype(f32)
    gating = pre_gating * normal_below(pre_gating)
    content = pre_content * normal_below(pre_content)
    mixed_grad = (grad.astype(f32) * content).astype(bf16)
    pieces = []
    for at in range(0, mixed_grad.shape[0], BLOCK):
        pieces.append(nn(flipped, mixed_grad[at : at + BLOCK]) * gain)
    return gating, mixed_grad, jnp.concatenate(pieces, axis=0), (pre_content, pre_gating)


def join_body(content, gating, out):
    both = jnp.concatenate([content[...], gating[...]], axis=1)
    for peer in range(out.shape[0]):
        out[peer] = both


def spread_body(arrived, out):
    for peer in range(out.shape[0]):
        out[peer] = arrived[...]


def flip_body(array, out):
    step = 256
    for at in range(0, array.shape[1], step):
        out[at : at + step] = array[:, at : at + step].T


def norm_body(full_width, sums, pre, grad, table, flipped, bias, gain, joined_out, mixing_out):
    gating, mixed_grad, back, (pre_content, pre_gating) = branches(
        pre[...], grad[...], flipped[...], gain[...]
    )
    content_slope = grad[...].astype(f32) * gelu_slope(pre_content)
    total = jnp.sum(sums[...], axis=0) * (1.0 / full_width)
    row_mean = total[0:1]
    row_var = total[1:2] - row_mean * row_mean
    inv_std = lax.rsqrt(row_var + norm_eps)
    first = total[2:3]
    second = inv_std * (total[3:4] - row_mean * first)
    columns = jnp.concatenate([row_mean, inv_std, first, second] * 2, axis=0).T
    row_mean, inv_std, first, second = [columns[:, i : i + 1] for i in range(4)]
    centred = (gating - row_mean) * inv_std
    normed = (centred * gain[...]).astype(bf16)
    shift = jnp.broadcast_to(bias[...], (8, BLOCK)).T[:, 0:1]
    width = normed.shape[1]
    mixing_grad = None
    for at in range(0, normed.shape[0], BLOCK):
        rows = slice(at, at + BLOCK)
        mixed = nn(table[...], normed[rows]) + shift
        joined_out[rows, :width] = (mixed * content_slope[rows]).astype(bf16)
        term = nt(mixed_grad[rows], normed[rows])
        mixing_grad = term if mixing_grad is None else mixing_grad + term
    gating_back = inv_std * (back - first - centred * second)
    joined_out[:, width:] = (gating_back * gelu_slope(pre_gating)).astype(bf16)
    mixing_grad = causal(mixing_grad).astype(bf16)
    half = BLOCK // 2
    mixing_out[...] = jnp.concatenate([mixing_grad[:half], mixing_grad[half:]], axis=1)


def weight_terms_body(hidden_t, joined, mixing_term, out, held, made, come, gone):
    n_x, n_all, rows, both = out.shape
    n_z = n_all - 1
    slab = n_x * rows
    loads = [
        pltpu.make_async_copy(hidden_t.at[pl.ds(z * slab, slab)], held.at[z], come.at[z])
        for z in range(n_z)
    ]
    stores = [
        pltpu.make_async_copy(made.at[z], out.at[:, z], gone.at[z]) for z in range(n_all)
    ]
    for load in loads:
        load.start()
    for x in range(n_x):
        made[n_z, x] = mixing_term[...]
    stores[n_z].start()
    for z in range(n_z):
        loads[z].wait()
        made[z] = nn(held[z], joined[...]).astype(bf16).reshape(n_x, rows, both)
        stores[z].start()
    for store in stores:
        store.wait()


def weight_terms(hidden_t, joined, mixing_term, n_x, n_z):
    tokens, both = joined.shape
    slab = hidden_t.shape[0] // n_z
    rows = slab // n_x
    near, far = pl.BlockSpec(memory_space=pltpu.VMEM), pl.BlockSpec(memory_space=pl.ANY)
    return pl.pallas_call(
        weight_terms_body,
        out_shape=stored((n_x, n_z + 1, rows, both), bf16),
        in_specs=[far, near, near],
        out_specs=far,
        scratch_shapes=[
            pltpu.VMEM((n_z, slab, tokens), bf16),
            pltpu.VMEM((n_z + 1, n_x, rows, both), bf16),
            pltpu.SemaphoreType.DMA((n_z,)),
            pltpu.SemaphoreType.DMA((n_z + 1,)),
        ],
        compiler_params=pltpu.CompilerParams(vmem_limit_bytes=20 * 1024 * 1024),
        name="weight_terms",
    )(
        pltpu.with_memory_space_constraint(hidden_t, pltpu.HBM),
        pltpu.with_memory_space_constraint(joined, pltpu.VMEM),
        pltpu.with_memory_space_constraint(mixing_term, pltpu.VMEM),
    )


def pick_body(where, weight, mixing, mine_out, theirs_out, table_out, flipped_out):
    table = causal(mixing[0].astype(f32))
    table_out[...] = table.astype(bf16)
    flipped_out[...] = table.T.astype(bf16)
    n_x, _, rows, both = weight.shape
    half = n_x // 2
    for out, base, core in ((mine_out, 0, where[10]), (theirs_out, 5, 1 - where[10])):
        at = 0
        for step in (3, 1, 2):
            block = weight[:, pl.ds(where[base + step], 1)].reshape(n_x * rows, both)
            out[at : at + n_x * rows] = block
            at += n_x * rows
        for step in (4, 0):
            block = weight[pl.ds(core * half, half), pl.ds(where[base + step], 1)]
            out[at : at + half * rows] = block.reshape(half * rows, both)
            at += half * rows


def input_terms_body(joined, joined_far, mine, far, odd, two, four, own):
    def term(at, n):
        rows = slice(at, at + n)
        return nt(joined[...], mine[rows]) + nt(joined_far[...], far[rows])

    single, pair = own.shape[1], two.shape[1]
    odd[...] = term(0, 2 * pair).astype(bf16)
    four[...] = term(3 * pair, single).astype(bf16)
    two[...] = term(2 * pair, pair)
    own[...] = term(3 * pair + single, single)


def merge_body(where, two, odd, four, out):
    half = four.shape[1]
    first = where[10] == 0
    extra = four[...].astype(f32)
    none = jnp.zeros_like(extra)
    left = two[:, :half] + odd[:, :half].astype(f32) + jnp.where(first, extra, none)
    right = two[:, half:] + odd[:, half : 2 * half].astype(f32) + jnp.where(first, none, extra)
    out[:, :half] = left.astype(bf16)
    out[:, half:] = right.astype(bf16)


def regroup_body(arrived, out):
    n_z = out.shape[0]
    total = arrived[0].astype(f32)
    for x in range(1, arrived.shape[0]):
        total = total + arrived[x].astype(f32)
    total = total.astype(bf16)
    for z in range(n_z):
        out[z, 0] = total[z]
        out[z, 1] = total[n_z]


def finish_body(scale, arrived, content_out, gating_out, mixing_out):
    total = arrived[0].astype(f32)
    for z in range(1, arrived.shape[0]):
        total = total + arrived[z].astype(f32)
    total = total * scale
    half = content_out.shape[1]
    content_out[...] = total[0][:, :half]
    gating_out[...] = total[0][:, half:]
    mixing_out[0, : BLOCK // 2] = total[1][:, :half]
    mixing_out[0, BLOCK // 2 :] = total[1][:, half:]


def gather_body(where, odd, two, own, keep_out, send_out):
    half = own.shape[1]
    total = odd[:, 2 * half :].astype(f32) + two[...].astype(f32)
    first = where[10] == 0
    left, right = total[:, :half], total[:, half:]
    keep_out[...] = own[...] + jnp.where(first, left, right)
    send_out[...] = jnp.where(first, right, left).astype(bf16)


def step(
    hidden_in, content_weight, gating_weight, norm_gain, mixing_weight, mixing_bias, out_grad
):
    tok_rows, width = hidden_in.shape
    shard_rows, local_width = content_weight.shape
    both = 2 * local_width
    n_z, n_x = lax.axis_size("sp_0"), lax.axis_size("sp_1")
    n_sp, n_dp = n_z * n_x, lax.axis_size(DP)
    ring = lax.axis_size("dp_0")
    full_width = local_width * n_dp
    out_cols = width // n_dp
    grad_scale = 1.0 / math.sqrt(tok_rows * n_sp)
    here, core = lax.axis_index("dp_0"), lax.axis_index("dp_1")
    side = 1 - 2 * core
    ahead = [(here + side * k + ring) % ring for k in range(5)]
    behind = [(here - side * k + ring) % ring for k in range(5)]
    where = jnp.stack(ahead + behind + [core]).astype(jnp.int32)
    gain = norm_gain[None, :]

    hidden_t = call(flip_body, stored((width, tok_rows), bf16))(hidden_in)
    shards = call(join_body, stored((n_z, shard_rows, both), bf16), cold=(0, 1))(
        content_weight, gating_weight
    )
    along_z = exchange(shards, "sp_0")
    spread = call(spread_body, like((n_x, n_z, shard_rows, both), bf16))(along_z)
    weight = exchange(spread, "sp_1")
    single, pair = (tok_rows, out_cols), (tok_rows, 2 * out_cols)
    wide_pair, picked = (tok_rows, 4 * out_cols), (width // 2, both)
    square = like((BLOCK, BLOCK), bf16)
    mine, theirs, table, flipped = call(
        pick_body, (like(picked, bf16), like(picked, bf16), square, square), scalars=True, cold=(2,)
    )(where, weight, mixing_weight)
    far = swapped(theirs)

    wide = (tok_rows, both)
    pre, sums = call(
        project_body, (like(wide, bf16), stored((n_dp, 4, tok_rows), f32))
    )(hidden_in, weight, mixing_weight, gain, out_grad)
    sums = exchange(sums, DP)
    joined, mixing_term = call(
        functools.partial(norm_body, full_width), (like(wide, bf16), like((BLOCK // 2, both), bf16))
    )(sums, pre, out_grad, table, flipped, mixing_bias, gain)

    joined_far = swapped(joined)
    terms = weight_terms(hidden_t, joined, mixing_term, n_x, n_z)
    along_x = exchange(terms, "sp_1")

    odd, two, four, own = call(
        input_terms_body,
        (like(wide_pair, bf16), like(pair, f32), like(single, bf16), like(single, f32)),
    )(joined, joined_far, mine, far)
    four = sent_apart(four, 2)
    odd = sent_apart(odd, 1)
    two = call(merge_body, like(pair, bf16), scalars=True)(where, two, odd, four)
    two = sent_apart(two, 2)

    regrouped = call(regroup_body, stored((n_z, 2, shard_rows, both), bf16))(along_x)
    arrived = exchange(regrouped, "sp_0")

    keep, send = call(
        gather_body, (like(single, f32), like(single, bf16)), scalars=True
    )(where, odd, two, own)
    input_grad = (keep + swapped(send).astype(f32)).astype(bf16)

    content_grad, gating_grad, mixing_grad = call(
        functools.partial(finish_body, grad_scale),
        (
            outside((shard_rows, local_width), f32),
            outside((shard_rows, local_width), f32),
            outside(mixing_weight.shape, f32),
        ),
    )(arrived)
    return (input_grad, content_grad, gating_grad, mixing_grad)


def solution(mesh):
    split = Mesh(mesh.devices.reshape(8, 4, 8, 2), (*SP, *DP))
    in_specs = (
        P(SP, None),
        P(SP, DP),
        P(SP, DP),
        P(DP),
        P(DP, None, None),
        P(DP, None),
        P(SP, DP),
    )
    out_specs = (P(SP, DP), P(SP, DP), P(SP, DP), P(DP, None, None))
    return jax.shard_map(step, mesh=split, in_specs=in_specs, out_specs=out_specs, check_vma=False)
```

```python
import functools
import math

import jax
import jax.numpy as jnp
from jax import lax
from jax.experimental import pallas as pl
from jax.experimental.pallas import tpu as pltpu
from jax.sharding import Mesh
from jax.sharding import PartitionSpec as P


BLOCK = 128
SP = ("sp_0", "sp_1")
DP = ("dp_0", "dp_1")


norm_eps = 1e-05
f32, bf16 = jnp.float32, jnp.bfloat16


def exchange(array, axis):
    return lax.all_to_all(array, axis, split_axis=0, concat_axis=0, tiled=True)


def swapped(array):
    return lax.ppermute(array, "dp_1", [(0, 1), (1, 0)])


def sent_apart(array, step, cross=False):
    ring = lax.axis_size("dp_0")
    moves = []
    for y in range(ring):
        for core, there in ((0, (y + step) % ring), (1, (y - step) % ring)):
            moves.append((2 * y + core, 2 * there + (1 - core if cross else core)))
    return lax.ppermute(array, DP, moves)


def normal_below(values):
    return 0.5 * (1.0 + lax.erf(values * (1.0 / math.sqrt(2.0))))


def gelu_slope(values):
    density = jnp.exp(-0.5 * values * values) * (1.0 / math.sqrt(2.0 * math.pi))
    return normal_below(values) + values * density


def causal(weights):
    rows = lax.broadcasted_iota(jnp.int32, (BLOCK, BLOCK), 0)
    cols = lax.broadcasted_iota(jnp.int32, (BLOCK, BLOCK), 1)
    return jnp.where(cols <= rows, weights, jnp.zeros_like(weights))


def nt(a, b, **kw):
    return lax.dot_general(a, b, (((1,), (1,)), ((), ())), preferred_element_type=f32, **kw)


def nn(a, b):
    return jnp.dot(a, b, preferred_element_type=f32)


def call(body, outs, scalars=False, cold=(), free=()):
    def run(*args):
        specs, operands = [], []
        for at, array in enumerate(args):
            if scalars and at == 0:
                specs.append(pl.BlockSpec(memory_space=pltpu.SMEM))
            elif at in free:
                specs.append(pl.BlockSpec())
            elif at in cold:
                specs.append(pl.BlockSpec())
                array = pltpu.with_memory_space_constraint(array, pltpu.HBM)
            else:
                specs.append(pl.BlockSpec(memory_space=pltpu.VMEM))
                array = pltpu.with_memory_space_constraint(array, pltpu.VMEM)
            operands.append(array)
        limit = pltpu.CompilerParams(vmem_limit_bytes=20 * 1024 * 1024)
        made = pl.pallas_call(body, out_shape=outs, in_specs=specs, compiler_params=limit)
        return made(*operands)

    return run


def like(shape, dtype):
    return pltpu.VMEM(shape, dtype)


def stored(shape, dtype):
    return pltpu.HBM(shape, dtype)


def outside(shape, dtype):
    return jax.ShapeDtypeStruct(shape, dtype)


def project_body(hidden, weight, mixing, gain, grad, pre_out, sums_out):
    n_x, n_z, rows, both = weight.shape
    slab = n_x * rows
    pre = None
    for z in range(n_z):
        term = nn(hidden[:, z * slab : (z + 1) * slab], weight[:, z].reshape(slab, both))
        pre = term if pre is None else pre + term
    pre = pre.astype(bf16)
    pre_out[...] = pre
    flipped = causal(mixing[0].astype(f32)).T.astype(bf16)
    gating, _, back, _ = branches(pre, grad[...], flipped, gain[...])
    lane = lax.broadcasted_iota(jnp.int32, gating.shape, 1)
    sums = jnp.zeros_like(gating)
    for at, values in enumerate((gating, gating * gating, back, back * gating)):
        sums = jnp.where(lane == at, jnp.sum(values, axis=1, keepdims=True), sums)
    sums = sums.T
    for peer in range(sums_out.shape[0]):
        sums_out[peer] = sums[:4]


def branches(pre, grad, flipped, gain):
    width = grad.shape[1]
    pre_content = pre[:, :width].astype(f32)
    pre_gating = pre[:, width:].astype(f32)
    gating = pre_gating * normal_below(pre_gating)
    content = pre_content * normal_below(pre_content)
    mixed_grad = (grad.astype(f32) * content).astype(bf16)
    pieces = []
    for at in range(0, mixed_grad.shape[0], BLOCK):
        pieces.append(nn(flipped, mixed_grad[at : at + BLOCK]) * gain)
    return gating, mixed_grad, jnp.concatenate(pieces, axis=0), (pre_content, pre_gating)


def join_body(content, gating, out):
    both = jnp.concatenate([content[...], gating[...]], axis=1)
    for peer in range(out.shape[0]):
        out[peer] = both


def spread_body(arrived, out):
    for peer in range(out.shape[0]):
        out[peer] = arrived[...]


def flip_body(array, out):
    step = 256
    for at in range(0, array.shape[1], step):
        out[at : at + step] = array[:, at : at + step].T


def norm_body(full_width, sums, pre, grad, table, flipped, bias, gain, joined_out, mixing_out):
    gating, mixed_grad, back, (pre_content, pre_gating) = branches(
        pre[...], grad[...], flipped[...], gain[...]
    )
    content_slope = grad[...].astype(f32) * gelu_slope(pre_content)
    total = jnp.sum(sums[...], axis=0) * (1.0 / full_width)
    row_mean = total[0:1]
    row_var = total[1:2] - row_mean * row_mean
    inv_std = lax.rsqrt(row_var + norm_eps)
    first = total[2:3]
    second = inv_std * (total[3:4] - row_mean * first)
    columns = jnp.concatenate([row_mean, inv_std, first, second] * 2, axis=0).T
    row_mean, inv_std, first, second = [columns[:, i : i + 1] for i in range(4)]
    centred = (gating - row_mean) * inv_std
    normed = (centred * gain[...]).astype(bf16)
    shift = jnp.broadcast_to(bias[...], (8, BLOCK)).T[:, 0:1]
    width = normed.shape[1]
    mixing_grad = None
    for at in range(0, normed.shape[0], BLOCK):
        rows = slice(at, at + BLOCK)
        mixed = nn(table[...], normed[rows]) + shift
        joined_out[rows, :width] = (mixed * content_slope[rows]).astype(bf16)
        term = nt(mixed_grad[rows], normed[rows])
        mixing_grad = term if mixing_grad is None else mixing_grad + term
    gating_back = inv_std * (back - first - centred * second)
    joined_out[:, width:] = (gating_back * gelu_slope(pre_gating)).astype(bf16)
    mixing_grad = causal(mixing_grad).astype(bf16)
    half = BLOCK // 2
    mixing_out[...] = jnp.concatenate([mixing_grad[:half], mixing_grad[half:]], axis=1)


def weight_terms_body(hidden_t, joined, mixing_term, out, held, made, come, gone):
    n_x, n_all, rows, both = out.shape
    parts, chunk, _ = held.shape
    deep = (n_all - 1) // parts
    loads = [
        pltpu.make_async_copy(hidden_t.at[pl.ds(i * chunk, chunk)], held.at[i], come.at[i])
        for i in range(parts)
    ]
    stores = [
        pltpu.make_async_copy(made.at[z], out.at[:, z], gone.at[z]) for z in range(n_all)
    ]
    for load in loads:
        load.start()
    for x in range(n_x):
        made[n_all - 1, x] = mixing_term[...]
    stores[n_all - 1].start()
    for i in range(parts):
        loads[i].wait()
        term = nn(held[i], joined[...]).astype(bf16)
        made[i * deep : (i + 1) * deep] = term.reshape(deep, n_x, rows, both)
        for z in range(i * deep, (i + 1) * deep):
            stores[z].start()
    for store in stores:
        store.wait()


def weight_terms(hidden_t, joined, mixing_term, n_x, n_z):
    tokens, both = joined.shape
    rows = hidden_t.shape[0] // (n_x * n_z)
    parts = 4
    near, far = pl.BlockSpec(memory_space=pltpu.VMEM), pl.BlockSpec(memory_space=pl.ANY)
    return pl.pallas_call(
        weight_terms_body,
        out_shape=stored((n_x, n_z + 1, rows, both), bf16),
        in_specs=[far, near, near],
        out_specs=far,
        scratch_shapes=[
            pltpu.VMEM((parts, hidden_t.shape[0] // parts, tokens), bf16),
            pltpu.VMEM((n_z + 1, n_x, rows, both), bf16),
            pltpu.SemaphoreType.DMA((parts,)),
            pltpu.SemaphoreType.DMA((n_z + 1,)),
        ],
        compiler_params=pltpu.CompilerParams(vmem_limit_bytes=20 * 1024 * 1024),
        name="weight_terms",
    )(
        pltpu.with_memory_space_constraint(hidden_t, pltpu.HBM),
        pltpu.with_memory_space_constraint(joined, pltpu.VMEM),
        pltpu.with_memory_space_constraint(mixing_term, pltpu.VMEM),
    )


def pick_body(where, weight, mixing, mine_out, theirs_out, table_out, flipped_out):
    table = causal(mixing[0].astype(f32))
    table_out[...] = table.astype(bf16)
    flipped_out[...] = table.T.astype(bf16)
    n_x, _, rows, both = weight.shape
    half = n_x // 2
    for out, base, core in ((mine_out, 0, where[10]), (theirs_out, 5, 1 - where[10])):
        at = 0
        for step in (3, 1, 2):
            block = weight[:, pl.ds(where[base + step], 1)].reshape(n_x * rows, both)
            out[at : at + n_x * rows] = block
            at += n_x * rows
        for step in (4, 0):
            block = weight[pl.ds(core * half, half), pl.ds(where[base + step], 1)]
            out[at : at + half * rows] = block.reshape(half * rows, both)
            at += half * rows


def input_terms_body(joined, joined_far, mine, far, odd, two, four, own):
    def term(at, n):
        rows = slice(at, at + n)
        return nt(joined[...], mine[rows]) + nt(joined_far[...], far[rows])

    single, pair = own.shape[1], two.shape[1]
    odd[...] = term(0, 2 * pair).astype(bf16)
    four[...] = term(3 * pair, single).astype(bf16)
    two[...] = term(2 * pair, pair)
    own[...] = term(3 * pair + single, single)


def merge_body(where, two, odd, four, same_out, other_out, keep_out, send_out):
    half = four.shape[1]
    first = where[10] == 0
    both = two[...] + odd[:, : 2 * half].astype(f32)
    left, right = both[:, :half], both[:, half:]
    same_out[...] = (jnp.where(first, left, right) + four[...].astype(f32)).astype(bf16)
    other_out[...] = jnp.where(first, right, left).astype(bf16)
    left, right = odd[:, 2 * half : 3 * half], odd[:, 3 * half :]
    left, right = left.astype(f32), right.astype(f32)
    keep_out[...] = jnp.where(first, left, right).astype(bf16)
    send_out[...] = jnp.where(first, right, left).astype(bf16)


def total_body(own, same, other, keep, sent, out):
    total = own[...]
    for part in (same, other, keep, sent):
        total = total + part[...].astype(f32)
    out[...] = total.astype(bf16)


def regroup_body(arrived, out):
    n_z = out.shape[0]
    total = arrived[0].astype(f32)
    for x in range(1, arrived.shape[0]):
        total = total + arrived[x].astype(f32)
    total = total.astype(bf16)
    for z in range(n_z):
        out[z, 0] = total[z]
        out[z, 1] = total[n_z]


def finish_body(scale, arrived, content_out, gating_out, mixing_out):
    total = arrived[0].astype(f32)
    for z in range(1, arrived.shape[0]):
        total = total + arrived[z].astype(f32)
    total = total * scale
    half = content_out.shape[1]
    content_out[...] = total[0][:, :half]
    gating_out[...] = total[0][:, half:]
    mixing_out[0, : BLOCK // 2] = total[1][:, :half]
    mixing_out[0, BLOCK // 2 :] = total[1][:, half:]


def step(
    hidden_in, content_weight, gating_weight, norm_gain, mixing_weight, mixing_bias, out_grad
):
    tok_rows, width = hidden_in.shape
    shard_rows, local_width = content_weight.shape
    both = 2 * local_width
    n_z, n_x = lax.axis_size("sp_0"), lax.axis_size("sp_1")
    n_sp, n_dp = n_z * n_x, lax.axis_size(DP)
    ring = lax.axis_size("dp_0")
    full_width = local_width * n_dp
    out_cols = width // n_dp
    grad_scale = 1.0 / math.sqrt(tok_rows * n_sp)
    here, core = lax.axis_index("dp_0"), lax.axis_index("dp_1")
    side = 1 - 2 * core
    ahead = [(here + side * k + ring) % ring for k in range(5)]
    behind = [(here - side * k + ring) % ring for k in range(5)]
    where = jnp.stack(ahead + behind + [core]).astype(jnp.int32)
    gain = norm_gain[None, :]

    hidden_t = call(flip_body, stored((width, tok_rows), bf16))(hidden_in)
    shards = call(join_body, stored((n_z, shard_rows, both), bf16), cold=(0, 1))(
        content_weight, gating_weight
    )
    along_z = exchange(shards, "sp_0")
    spread = call(spread_body, like((n_x, n_z, shard_rows, both), bf16))(along_z)
    weight = exchange(spread, "sp_1")
    single, pair = (tok_rows, out_cols), (tok_rows, 2 * out_cols)
    wide_pair, picked = (tok_rows, 4 * out_cols), (width // 2, both)
    square = like((BLOCK, BLOCK), bf16)
    mine, theirs, table, flipped = call(
        pick_body, (like(picked, bf16), like(picked, bf16), square, square), scalars=True, cold=(2,)
    )(where, weight, mixing_weight)
    far = swapped(theirs)

    wide = (tok_rows, both)
    pre, sums = call(
        project_body, (like(wide, bf16), stored((n_dp, 4, tok_rows), f32))
    )(hidden_in, weight, mixing_weight, gain, out_grad)
    sums = exchange(sums, DP)
    joined, mixing_term = call(
        functools.partial(norm_body, full_width), (like(wide, bf16), like((BLOCK // 2, both), bf16))
    )(sums, pre, out_grad, table, flipped, mixing_bias, gain)

    joined_far = swapped(joined)
    terms = weight_terms(hidden_t, joined, mixing_term, n_x, n_z)
    along_x = exchange(terms, "sp_1")

    odd, two, four, own = call(
        input_terms_body,
        (like(wide_pair, bf16), like(pair, f32), like(single, bf16), like(single, f32)),
    )(joined, joined_far, mine, far)
    four = sent_apart(four, 2)
    odd = sent_apart(odd, 1)
    small = like(single, bf16)
    same, other, keep, send = call(merge_body, (small,) * 4, scalars=True)(where, two, odd, four)
    same = sent_apart(same, 2)
    other = sent_apart(other, 2, True)
    sent = swapped(send)

    regrouped = call(regroup_body, stored((n_z, 2, shard_rows, both), bf16))(along_x)
    arrived = exchange(regrouped, "sp_0")

    input_grad = call(total_body, outside(single, bf16))(own, same, other, keep, sent)

    content_grad, gating_grad, mixing_grad = call(
        functools.partial(finish_body, grad_scale),
        (
            outside((shard_rows, local_width), f32),
            outside((shard_rows, local_width), f32),
            outside(mixing_weight.shape, f32),
        ),
    )(arrived)
    return (input_grad, content_grad, gating_grad, mixing_grad)


def solution(mesh):
    split = Mesh(mesh.devices.reshape(8, 4, 8, 2), (*SP, *DP))
    in_specs = (
        P(SP, None),
        P(SP, DP),
        P(SP, DP),
        P(DP),
        P(DP, None, None),
        P(DP, None),
        P(SP, DP),
    )
    out_specs = (P(SP, DP), P(SP, DP), P(SP, DP), P(DP, None, None))
    return jax.shard_map(step, mesh=split, in_specs=in_specs, out_specs=out_specs, check_vma=False)
```

```python
import functools
import math

import jax
import jax.numpy as jnp
from jax import lax
from jax.experimental import pallas as pl
from jax.experimental.pallas import tpu as pltpu
from jax.sharding import Mesh
from jax.sharding import PartitionSpec as P


BLOCK = 128
SP = ("sp_0", "sp_1")
DP = ("dp_0", "dp_1")


norm_eps = 1e-05
f32, bf16 = jnp.float32, jnp.bfloat16


def exchange(array, axis):
    return lax.all_to_all(array, axis, split_axis=0, concat_axis=0, tiled=True)


def swapped(array):
    return lax.ppermute(array, "dp_1", [(0, 1), (1, 0)])


def sent_apart(array, step, cross=False):
    ring = lax.axis_size("dp_0")
    moves = []
    for y in range(ring):
        for core, there in ((0, (y + step) % ring), (1, (y - step) % ring)):
            moves.append((2 * y + core, 2 * there + (1 - core if cross else core)))
    return lax.ppermute(array, DP, moves)


def normal_below(values):
    return 0.5 * (1.0 + lax.erf(values * (1.0 / math.sqrt(2.0))))


def gelu_slope(values):
    density = jnp.exp(-0.5 * values * values) * (1.0 / math.sqrt(2.0 * math.pi))
    return normal_below(values) + values * density


def causal(weights):
    rows = lax.broadcasted_iota(jnp.int32, (BLOCK, BLOCK), 0)
    cols = lax.broadcasted_iota(jnp.int32, (BLOCK, BLOCK), 1)
    return jnp.where(cols <= rows, weights, jnp.zeros_like(weights))


def nt(a, b, **kw):
    return lax.dot_general(a, b, (((1,), (1,)), ((), ())), preferred_element_type=f32, **kw)


def nn(a, b):
    return jnp.dot(a, b, preferred_element_type=f32)


def call(body, outs, scalars=False, cold=(), free=()):
    def run(*args):
        specs, operands = [], []
        for at, array in enumerate(args):
            if scalars and at == 0:
                specs.append(pl.BlockSpec(memory_space=pltpu.SMEM))
            elif at in free:
                specs.append(pl.BlockSpec())
            elif at in cold:
                specs.append(pl.BlockSpec())
                array = pltpu.with_memory_space_constraint(array, pltpu.HBM)
            else:
                specs.append(pl.BlockSpec(memory_space=pltpu.VMEM))
                array = pltpu.with_memory_space_constraint(array, pltpu.VMEM)
            operands.append(array)
        limit = pltpu.CompilerParams(vmem_limit_bytes=20 * 1024 * 1024)
        made = pl.pallas_call(body, out_shape=outs, in_specs=specs, compiler_params=limit)
        return made(*operands)

    return run


def like(shape, dtype):
    return pltpu.VMEM(shape, dtype)


def stored(shape, dtype):
    return pltpu.HBM(shape, dtype)


def outside(shape, dtype):
    return jax.ShapeDtypeStruct(shape, dtype)


def project_body(hidden, weight, mixing, gain, grad, pre_out, sums_out):
    n_x, n_z, rows, both = weight.shape
    slab = n_x * rows
    pre = None
    for z in range(n_z):
        term = nn(hidden[:, z * slab : (z + 1) * slab], weight[:, z].reshape(slab, both))
        pre = term if pre is None else pre + term
    pre = pre.astype(bf16)
    pre_out[...] = pre
    flipped = causal(mixing[0].astype(f32)).T.astype(bf16)
    gating, _, back, _ = branches(pre, grad[...], flipped, gain[...])
    lane = lax.broadcasted_iota(jnp.int32, gating.shape, 1)
    sums = jnp.zeros_like(gating)
    for at, values in enumerate((gating, gating * gating, back, back * gating)):
        sums = jnp.where(lane == at, jnp.sum(values, axis=1, keepdims=True), sums)
    sums = sums.T
    for peer in range(sums_out.shape[0]):
        sums_out[peer] = sums[:4]


def branches(pre, grad, flipped, gain):
    width = grad.shape[1]
    pre_content = pre[:, :width].astype(f32)
    pre_gating = pre[:, width:].astype(f32)
    gating = pre_gating * normal_below(pre_gating)
    content = pre_content * normal_below(pre_content)
    mixed_grad = (grad.astype(f32) * content).astype(bf16)
    pieces = []
    for at in range(0, mixed_grad.shape[0], BLOCK):
        pieces.append(nn(flipped, mixed_grad[at : at + BLOCK]) * gain)
    return gating, mixed_grad, jnp.concatenate(pieces, axis=0), (pre_content, pre_gating)


def join_body(content, gating, out):
    both = jnp.concatenate([content[...], gating[...]], axis=1)
    for peer in range(out.shape[0]):
        out[peer] = both


def spread_body(arrived, out):
    for peer in range(out.shape[0]):
        out[peer] = arrived[...]


def flip_body(array, out):
    step = 256
    for at in range(0, array.shape[1], step):
        out[at : at + step] = array[:, at : at + step].T


def norm_terms_body(full_width, sums, pre, grad, table, flipped, bias, gain, hidden_t, joined_out, out, held, made, come, gone):
    n_x, n_all, rows, both = out.shape
    parts, chunk, _ = held.shape
    deep = (n_all - 1) // parts
    loads = [
        pltpu.make_async_copy(hidden_t.at[pl.ds(i * chunk, chunk)], held.at[i], come.at[i])
        for i in range(parts)
    ]
    stores = [
        pltpu.make_async_copy(made.at[z], out.at[:, z], gone.at[z]) for z in range(n_all)
    ]
    for load in loads:
        load.start()
    gating, mixed_grad, back, (pre_content, pre_gating) = branches(
        pre[...], grad[...], flipped[...], gain[...]
    )
    content_slope = grad[...].astype(f32) * gelu_slope(pre_content)
    total = jnp.sum(sums[...], axis=0) * (1.0 / full_width)
    row_mean = total[0:1]
    row_var = total[1:2] - row_mean * row_mean
    inv_std = lax.rsqrt(row_var + norm_eps)
    first = total[2:3]
    second = inv_std * (total[3:4] - row_mean * first)
    columns = jnp.concatenate([row_mean, inv_std, first, second] * 2, axis=0).T
    row_mean, inv_std, first, second = [columns[:, i : i + 1] for i in range(4)]
    centred = (gating - row_mean) * inv_std
    normed = (centred * gain[...]).astype(bf16)
    shift = jnp.broadcast_to(bias[...], (8, BLOCK)).T[:, 0:1]
    width = normed.shape[1]
    mixing_grad = None
    for at in range(0, normed.shape[0], BLOCK):
        block = slice(at, at + BLOCK)
        mixed = nn(table[...], normed[block]) + shift
        joined_out[block, :width] = (mixed * content_slope[block]).astype(bf16)
        term = nt(mixed_grad[block], normed[block])
        mixing_grad = term if mixing_grad is None else mixing_grad + term
    gating_back = inv_std * (back - first - centred * second)
    joined_out[:, width:] = (gating_back * gelu_slope(pre_gating)).astype(bf16)
    mixing_grad = causal(mixing_grad).astype(bf16)
    half = BLOCK // 2
    mixing_term = jnp.concatenate([mixing_grad[:half], mixing_grad[half:]], axis=1)
    for x in range(n_x):
        made[n_all - 1, x] = mixing_term
    stores[n_all - 1].start()
    for i in range(parts):
        loads[i].wait()
        term = nn(held[i], joined_out[...]).astype(bf16)
        made[i * deep : (i + 1) * deep] = term.reshape(deep, n_x, rows, both)
        for z in range(i * deep, (i + 1) * deep):
            stores[z].start()
    for store in stores:
        store.wait()


def norm_terms(full_width, small, hidden_t, n_x, n_z):
    width, tokens = hidden_t.shape
    both = 2 * small[2].shape[1]
    rows = width // (n_x * n_z)
    parts = 4
    near, far = pl.BlockSpec(memory_space=pltpu.VMEM), pl.BlockSpec(memory_space=pl.ANY)
    return pl.pallas_call(
        functools.partial(norm_terms_body, full_width),
        out_shape=(like((tokens, both), bf16), stored((n_x, n_z + 1, rows, both), bf16)),
        in_specs=[near] * len(small) + [far],
        out_specs=(near, far),
        scratch_shapes=[
            pltpu.VMEM((parts, width // parts, tokens), bf16),
            pltpu.VMEM((n_z + 1, n_x, rows, both), bf16),
            pltpu.SemaphoreType.DMA((parts,)),
            pltpu.SemaphoreType.DMA((n_z + 1,)),
        ],
        compiler_params=pltpu.CompilerParams(vmem_limit_bytes=20 * 1024 * 1024),
        name="norm_terms",
    )(
        *[pltpu.with_memory_space_constraint(a, pltpu.VMEM) for a in small],
        pltpu.with_memory_space_constraint(hidden_t, pltpu.HBM),
    )


def pick_body(where, weight, mixing, mine_out, theirs_out, table_out, flipped_out):
    table = causal(mixing[0].astype(f32))
    table_out[...] = table.astype(bf16)
    flipped_out[...] = table.T.astype(bf16)
    n_x, _, rows, both = weight.shape
    half = n_x // 2
    for out, base, core in ((mine_out, 0, where[10]), (theirs_out, 5, 1 - where[10])):
        at = 0
        for step in (3, 1, 2):
            block = weight[:, pl.ds(where[base + step], 1)].reshape(n_x * rows, both)
            out[at : at + n_x * rows] = block
            at += n_x * rows
        for step in (4, 0):
            block = weight[pl.ds(core * half, half), pl.ds(where[base + step], 1)]
            out[at : at + half * rows] = block.reshape(half * rows, both)
            at += half * rows


def input_terms_body(joined, joined_far, mine, far, odd, two, four, own):
    def term(at, n):
        rows = slice(at, at + n)
        return nt(joined[...], mine[rows]) + nt(joined_far[...], far[rows])

    single, pair = own.shape[1], two.shape[1]
    odd[...] = term(0, 2 * pair).astype(bf16)
    four[...] = term(3 * pair, single).astype(bf16)
    two[...] = term(2 * pair, pair)
    own[...] = term(3 * pair + single, single)


def merge_body(where, two, odd, four, same_out, other_out, keep_out, send_out):
    half = four.shape[1]
    first = where[10] == 0
    both = two[...] + odd[:, : 2 * half].astype(f32)
    left, right = both[:, :half], both[:, half:]
    same_out[...] = (jnp.where(first, left, right) + four[...].astype(f32)).astype(bf16)
    other_out[...] = jnp.where(first, right, left).astype(bf16)
    left, right = odd[:, 2 * half : 3 * half], odd[:, 3 * half :]
    left, right = left.astype(f32), right.astype(f32)
    keep_out[...] = jnp.where(first, left, right).astype(bf16)
    send_out[...] = jnp.where(first, right, left).astype(bf16)


def total_body(own, same, other, keep, sent, out):
    total = own[...]
    for part in (same, other, keep, sent):
        total = total + part[...].astype(f32)
    out[...] = total.astype(bf16)


def regroup_body(arrived, out):
    n_z = out.shape[0]
    total = arrived[0].astype(f32)
    for x in range(1, arrived.shape[0]):
        total = total + arrived[x].astype(f32)
    total = total.astype(bf16)
    for z in range(n_z):
        out[z, 0] = total[z]
        out[z, 1] = total[n_z]


def finish_body(scale, arrived, content_out, gating_out, mixing_out):
    total = arrived[0].astype(f32)
    for z in range(1, arrived.shape[0]):
        total = total + arrived[z].astype(f32)
    total = total * scale
    half = content_out.shape[1]
    content_out[...] = total[0][:, :half]
    gating_out[...] = total[0][:, half:]
    mixing_out[0, : BLOCK // 2] = total[1][:, :half]
    mixing_out[0, BLOCK // 2 :] = total[1][:, half:]


def step(
    hidden_in, content_weight, gating_weight, norm_gain, mixing_weight, mixing_bias, out_grad
):
    tok_rows, width = hidden_in.shape
    shard_rows, local_width = content_weight.shape
    both = 2 * local_width
    n_z, n_x = lax.axis_size("sp_0"), lax.axis_size("sp_1")
    n_sp, n_dp = n_z * n_x, lax.axis_size(DP)
    ring = lax.axis_size("dp_0")
    full_width = local_width * n_dp
    out_cols = width // n_dp
    grad_scale = 1.0 / math.sqrt(tok_rows * n_sp)
    here, core = lax.axis_index("dp_0"), lax.axis_index("dp_1")
    side = 1 - 2 * core
    ahead = [(here + side * k + ring) % ring for k in range(5)]
    behind = [(here - side * k + ring) % ring for k in range(5)]
    where = jnp.stack(ahead + behind + [core]).astype(jnp.int32)
    gain = norm_gain[None, :]

    hidden_t = call(flip_body, stored((width, tok_rows), bf16))(hidden_in)
    shards = call(join_body, stored((n_z, shard_rows, both), bf16), cold=(0, 1))(
        content_weight, gating_weight
    )
    along_z = exchange(shards, "sp_0")
    spread = call(spread_body, like((n_x, n_z, shard_rows, both), bf16))(along_z)
    weight = exchange(spread, "sp_1")
    single, pair = (tok_rows, out_cols), (tok_rows, 2 * out_cols)
    wide_pair, picked = (tok_rows, 4 * out_cols), (width // 2, both)
    square = like((BLOCK, BLOCK), bf16)
    mine, theirs, table, flipped = call(
        pick_body, (like(picked, bf16), like(picked, bf16), square, square), scalars=True, cold=(2,)
    )(where, weight, mixing_weight)
    far = swapped(theirs)

    wide = (tok_rows, both)
    pre, sums = call(
        project_body, (like(wide, bf16), stored((n_dp, 4, tok_rows), f32))
    )(hidden_in, weight, mixing_weight, gain, out_grad)
    sums = exchange(sums, DP)
    small = (sums, pre, out_grad, table, flipped, mixing_bias, gain)
    joined, terms = norm_terms(full_width, small, hidden_t, n_x, n_z)

    joined_far = swapped(joined)
    along_x = exchange(terms, "sp_1")

    odd, two, four, own = call(
        input_terms_body,
        (like(wide_pair, bf16), like(pair, f32), like(single, bf16), like(single, f32)),
    )(joined, joined_far, mine, far)
    four = sent_apart(four, 2)
    odd = sent_apart(odd, 1)
    same, other, keep, send = call(merge_body, (like(single, bf16),) * 4, scalars=True)(
        where, two, odd, four
    )
    same = sent_apart(same, 2)
    other = sent_apart(other, 2, True)
    sent = swapped(send)

    regrouped = call(regroup_body, stored((n_z, 2, shard_rows, both), bf16))(along_x)
    arrived = exchange(regrouped, "sp_0")

    input_grad = call(total_body, outside(single, bf16))(own, same, other, keep, sent)

    content_grad, gating_grad, mixing_grad = call(
        functools.partial(finish_body, grad_scale),
        (
            outside((shard_rows, local_width), f32),
            outside((shard_rows, local_width), f32),
            outside(mixing_weight.shape, f32),
        ),
    )(arrived)
    return (input_grad, content_grad, gating_grad, mixing_grad)


def solution(mesh):
    split = Mesh(mesh.devices.reshape(8, 4, 8, 2), (*SP, *DP))
    in_specs = (
        P(SP, None),
        P(SP, DP),
        P(SP, DP),
        P(DP),
        P(DP, None, None),
        P(DP, None),
        P(SP, DP),
    )
    out_specs = (P(SP, DP), P(SP, DP), P(SP, DP), P(DP, None, None))
    return jax.shard_map(step, mesh=split, in_specs=in_specs, out_specs=out_specs, check_vma=False)
```

```python
import functools
import math

import jax
import jax.numpy as jnp
from jax import lax
from jax.experimental import pallas as pl
from jax.experimental.pallas import tpu as pltpu
from jax.sharding import Mesh
from jax.sharding import PartitionSpec as P


BLOCK = 128
SP = ("sp_0", "sp_1")
DP = ("dp_0", "dp_1")


norm_eps = 1e-05
f32, bf16 = jnp.float32, jnp.bfloat16


def exchange(array, axis):
    return lax.all_to_all(array, axis, split_axis=0, concat_axis=0, tiled=True)


def swapped(array):
    return lax.ppermute(array, "dp_1", [(0, 1), (1, 0)])


def sent_apart(array, step, cross=False):
    ring = lax.axis_size("dp_0")
    moves = []
    for y in range(ring):
        for core, there in ((0, (y + step) % ring), (1, (y - step) % ring)):
            moves.append((2 * y + core, 2 * there + (1 - core if cross else core)))
    return lax.ppermute(array, DP, moves)


def normal_below(values):
    return 0.5 * (1.0 + lax.erf(values * (1.0 / math.sqrt(2.0))))


def gelu_slope(values):
    density = jnp.exp(-0.5 * values * values) * (1.0 / math.sqrt(2.0 * math.pi))
    return normal_below(values) + values * density


def causal(weights):
    rows = lax.broadcasted_iota(jnp.int32, (BLOCK, BLOCK), 0)
    cols = lax.broadcasted_iota(jnp.int32, (BLOCK, BLOCK), 1)
    return jnp.where(cols <= rows, weights, jnp.zeros_like(weights))


PACKED = BLOCK // 4 + 8


def packed(grad):
    half = BLOCK // 2
    rows = lax.broadcasted_iota(jnp.int32, (half, BLOCK), 0)
    cols = lax.broadcasted_iota(jnp.int32, (half, BLOCK), 1)
    turned = pltpu.roll(grad.T, half, 1)[:half]
    body = grad[half:] + jnp.where(cols - half > rows, turned, 0.0)
    spine = jnp.sum(jnp.where(rows == cols, grad[:half], 0.0), axis=0, keepdims=True)
    spine = jnp.broadcast_to(spine, (8, BLOCK))
    body = jnp.concatenate([body[: half // 2], body[half // 2 :]], axis=1)
    return jnp.concatenate([body, jnp.concatenate([spine, spine], axis=1)], axis=0)


def unpacked(terms):
    half = BLOCK // 2
    rows = lax.broadcasted_iota(jnp.int32, (half, BLOCK), 0)
    cols = lax.broadcasted_iota(jnp.int32, (half, BLOCK), 1)
    body = terms[: half // 2]
    body = jnp.concatenate([body[:, :BLOCK], body[:, BLOCK:]], axis=0)
    spine = jnp.broadcast_to(terms[half // 2 : half // 2 + 1, :BLOCK], (half, BLOCK))
    above = jnp.where(cols - half > rows, body, 0.0)
    top = jnp.concatenate([above, jnp.zeros_like(above)], axis=0).T[half:]
    top = top + jnp.where(rows == cols, spine, 0.0)
    return top, jnp.where(cols - half <= rows, body, 0.0)


def nt(a, b, **kw):
    return lax.dot_general(a, b, (((1,), (1,)), ((), ())), preferred_element_type=f32, **kw)


def nn(a, b):
    return jnp.dot(a, b, preferred_element_type=f32)


def call(body, outs, scalars=False, cold=(), free=()):
    def run(*args):
        specs, operands = [], []
        for at, array in enumerate(args):
            if scalars and at == 0:
                specs.append(pl.BlockSpec(memory_space=pltpu.SMEM))
            elif at in free:
                specs.append(pl.BlockSpec())
            elif at in cold:
                specs.append(pl.BlockSpec())
                array = pltpu.with_memory_space_constraint(array, pltpu.HBM)
            else:
                specs.append(pl.BlockSpec(memory_space=pltpu.VMEM))
                array = pltpu.with_memory_space_constraint(array, pltpu.VMEM)
            operands.append(array)
        limit = pltpu.CompilerParams(vmem_limit_bytes=20 * 1024 * 1024)
        made = pl.pallas_call(body, out_shape=outs, in_specs=specs, compiler_params=limit)
        return made(*operands)

    return run


def like(shape, dtype):
    return pltpu.VMEM(shape, dtype)


def stored(shape, dtype):
    return pltpu.HBM(shape, dtype)


def outside(shape, dtype):
    return jax.ShapeDtypeStruct(shape, dtype)


def project_body(hidden, weight, mixing, gain, grad, pre_out, sums_out):
    n_x, n_z, rows, both = weight.shape
    slab = n_x * rows
    pre = None
    for z in range(n_z):
        term = nn(hidden[:, z * slab : (z + 1) * slab], weight[:, z].reshape(slab, both))
        pre = term if pre is None else pre + term
    pre = pre.astype(bf16)
    pre_out[...] = pre
    flipped = causal(mixing[0].astype(f32)).T.astype(bf16)
    gating, _, back, _ = branches(pre, grad[...], flipped, gain[...])
    lane = lax.broadcasted_iota(jnp.int32, gating.shape, 1)
    sums = jnp.zeros_like(gating)
    for at, values in enumerate((gating, gating * gating, back, back * gating)):
        sums = jnp.where(lane == at, jnp.sum(values, axis=1, keepdims=True), sums)
    sums = sums.T
    for peer in range(sums_out.shape[0]):
        sums_out[peer] = sums[:4]


def branches(pre, grad, flipped, gain):
    width = grad.shape[1]
    pre_content = pre[:, :width].astype(f32)
    pre_gating = pre[:, width:].astype(f32)
    gating = pre_gating * normal_below(pre_gating)
    content = pre_content * normal_below(pre_content)
    mixed_grad = (grad.astype(f32) * content).astype(bf16)
    pieces = []
    for at in range(0, mixed_grad.shape[0], BLOCK):
        pieces.append(nn(flipped, mixed_grad[at : at + BLOCK]) * gain)
    return gating, mixed_grad, jnp.concatenate(pieces, axis=0), (pre_content, pre_gating)


def join_body(content, gating, out):
    both = jnp.concatenate([content[...], gating[...]], axis=1)
    for peer in range(out.shape[0]):
        out[peer] = both


def spread_body(arrived, out):
    for peer in range(out.shape[0]):
        out[peer] = arrived[...]


def flip_body(array, out):
    step = 256
    for at in range(0, array.shape[1], step):
        out[at : at + step] = array[:, at : at + step].T


def norm_terms_body(full_width, sums, pre, grad, table, flipped, bias, gain, hidden_t, joined_out, out, held, made, mixed_made, come, gone):
    deep, n_x, rows, both = made.shape[1:]
    parts, chunk, _ = held.shape
    n_z = parts * deep
    loads = [
        pltpu.make_async_copy(hidden_t.at[pl.ds(i * chunk, chunk)], held.at[i], come.at[i])
        for i in range(parts)
    ]
    stores = [
        pltpu.make_async_copy(
            made.at[z // deep, z % deep], out.at[:, pl.ds(z * rows, rows)], gone.at[z]
        )
        for z in range(n_z)
    ]
    stores.append(
        pltpu.make_async_copy(mixed_made, out.at[:, pl.ds(n_z * rows, PACKED)], gone.at[n_z])
    )
    for load in loads:
        load.start()
    gating, mixed_grad, back, (pre_content, pre_gating) = branches(
        pre[...], grad[...], flipped[...], gain[...]
    )
    content_slope = grad[...].astype(f32) * gelu_slope(pre_content)
    total = jnp.sum(sums[...], axis=0) * (1.0 / full_width)
    row_mean = total[0:1]
    row_var = total[1:2] - row_mean * row_mean
    inv_std = lax.rsqrt(row_var + norm_eps)
    first = total[2:3]
    second = inv_std * (total[3:4] - row_mean * first)
    columns = jnp.concatenate([row_mean, inv_std, first, second] * 2, axis=0).T
    row_mean, inv_std, first, second = [columns[:, i : i + 1] for i in range(4)]
    centred = (gating - row_mean) * inv_std
    normed = (centred * gain[...]).astype(bf16)
    shift = jnp.broadcast_to(bias[...], (8, BLOCK)).T[:, 0:1]
    width = normed.shape[1]
    mixing_grad = None
    for at in range(0, normed.shape[0], BLOCK):
        block = slice(at, at + BLOCK)
        mixed = nn(table[...], normed[block]) + shift
        joined_out[block, :width] = (mixed * content_slope[block]).astype(bf16)
        term = nt(mixed_grad[block], normed[block])
        mixing_grad = term if mixing_grad is None else mixing_grad + term
    gating_back = inv_std * (back - first - centred * second)
    joined_out[:, width:] = (gating_back * gelu_slope(pre_gating)).astype(bf16)
    mixing_term = packed(causal(mixing_grad)).astype(bf16)
    for x in range(n_x):
        mixed_made[x] = mixing_term
    stores[n_z].start()
    for i in range(parts):
        loads[i].wait()
        term = nn(held[i], joined_out[...]).astype(bf16)
        made[i] = term.reshape(deep, n_x, rows, both)
        for z in range(i * deep, (i + 1) * deep):
            stores[z].start()
    for store in stores:
        store.wait()


def norm_terms(full_width, small, hidden_t, n_x, n_z):
    width, tokens = hidden_t.shape
    both = 2 * small[2].shape[1]
    rows = width // (n_x * n_z)
    parts = 4
    near, far = pl.BlockSpec(memory_space=pltpu.VMEM), pl.BlockSpec(memory_space=pl.ANY)
    return pl.pallas_call(
        functools.partial(norm_terms_body, full_width),
        out_shape=(like((tokens, both), bf16), stored((n_x, n_z * rows + PACKED, both), bf16)),
        in_specs=[near] * len(small) + [far],
        out_specs=(near, far),
        scratch_shapes=[
            pltpu.VMEM((parts, width // parts, tokens), bf16),
            pltpu.VMEM((parts, n_z // parts, n_x, rows, both), bf16),
            pltpu.VMEM((n_x, PACKED, both), bf16),
            pltpu.SemaphoreType.DMA((parts,)),
            pltpu.SemaphoreType.DMA((n_z + 1,)),
        ],
        compiler_params=pltpu.CompilerParams(vmem_limit_bytes=20 * 1024 * 1024),
        name="norm_terms",
    )(
        *[pltpu.with_memory_space_constraint(a, pltpu.VMEM) for a in small],
        pltpu.with_memory_space_constraint(hidden_t, pltpu.HBM),
    )


def pick_body(where, weight, mixing, mine_out, theirs_out, table_out, flipped_out):
    table = causal(mixing[0].astype(f32))
    table_out[...] = table.astype(bf16)
    flipped_out[...] = table.T.astype(bf16)
    n_x, _, rows, both = weight.shape
    half = n_x // 2
    for out, base, core in ((mine_out, 0, where[10]), (theirs_out, 5, 1 - where[10])):
        at = 0
        for step in (3, 1, 2):
            block = weight[:, pl.ds(where[base + step], 1)].reshape(n_x * rows, both)
            out[at : at + n_x * rows] = block
            at += n_x * rows
        for step in (4, 0):
            block = weight[pl.ds(core * half, half), pl.ds(where[base + step], 1)]
            out[at : at + half * rows] = block.reshape(half * rows, both)
            at += half * rows


def input_terms_body(joined, joined_far, mine, far, odd, two, four, own):
    def term(at, n):
        rows = slice(at, at + n)
        return nt(joined[...], mine[rows]) + nt(joined_far[...], far[rows])

    single, pair = own.shape[1], two.shape[1]
    odd[...] = term(0, 2 * pair).astype(bf16)
    four[...] = term(3 * pair, single).astype(bf16)
    two[...] = term(2 * pair, pair)
    own[...] = term(3 * pair + single, single)


def merge_body(where, two, odd, four, same_out, other_out, keep_out, send_out):
    half = four.shape[1]
    first = where[10] == 0
    both = two[...] + odd[:, : 2 * half].astype(f32)
    left, right = both[:, :half], both[:, half:]
    same_out[...] = (jnp.where(first, left, right) + four[...].astype(f32)).astype(bf16)
    other_out[...] = jnp.where(first, right, left).astype(bf16)
    left, right = odd[:, 2 * half : 3 * half], odd[:, 3 * half :]
    left, right = left.astype(f32), right.astype(f32)
    keep_out[...] = jnp.where(first, left, right).astype(bf16)
    send_out[...] = jnp.where(first, right, left).astype(bf16)


def total_body(own, same, other, keep, sent, out):
    total = own[...]
    for part in (same, other, keep, sent):
        total = total + part[...].astype(f32)
    out[...] = total.astype(bf16)


def regroup_body(arrived, out):
    n_z = out.shape[0]
    rows = out.shape[1] - PACKED
    total = arrived[0].astype(f32)
    for x in range(1, arrived.shape[0]):
        total = total + arrived[x].astype(f32)
    total = total.astype(bf16)
    for z in range(n_z):
        out[z, :rows] = total[z * rows : (z + 1) * rows]
        out[z, rows:] = total[n_z * rows :]


def finish_body(scale, arrived, content_out, gating_out, mixing_out):
    total = arrived[0].astype(f32)
    for z in range(1, arrived.shape[0]):
        total = total + arrived[z].astype(f32)
    total = total * scale
    rows, half = content_out.shape
    content_out[...] = total[:rows, :half]
    gating_out[...] = total[:rows, half:]
    top, bottom = unpacked(total[rows:])
    mixing_out[0, : BLOCK // 2] = top
    mixing_out[0, BLOCK // 2 :] = bottom


def step(
    hidden_in, content_weight, gating_weight, norm_gain, mixing_weight, mixing_bias, out_grad
):
    tok_rows, width = hidden_in.shape
    shard_rows, local_width = content_weight.shape
    both = 2 * local_width
    n_z, n_x = lax.axis_size("sp_0"), lax.axis_size("sp_1")
    n_sp, n_dp = n_z * n_x, lax.axis_size(DP)
    ring = lax.axis_size("dp_0")
    full_width = local_width * n_dp
    out_cols = width // n_dp
    grad_scale = 1.0 / math.sqrt(tok_rows * n_sp)
    here, core = lax.axis_index("dp_0"), lax.axis_index("dp_1")
    side = 1 - 2 * core
    ahead = [(here + side * k + ring) % ring for k in range(5)]
    behind = [(here - side * k + ring) % ring for k in range(5)]
    where = jnp.stack(ahead + behind + [core]).astype(jnp.int32)
    gain = norm_gain[None, :]

    hidden_t = call(flip_body, stored((width, tok_rows), bf16))(hidden_in)
    shards = call(join_body, stored((n_z, shard_rows, both), bf16), cold=(0, 1))(
        content_weight, gating_weight
    )
    along_z = exchange(shards, "sp_0")
    spread = call(spread_body, like((n_x, n_z, shard_rows, both), bf16))(along_z)
    weight = exchange(spread, "sp_1")
    single, pair = (tok_rows, out_cols), (tok_rows, 2 * out_cols)
    wide_pair, picked = (tok_rows, 4 * out_cols), (width // 2, both)
    square = like((BLOCK, BLOCK), bf16)
    mine, theirs, table, flipped = call(
        pick_body, (like(picked, bf16), like(picked, bf16), square, square), scalars=True, cold=(2,)
    )(where, weight, mixing_weight)
    far = swapped(theirs)

    wide = (tok_rows, both)
    pre, sums = call(
        project_body, (like(wide, bf16), stored((n_dp, 4, tok_rows), f32))
    )(hidden_in, weight, mixing_weight, gain, out_grad)
    sums = exchange(sums, DP)
    small = (sums, pre, out_grad, table, flipped, mixing_bias, gain)
    joined, terms = norm_terms(full_width, small, hidden_t, n_x, n_z)

    joined_far = swapped(joined)
    along_x = exchange(terms, "sp_1")

    odd, two, four, own = call(
        input_terms_body,
        (like(wide_pair, bf16), like(pair, f32), like(single, bf16), like(single, f32)),
    )(joined, joined_far, mine, far)
    four = sent_apart(four, 2)
    odd = sent_apart(odd, 1)
    same, other, keep, send = call(merge_body, (like(single, bf16),) * 4, scalars=True)(
        where, two, odd, four
    )
    same = sent_apart(same, 2)
    other = sent_apart(other, 2, True)
    sent = swapped(send)

    regrouped = call(regroup_body, stored((n_z, shard_rows + PACKED, both), bf16))(along_x)
    arrived = exchange(regrouped, "sp_0")

    input_grad = call(total_body, outside(single, bf16))(own, same, other, keep, sent)

    content_grad, gating_grad, mixing_grad = call(
        functools.partial(finish_body, grad_scale),
        (
            outside((shard_rows, local_width), f32),
            outside((shard_rows, local_width), f32),
            outside(mixing_weight.shape, f32),
        ),
    )(arrived)
    return (input_grad, content_grad, gating_grad, mixing_grad)


def solution(mesh):
    split = Mesh(mesh.devices.reshape(8, 4, 8, 2), (*SP, *DP))
    in_specs = (
        P(SP, None),
        P(SP, DP),
        P(SP, DP),
        P(DP),
        P(DP, None, None),
        P(DP, None),
        P(SP, DP),
    )
    out_specs = (P(SP, DP), P(SP, DP), P(SP, DP), P(DP, None, None))
    return jax.shard_map(step, mesh=split, in_specs=in_specs, out_specs=out_specs, check_vma=False)
```

```python
import functools
import math

import jax
import jax.numpy as jnp
from jax import lax
from jax.experimental import pallas as pl
from jax.experimental.pallas import tpu as pltpu
from jax.sharding import Mesh
from jax.sharding import PartitionSpec as P


BLOCK = 128
SP = ("sp_0", "sp_1")
DP = ("dp_0", "dp_1")


norm_eps = 1e-05
f32, bf16 = jnp.float32, jnp.bfloat16


def exchange(array, axis):
    return lax.all_to_all(array, axis, split_axis=0, concat_axis=0, tiled=True)


def swapped(array):
    return lax.ppermute(array, "dp_1", [(0, 1), (1, 0)])


def sent_apart(array, step, cross=False):
    ring = lax.axis_size("dp_0")
    moves = []
    for y in range(ring):
        for core, there in ((0, (y + step) % ring), (1, (y - step) % ring)):
            moves.append((2 * y + core, 2 * there + (1 - core if cross else core)))
    return lax.ppermute(array, DP, moves)


def normal_below(values):
    return 0.5 * (1.0 + lax.erf(values * (1.0 / math.sqrt(2.0))))


def gelu_slope(values):
    density = jnp.exp(-0.5 * values * values) * (1.0 / math.sqrt(2.0 * math.pi))
    return normal_below(values) + values * density


def causal(weights):
    rows = lax.broadcasted_iota(jnp.int32, (BLOCK, BLOCK), 0)
    cols = lax.broadcasted_iota(jnp.int32, (BLOCK, BLOCK), 1)
    return jnp.where(cols <= rows, weights, jnp.zeros_like(weights))


PACKED = BLOCK // 4 + 8


def packed(grad):
    half = BLOCK // 2
    rows = lax.broadcasted_iota(jnp.int32, (half, BLOCK), 0)
    cols = lax.broadcasted_iota(jnp.int32, (half, BLOCK), 1)
    turned = pltpu.roll(grad.T, half, 1)[:half]
    body = grad[half:] + jnp.where(cols - half > rows, turned, 0.0)
    spine = jnp.sum(jnp.where(rows == cols, grad[:half], 0.0), axis=0, keepdims=True)
    spine = jnp.broadcast_to(spine, (8, BLOCK))
    body = jnp.concatenate([body[: half // 2], body[half // 2 :]], axis=1)
    return jnp.concatenate([body, jnp.concatenate([spine, spine], axis=1)], axis=0)


def unpacked(terms):
    half = BLOCK // 2
    rows = lax.broadcasted_iota(jnp.int32, (half, BLOCK), 0)
    cols = lax.broadcasted_iota(jnp.int32, (half, BLOCK), 1)
    body = terms[: half // 2]
    body = jnp.concatenate([body[:, :BLOCK], body[:, BLOCK:]], axis=0)
    spine = jnp.broadcast_to(terms[half // 2 : half // 2 + 1, :BLOCK], (half, BLOCK))
    above = jnp.where(cols - half > rows, body, 0.0)
    top = jnp.concatenate([above, jnp.zeros_like(above)], axis=0).T[half:]
    top = top + jnp.where(rows == cols, spine, 0.0)
    return top, jnp.where(cols - half <= rows, body, 0.0)


def nt(a, b, **kw):
    return lax.dot_general(a, b, (((1,), (1,)), ((), ())), preferred_element_type=f32, **kw)


def nn(a, b):
    return jnp.dot(a, b, preferred_element_type=f32)


def call(body, outs, scalars=False, cold=(), free=()):
    def run(*args):
        specs, operands = [], []
        for at, array in enumerate(args):
            if scalars and at == 0:
                specs.append(pl.BlockSpec(memory_space=pltpu.SMEM))
            elif at in free:
                specs.append(pl.BlockSpec())
            elif at in cold:
                specs.append(pl.BlockSpec())
                array = pltpu.with_memory_space_constraint(array, pltpu.HBM)
            else:
                specs.append(pl.BlockSpec(memory_space=pltpu.VMEM))
                array = pltpu.with_memory_space_constraint(array, pltpu.VMEM)
            operands.append(array)
        limit = pltpu.CompilerParams(vmem_limit_bytes=20 * 1024 * 1024)
        made = pl.pallas_call(body, out_shape=outs, in_specs=specs, compiler_params=limit)
        return made(*operands)

    return run


def like(shape, dtype):
    return pltpu.VMEM(shape, dtype)


def stored(shape, dtype):
    return pltpu.HBM(shape, dtype)


def outside(shape, dtype):
    return jax.ShapeDtypeStruct(shape, dtype)


def project_body(hidden, weight, mixing, gain, grad, pre_out, sums_out):
    n_x, n_z, rows, both = weight.shape
    slab = n_x * rows
    pre = None
    for z in range(n_z):
        term = nn(hidden[:, z * slab : (z + 1) * slab], weight[:, z].reshape(slab, both))
        pre = term if pre is None else pre + term
    pre = pre.astype(bf16)
    pre_out[...] = pre
    flipped = causal(mixing[0].astype(f32)).T.astype(bf16)
    gating, _, back, _ = branches(pre, grad[...], flipped, gain[...])
    lane = lax.broadcasted_iota(jnp.int32, gating.shape, 1)
    sums = jnp.zeros_like(gating)
    for at, values in enumerate((gating, gating * gating, back, back * gating)):
        sums = jnp.where(lane == at, jnp.sum(values, axis=1, keepdims=True), sums)
    sums = sums.T
    for peer in range(sums_out.shape[0]):
        sums_out[peer] = sums[:4]


def branches(pre, grad, flipped, gain):
    width = grad.shape[1]
    pre_content = pre[:, :width].astype(f32)
    pre_gating = pre[:, width:].astype(f32)
    gating = pre_gating * normal_below(pre_gating)
    content = pre_content * normal_below(pre_content)
    mixed_grad = (grad.astype(f32) * content).astype(bf16)
    pieces = []
    for at in range(0, mixed_grad.shape[0], BLOCK):
        pieces.append(nn(flipped, mixed_grad[at : at + BLOCK]) * gain)
    return gating, mixed_grad, jnp.concatenate(pieces, axis=0), (pre_content, pre_gating)


def join_body(content, gating, out):
    both = jnp.concatenate([content[...], gating[...]], axis=1)
    for peer in range(out.shape[0]):
        out[peer] = both


def spread_body(arrived, out):
    for peer in range(out.shape[0]):
        out[peer] = arrived[...]


def flip_body(array, top, bottom):
    step, half = 256, top.shape[0]
    for at in range(0, half, step):
        top[at : at + step] = array[:, at : at + step].T
        bottom[at : at + step] = array[:, half + at : half + at + step].T


def norm_terms_body(full_width, sums, pre, grad, table, flipped, bias, gain, top, bottom, joined_out, out, held, made, mixed_made, come, gone):
    deep, n_x, rows, both = made.shape[1:]
    later, chunk, _ = held.shape
    parts = made.shape[0]
    ready = parts - later
    n_z = parts * deep
    loads = [
        pltpu.make_async_copy(bottom.at[pl.ds(i * chunk, chunk)], held.at[i], come.at[i])
        for i in range(later)
    ]
    stores = [
        pltpu.make_async_copy(
            made.at[z // deep, z % deep], out.at[:, pl.ds(z * rows, rows)], gone.at[z]
        )
        for z in range(n_z)
    ]
    stores.append(
        pltpu.make_async_copy(mixed_made, out.at[:, pl.ds(n_z * rows, PACKED)], gone.at[n_z])
    )
    for load in loads:
        load.start()
    gating, mixed_grad, back, (pre_content, pre_gating) = branches(
        pre[...], grad[...], flipped[...], gain[...]
    )
    content_slope = grad[...].astype(f32) * gelu_slope(pre_content)
    total = jnp.sum(sums[...], axis=0) * (1.0 / full_width)
    row_mean = total[0:1]
    row_var = total[1:2] - row_mean * row_mean
    inv_std = lax.rsqrt(row_var + norm_eps)
    first = total[2:3]
    second = inv_std * (total[3:4] - row_mean * first)
    columns = jnp.concatenate([row_mean, inv_std, first, second] * 2, axis=0).T
    row_mean, inv_std, first, second = [columns[:, i : i + 1] for i in range(4)]
    centred = (gating - row_mean) * inv_std
    normed = (centred * gain[...]).astype(bf16)
    shift = jnp.broadcast_to(bias[...], (8, BLOCK)).T[:, 0:1]
    width = normed.shape[1]
    mixing_grad = None
    for at in range(0, normed.shape[0], BLOCK):
        block = slice(at, at + BLOCK)
        mixed = nn(table[...], normed[block]) + shift
        joined_out[block, :width] = (mixed * content_slope[block]).astype(bf16)
        term = nt(mixed_grad[block], normed[block])
        mixing_grad = term if mixing_grad is None else mixing_grad + term
    gating_back = inv_std * (back - first - centred * second)
    joined_out[:, width:] = (gating_back * gelu_slope(pre_gating)).astype(bf16)
    mixing_term = packed(causal(mixing_grad)).astype(bf16)
    for x in range(n_x):
        mixed_made[x] = mixing_term
    stores[n_z].start()
    for i in range(parts):
        if i < ready:
            slab = top[i * chunk : (i + 1) * chunk]
        else:
            loads[i - ready].wait()
            slab = held[i - ready]
        term = nn(slab, joined_out[...]).astype(bf16)
        made[i] = term.reshape(deep, n_x, rows, both)
        for z in range(i * deep, (i + 1) * deep):
            stores[z].start()
    for store in stores:
        store.wait()


def norm_terms(full_width, small, top, bottom, n_x, n_z):
    width, tokens = 2 * top.shape[0], top.shape[1]
    both = 2 * small[2].shape[1]
    rows = width // (n_x * n_z)
    parts = 4
    near, far = pl.BlockSpec(memory_space=pltpu.VMEM), pl.BlockSpec(memory_space=pl.ANY)
    return pl.pallas_call(
        functools.partial(norm_terms_body, full_width),
        out_shape=(like((tokens, both), bf16), stored((n_x, n_z * rows + PACKED, both), bf16)),
        in_specs=[near] * (len(small) + 1) + [far],
        out_specs=(near, far),
        scratch_shapes=[
            pltpu.VMEM((parts // 2, width // parts, tokens), bf16),
            pltpu.VMEM((parts, n_z // parts, n_x, rows, both), bf16),
            pltpu.VMEM((n_x, PACKED, both), bf16),
            pltpu.SemaphoreType.DMA((parts // 2,)),
            pltpu.SemaphoreType.DMA((n_z + 1,)),
        ],
        compiler_params=pltpu.CompilerParams(vmem_limit_bytes=20 * 1024 * 1024),
        name="norm_terms",
    )(
        *[pltpu.with_memory_space_constraint(a, pltpu.VMEM) for a in (*small, top)],
        pltpu.with_memory_space_constraint(bottom, pltpu.HBM),
    )


def pick_body(where, weight, mixing, mine_out, theirs_out, table_out, flipped_out):
    table = causal(mixing[0].astype(f32))
    table_out[...] = table.astype(bf16)
    flipped_out[...] = table.T.astype(bf16)
    n_x, _, rows, both = weight.shape
    half = n_x // 2
    for out, base, core in ((mine_out, 0, where[10]), (theirs_out, 5, 1 - where[10])):
        at = 0
        for step in (3, 1, 2):
            block = weight[:, pl.ds(where[base + step], 1)].reshape(n_x * rows, both)
            out[at : at + n_x * rows] = block
            at += n_x * rows
        for step in (4, 0):
            block = weight[pl.ds(core * half, half), pl.ds(where[base + step], 1)]
            out[at : at + half * rows] = block.reshape(half * rows, both)
            at += half * rows


def input_terms_body(joined, joined_far, mine, far, odd, two, four, own):
    def term(at, n):
        rows = slice(at, at + n)
        return nt(joined[...], mine[rows]) + nt(joined_far[...], far[rows])

    single, pair = own.shape[1], two.shape[1]
    odd[...] = term(0, 2 * pair).astype(bf16)
    four[...] = term(3 * pair, single).astype(bf16)
    two[...] = term(2 * pair, pair)
    own[...] = term(3 * pair + single, single)


def merge_body(where, two, odd, four, same_out, other_out, keep_out, send_out):
    half = four.shape[1]
    first = where[10] == 0
    both = two[...] + odd[:, : 2 * half].astype(f32)
    left, right = both[:, :half], both[:, half:]
    same_out[...] = (jnp.where(first, left, right) + four[...].astype(f32)).astype(bf16)
    other_out[...] = jnp.where(first, right, left).astype(bf16)
    left, right = odd[:, 2 * half : 3 * half], odd[:, 3 * half :]
    left, right = left.astype(f32), right.astype(f32)
    keep_out[...] = jnp.where(first, left, right).astype(bf16)
    send_out[...] = jnp.where(first, right, left).astype(bf16)


def total_body(own, same, other, keep, sent, out):
    total = own[...]
    for part in (same, other, keep, sent):
        total = total + part[...].astype(f32)
    out[...] = total.astype(bf16)


def regroup_body(arrived, out):
    n_z = out.shape[0]
    rows = out.shape[1] - PACKED
    total = arrived[0].astype(f32)
    for x in range(1, arrived.shape[0]):
        total = total + arrived[x].astype(f32)
    total = total.astype(bf16)
    for z in range(n_z):
        out[z, :rows] = total[z * rows : (z + 1) * rows]
        out[z, rows:] = total[n_z * rows :]


def finish_body(scale, arrived, content_out, gating_out, mixing_out):
    total = arrived[0].astype(f32)
    for z in range(1, arrived.shape[0]):
        total = total + arrived[z].astype(f32)
    total = total * scale
    rows, half = content_out.shape
    content_out[...] = total[:rows, :half]
    gating_out[...] = total[:rows, half:]
    top, bottom = unpacked(total[rows:])
    mixing_out[0, : BLOCK // 2] = top
    mixing_out[0, BLOCK // 2 :] = bottom


def step(
    hidden_in, content_weight, gating_weight, norm_gain, mixing_weight, mixing_bias, out_grad
):
    tok_rows, width = hidden_in.shape
    shard_rows, local_width = content_weight.shape
    both = 2 * local_width
    n_z, n_x = lax.axis_size("sp_0"), lax.axis_size("sp_1")
    n_sp, n_dp = n_z * n_x, lax.axis_size(DP)
    ring = lax.axis_size("dp_0")
    full_width = local_width * n_dp
    out_cols = width // n_dp
    grad_scale = 1.0 / math.sqrt(tok_rows * n_sp)
    here, core = lax.axis_index("dp_0"), lax.axis_index("dp_1")
    side = 1 - 2 * core
    ahead = [(here + side * k + ring) % ring for k in range(5)]
    behind = [(here - side * k + ring) % ring for k in range(5)]
    where = jnp.stack(ahead + behind + [core]).astype(jnp.int32)
    gain = norm_gain[None, :]

    half = (width // 2, tok_rows)
    top, bottom = call(flip_body, (like(half, bf16), stored(half, bf16)))(hidden_in)
    shards = call(join_body, stored((n_z, shard_rows, both), bf16), cold=(0, 1))(
        content_weight, gating_weight
    )
    along_z = exchange(shards, "sp_0")
    spread = call(spread_body, like((n_x, n_z, shard_rows, both), bf16))(along_z)
    weight = exchange(spread, "sp_1")
    single, pair = (tok_rows, out_cols), (tok_rows, 2 * out_cols)
    wide_pair, picked = (tok_rows, 4 * out_cols), (width // 2, both)
    square = like((BLOCK, BLOCK), bf16)
    mine, theirs, table, flipped = call(
        pick_body,
        (stored(picked, bf16), stored(picked, bf16), square, square),
        scalars=True,
        cold=(2,),
    )(where, weight, mixing_weight)
    far = swapped(theirs)

    wide = (tok_rows, both)
    pre, sums = call(
        project_body, (like(wide, bf16), stored((n_dp, 4, tok_rows), f32))
    )(hidden_in, weight, mixing_weight, gain, out_grad)
    sums = exchange(sums, DP)
    small = (sums, pre, out_grad, table, flipped, mixing_bias, gain)
    joined, terms = norm_terms(full_width, small, top, bottom, n_x, n_z)

    joined_far = swapped(joined)
    along_x = exchange(terms, "sp_1")

    odd, two, four, own = call(
        input_terms_body,
        (like(wide_pair, bf16), like(pair, f32), like(single, bf16), like(single, f32)),
        cold=(2,),
    )(joined, joined_far, mine, far)
    four = sent_apart(four, 2)
    odd = sent_apart(odd, 1)
    same, other, keep, send = call(merge_body, (like(single, bf16),) * 4, scalars=True)(
        where, two, odd, four
    )
    same = sent_apart(same, 2)
    other = sent_apart(other, 2, True)
    sent = swapped(send)

    regrouped = call(regroup_body, stored((n_z, shard_rows + PACKED, both), bf16))(along_x)
    arrived = exchange(regrouped, "sp_0")

    input_grad = call(total_body, outside(single, bf16))(own, same, other, keep, sent)

    content_grad, gating_grad, mixing_grad = call(
        functools.partial(finish_body, grad_scale),
        (
            outside((shard_rows, local_width), f32),
            outside((shard_rows, local_width), f32),
            outside(mixing_weight.shape, f32),
        ),
    )(arrived)
    return (input_grad, content_grad, gating_grad, mixing_grad)


def solution(mesh):
    split = Mesh(mesh.devices.reshape(8, 4, 8, 2), (*SP, *DP))
    in_specs = (
        P(SP, None),
        P(SP, DP),
        P(SP, DP),
        P(DP),
        P(DP, None, None),
        P(DP, None),
        P(SP, DP),
    )
    out_specs = (P(SP, DP), P(SP, DP), P(SP, DP), P(DP, None, None))
    return jax.shard_map(step, mesh=split, in_specs=in_specs, out_specs=out_specs, check_vma=False)
```

```python
import functools
import math

import jax
import jax.numpy as jnp
from jax import lax
from jax.experimental import pallas as pl
from jax.experimental.pallas import tpu as pltpu
from jax.sharding import Mesh
from jax.sharding import PartitionSpec as P


BLOCK = 128
SP = ("sp_0", "sp_1")
DP = ("dp_0", "dp_1")


norm_eps = 1e-05
f32, bf16 = jnp.float32, jnp.bfloat16


def exchange(array, axis):
    return lax.all_to_all(array, axis, split_axis=0, concat_axis=0, tiled=True)


def swapped(array):
    return lax.ppermute(array, "dp_1", [(0, 1), (1, 0)])


def sent_apart(array, step, cross=False):
    ring = lax.axis_size("dp_0")
    moves = []
    for y in range(ring):
        for core, there in ((0, (y + step) % ring), (1, (y - step) % ring)):
            moves.append((2 * y + core, 2 * there + (1 - core if cross else core)))
    return lax.ppermute(array, DP, moves)


def normal_below(values):
    return 0.5 * (1.0 + lax.erf(values * (1.0 / math.sqrt(2.0))))


def gelu_slope(values):
    density = jnp.exp(-0.5 * values * values) * (1.0 / math.sqrt(2.0 * math.pi))
    return normal_below(values) + values * density


def causal(weights):
    rows = lax.broadcasted_iota(jnp.int32, (BLOCK, BLOCK), 0)
    cols = lax.broadcasted_iota(jnp.int32, (BLOCK, BLOCK), 1)
    return jnp.where(cols <= rows, weights, jnp.zeros_like(weights))


PACKED = BLOCK // 4 + 8


def packed(grad):
    half = BLOCK // 2
    rows = lax.broadcasted_iota(jnp.int32, (half, BLOCK), 0)
    cols = lax.broadcasted_iota(jnp.int32, (half, BLOCK), 1)
    turned = pltpu.roll(grad.T, half, 1)[:half]
    body = grad[half:] + jnp.where(cols - half > rows, turned, 0.0)
    spine = jnp.sum(jnp.where(rows == cols, grad[:half], 0.0), axis=0, keepdims=True)
    spine = jnp.broadcast_to(spine, (8, BLOCK))
    body = jnp.concatenate([body[: half // 2], body[half // 2 :]], axis=1)
    return jnp.concatenate([body, jnp.concatenate([spine, spine], axis=1)], axis=0)


def unpacked(terms):
    half = BLOCK // 2
    rows = lax.broadcasted_iota(jnp.int32, (half, BLOCK), 0)
    cols = lax.broadcasted_iota(jnp.int32, (half, BLOCK), 1)
    body = terms[: half // 2]
    body = jnp.concatenate([body[:, :BLOCK], body[:, BLOCK:]], axis=0)
    spine = jnp.broadcast_to(terms[half // 2 : half // 2 + 1, :BLOCK], (half, BLOCK))
    above = jnp.where(cols - half > rows, body, 0.0)
    top = jnp.concatenate([above, jnp.zeros_like(above)], axis=0).T[half:]
    top = top + jnp.where(rows == cols, spine, 0.0)
    return top, jnp.where(cols - half <= rows, body, 0.0)


def nt(a, b, **kw):
    return lax.dot_general(a, b, (((1,), (1,)), ((), ())), preferred_element_type=f32, **kw)


def nn(a, b):
    return jnp.dot(a, b, preferred_element_type=f32)


def call(body, outs, scalars=False, cold=(), free=()):
    def run(*args):
        specs, operands = [], []
        for at, array in enumerate(args):
            if scalars and at == 0:
                specs.append(pl.BlockSpec(memory_space=pltpu.SMEM))
            elif at in free:
                specs.append(pl.BlockSpec())
            elif at in cold:
                specs.append(pl.BlockSpec())
                array = pltpu.with_memory_space_constraint(array, pltpu.HBM)
            else:
                specs.append(pl.BlockSpec(memory_space=pltpu.VMEM))
                array = pltpu.with_memory_space_constraint(array, pltpu.VMEM)
            operands.append(array)
        limit = pltpu.CompilerParams(vmem_limit_bytes=20 * 1024 * 1024)
        made = pl.pallas_call(body, out_shape=outs, in_specs=specs, compiler_params=limit)
        return made(*operands)

    return run


def like(shape, dtype):
    return pltpu.VMEM(shape, dtype)


def stored(shape, dtype):
    return pltpu.HBM(shape, dtype)


def outside(shape, dtype):
    return jax.ShapeDtypeStruct(shape, dtype)


def project_body(hidden, weight, mixing, gain, grad, pre_out, sums_out):
    n_x, n_z, rows, both = weight.shape
    slab = n_x * rows
    pre = None
    for z in range(n_z):
        term = nn(hidden[:, z * slab : (z + 1) * slab], weight[:, z].reshape(slab, both))
        pre = term if pre is None else pre + term
    pre = pre.astype(bf16)
    pre_out[...] = pre
    flipped = causal(mixing[0].astype(f32)).T.astype(bf16)
    gating, _, back, _ = branches(pre, grad[...], flipped, gain[...])
    lane = lax.broadcasted_iota(jnp.int32, gating.shape, 1)
    sums = jnp.zeros_like(gating)
    for at, values in enumerate((gating, gating * gating, back, back * gating)):
        sums = jnp.where(lane == at, jnp.sum(values, axis=1, keepdims=True), sums)
    sums = sums.T
    for peer in range(sums_out.shape[0]):
        sums_out[peer] = sums[:4]


def branches(pre, grad, flipped, gain):
    width = grad.shape[1]
    pre_content = pre[:, :width].astype(f32)
    pre_gating = pre[:, width:].astype(f32)
    gating = pre_gating * normal_below(pre_gating)
    content = pre_content * normal_below(pre_content)
    mixed_grad = (grad.astype(f32) * content).astype(bf16)
    pieces = []
    for at in range(0, mixed_grad.shape[0], BLOCK):
        pieces.append(nn(flipped, mixed_grad[at : at + BLOCK]) * gain)
    return gating, mixed_grad, jnp.concatenate(pieces, axis=0), (pre_content, pre_gating)


def join_body(content, gating, out):
    both = jnp.concatenate([content[...], gating[...]], axis=1)
    for peer in range(out.shape[0]):
        out[peer] = both


def spread_body(arrived, out):
    for peer in range(out.shape[0]):
        out[peer] = arrived[...]


def flip_body(array, top, bottom):
    step, half = 256, top.shape[0]
    for at in range(0, half, step):
        top[at : at + step] = array[:, at : at + step].T
        bottom[at : at + step] = array[:, half + at : half + at + step].T


def norm_terms_body(full_width, rows, sums, pre, grad, table, flipped, bias, gain, top, bottom, joined_out, out, held, come):
    n_x, tall, _ = out.shape
    n_z = (tall - PACKED) // rows
    later, chunk, _ = held.shape
    loads = [
        pltpu.make_async_copy(bottom.at[pl.ds(i * chunk, chunk)], held.at[i], come.at[i])
        for i in range(later)
    ]
    for load in loads:
        load.start()
    gating, mixed_grad, back, (pre_content, pre_gating) = branches(
        pre[...], grad[...], flipped[...], gain[...]
    )
    content_slope = grad[...].astype(f32) * gelu_slope(pre_content)
    total = jnp.sum(sums[...], axis=0) * (1.0 / full_width)
    row_mean = total[0:1]
    row_var = total[1:2] - row_mean * row_mean
    inv_std = lax.rsqrt(row_var + norm_eps)
    first = total[2:3]
    second = inv_std * (total[3:4] - row_mean * first)
    columns = jnp.concatenate([row_mean, inv_std, first, second] * 2, axis=0).T
    row_mean, inv_std, first, second = [columns[:, i : i + 1] for i in range(4)]
    centred = (gating - row_mean) * inv_std
    normed = (centred * gain[...]).astype(bf16)
    shift = jnp.broadcast_to(bias[...], (8, BLOCK)).T[:, 0:1]
    width = normed.shape[1]
    mixing_grad = None
    for at in range(0, normed.shape[0], BLOCK):
        block = slice(at, at + BLOCK)
        mixed = nn(table[...], normed[block]) + shift
        joined_out[block, :width] = (mixed * content_slope[block]).astype(bf16)
        term = nt(mixed_grad[block], normed[block])
        mixing_grad = term if mixing_grad is None else mixing_grad + term
    gating_back = inv_std * (back - first - centred * second)
    joined_out[:, width:] = (gating_back * gelu_slope(pre_gating)).astype(bf16)
    mixing_term = packed(causal(mixing_grad)).astype(bf16)
    for x in range(n_x):
        out[x, n_z * rows :] = mixing_term
    slab = n_x * rows
    ready = top.shape[0] // slab
    for z in range(n_z):
        if z < ready:
            part = top[z * slab : (z + 1) * slab]
        else:
            at = (z - ready) * slab
            if at % chunk == 0:
                loads[at // chunk].wait()
            part = held[at // chunk, at % chunk : at % chunk + slab]
        term = nn(part, joined_out[...]).astype(bf16)
        for x in range(n_x):
            out[x, z * rows : (z + 1) * rows] = term[x * rows : (x + 1) * rows]


def norm_terms(full_width, small, top, bottom, n_x, n_z):
    width, tokens = 2 * top.shape[0], top.shape[1]
    both = 2 * small[2].shape[1]
    rows = width // (n_x * n_z)
    near, far = pl.BlockSpec(memory_space=pltpu.VMEM), pl.BlockSpec(memory_space=pl.ANY)
    return pl.pallas_call(
        functools.partial(norm_terms_body, full_width, rows),
        out_shape=(like((tokens, both), bf16), stored((n_x, n_z * rows + PACKED, both), bf16)),
        in_specs=[near] * (len(small) + 1) + [far],
        out_specs=(near, pl.BlockSpec()),
        scratch_shapes=[
            pltpu.VMEM((1, bottom.shape[0], tokens), bf16),
            pltpu.SemaphoreType.DMA((1,)),
        ],
        compiler_params=pltpu.CompilerParams(vmem_limit_bytes=20 * 1024 * 1024),
        name="norm_terms",
    )(
        *[pltpu.with_memory_space_constraint(a, pltpu.VMEM) for a in (*small, top)],
        pltpu.with_memory_space_constraint(bottom, pltpu.HBM),
    )


def pick_body(where, weight, mixing, mine_out, theirs_out, table_out, flipped_out):
    table = causal(mixing[0].astype(f32))
    table_out[...] = table.astype(bf16)
    flipped_out[...] = table.T.astype(bf16)
    n_x, _, rows, both = weight.shape
    half = n_x // 2
    for out, base, core in ((mine_out, 0, where[10]), (theirs_out, 5, 1 - where[10])):
        at = 0
        for step in (3, 1, 2):
            block = weight[:, pl.ds(where[base + step], 1)].reshape(n_x * rows, both)
            out[at : at + n_x * rows] = block
            at += n_x * rows
        for step in (4, 0):
            block = weight[pl.ds(core * half, half), pl.ds(where[base + step], 1)]
            out[at : at + half * rows] = block.reshape(half * rows, both)
            at += half * rows


def input_terms_body(joined, joined_far, mine, far, odd, two, four, own):
    def term(at, n):
        rows = slice(at, at + n)
        return nt(joined[...], mine[rows]) + nt(joined_far[...], far[rows])

    single, pair = own.shape[1], two.shape[1]
    odd[...] = term(0, 2 * pair).astype(bf16)
    four[...] = term(3 * pair, single).astype(bf16)
    two[...] = term(2 * pair, pair)
    own[...] = term(3 * pair + single, single)


def merge_body(where, two, odd, four, same_out, other_out, keep_out, send_out):
    half = four.shape[1]
    first = where[10] == 0
    both = two[...] + odd[:, : 2 * half].astype(f32)
    left, right = both[:, :half], both[:, half:]
    same_out[...] = (jnp.where(first, left, right) + four[...].astype(f32)).astype(bf16)
    other_out[...] = jnp.where(first, right, left).astype(bf16)
    left, right = odd[:, 2 * half : 3 * half], odd[:, 3 * half :]
    left, right = left.astype(f32), right.astype(f32)
    keep_out[...] = jnp.where(first, left, right).astype(bf16)
    send_out[...] = jnp.where(first, right, left).astype(bf16)


def total_body(own, same, other, keep, sent, out):
    total = own[...]
    for part in (same, other, keep, sent):
        total = total + part[...].astype(f32)
    out[...] = total.astype(bf16)


def regroup_body(arrived, out):
    n_z = out.shape[0]
    rows = out.shape[1] - PACKED
    total = arrived[0].astype(f32)
    for x in range(1, arrived.shape[0]):
        total = total + arrived[x].astype(f32)
    total = total.astype(bf16)
    for z in range(n_z):
        out[z, :rows] = total[z * rows : (z + 1) * rows]
        out[z, rows:] = total[n_z * rows :]


def finish_body(scale, arrived, content_out, gating_out, mixing_out):
    total = arrived[0].astype(f32)
    for z in range(1, arrived.shape[0]):
        total = total + arrived[z].astype(f32)
    total = total * scale
    rows, half = content_out.shape
    content_out[...] = total[:rows, :half]
    gating_out[...] = total[:rows, half:]
    top, bottom = unpacked(total[rows:])
    mixing_out[0, : BLOCK // 2] = top
    mixing_out[0, BLOCK // 2 :] = bottom


def step(
    hidden_in, content_weight, gating_weight, norm_gain, mixing_weight, mixing_bias, out_grad
):
    tok_rows, width = hidden_in.shape
    shard_rows, local_width = content_weight.shape
    both = 2 * local_width
    n_z, n_x = lax.axis_size("sp_0"), lax.axis_size("sp_1")
    n_sp, n_dp = n_z * n_x, lax.axis_size(DP)
    ring = lax.axis_size("dp_0")
    full_width = local_width * n_dp
    out_cols = width // n_dp
    grad_scale = 1.0 / math.sqrt(tok_rows * n_sp)
    here, core = lax.axis_index("dp_0"), lax.axis_index("dp_1")
    side = 1 - 2 * core
    ahead = [(here + side * k + ring) % ring for k in range(5)]
    behind = [(here - side * k + ring) % ring for k in range(5)]
    where = jnp.stack(ahead + behind + [core]).astype(jnp.int32)
    gain = norm_gain[None, :]

    half = (width // 2, tok_rows)
    top, bottom = call(flip_body, (like(half, bf16), stored(half, bf16)))(hidden_in)
    shards = call(join_body, stored((n_z, shard_rows, both), bf16), cold=(0, 1))(
        content_weight, gating_weight
    )
    along_z = exchange(shards, "sp_0")
    spread = call(spread_body, like((n_x, n_z, shard_rows, both), bf16))(along_z)
    weight = exchange(spread, "sp_1")
    single, pair = (tok_rows, out_cols), (tok_rows, 2 * out_cols)
    wide_pair, picked = (tok_rows, 4 * out_cols), (width // 2, both)
    square = like((BLOCK, BLOCK), bf16)
    mine, theirs, table, flipped = call(
        pick_body,
        (stored(picked, bf16), stored(picked, bf16), square, square),
        scalars=True,
        cold=(2,),
    )(where, weight, mixing_weight)
    far = swapped(theirs)

    wide = (tok_rows, both)
    pre, sums = call(
        project_body, (like(wide, bf16), stored((n_dp, 4, tok_rows), f32))
    )(hidden_in, weight, mixing_weight, gain, out_grad)
    sums = exchange(sums, DP)
    small = (sums, pre, out_grad, table, flipped, mixing_bias, gain)
    joined, terms = norm_terms(full_width, small, top, bottom, n_x, n_z)

    joined_far = swapped(joined)
    along_x = exchange(terms, "sp_1")

    odd, two, four, own = call(
        input_terms_body,
        (like(wide_pair, bf16), like(pair, f32), like(single, bf16), like(single, f32)),
        cold=(2,),
    )(joined, joined_far, mine, far)
    four = sent_apart(four, 2)
    odd = sent_apart(odd, 1)
    same, other, keep, send = call(merge_body, (like(single, bf16),) * 4, scalars=True)(
        where, two, odd, four
    )
    same = sent_apart(same, 2)
    other = sent_apart(other, 2, True)
    sent = swapped(send)

    regrouped = call(regroup_body, stored((n_z, shard_rows + PACKED, both), bf16))(along_x)
    arrived = exchange(regrouped, "sp_0")

    input_grad = call(total_body, outside(single, bf16))(own, same, other, keep, sent)

    content_grad, gating_grad, mixing_grad = call(
        functools.partial(finish_body, grad_scale),
        (
            outside((shard_rows, local_width), f32),
            outside((shard_rows, local_width), f32),
            outside(mixing_weight.shape, f32),
        ),
    )(arrived)
    return (input_grad, content_grad, gating_grad, mixing_grad)


def solution(mesh):
    split = Mesh(mesh.devices.reshape(8, 4, 8, 2), (*SP, *DP))
    in_specs = (
        P(SP, None),
        P(SP, DP),
        P(SP, DP),
        P(DP),
        P(DP, None, None),
        P(DP, None),
        P(SP, DP),
    )
    out_specs = (P(SP, DP), P(SP, DP), P(SP, DP), P(DP, None, None))
    return jax.shard_map(step, mesh=split, in_specs=in_specs, out_specs=out_specs, check_vma=False)
```

```python
import functools
import math

import jax
import jax.numpy as jnp
from jax import lax
from jax.experimental import pallas as pl
from jax.experimental.pallas import tpu as pltpu
from jax.sharding import Mesh
from jax.sharding import PartitionSpec as P


BLOCK = 128
SP = ("sp_0", "sp_1")
DP = ("dp_0", "dp_1")


norm_eps = 1e-05
f32, bf16 = jnp.float32, jnp.bfloat16


def exchange(array, axis):
    return lax.all_to_all(array, axis, split_axis=0, concat_axis=0, tiled=True)


def swapped(array):
    return lax.ppermute(array, "dp_1", [(0, 1), (1, 0)])


def sent_apart(array, step, cross=False):
    ring = lax.axis_size("dp_0")
    moves = []
    for y in range(ring):
        for core, there in ((0, (y + step) % ring), (1, (y - step) % ring)):
            moves.append((2 * y + core, 2 * there + (1 - core if cross else core)))
    return lax.ppermute(array, DP, moves)


def normal_below(values):
    return 0.5 * (1.0 + lax.erf(values * (1.0 / math.sqrt(2.0))))


def gelu_slope(values):
    density = jnp.exp(-0.5 * values * values) * (1.0 / math.sqrt(2.0 * math.pi))
    return normal_below(values) + values * density


def causal(weights):
    rows = lax.broadcasted_iota(jnp.int32, (BLOCK, BLOCK), 0)
    cols = lax.broadcasted_iota(jnp.int32, (BLOCK, BLOCK), 1)
    return jnp.where(cols <= rows, weights, jnp.zeros_like(weights))


PACKED = BLOCK // 4 + 8


def packed(grad):
    half = BLOCK // 2
    rows = lax.broadcasted_iota(jnp.int32, (half, BLOCK), 0)
    cols = lax.broadcasted_iota(jnp.int32, (half, BLOCK), 1)
    turned = pltpu.roll(grad.T, half, 1)[:half]
    body = grad[half:] + jnp.where(cols - half > rows, turned, 0.0)
    spine = jnp.sum(jnp.where(rows == cols, grad[:half], 0.0), axis=0, keepdims=True)
    spine = jnp.broadcast_to(spine, (8, BLOCK))
    body = jnp.concatenate([body[: half // 2], body[half // 2 :]], axis=1)
    return jnp.concatenate([body, jnp.concatenate([spine, spine], axis=1)], axis=0)


def unpacked(terms):
    half = BLOCK // 2
    rows = lax.broadcasted_iota(jnp.int32, (half, BLOCK), 0)
    cols = lax.broadcasted_iota(jnp.int32, (half, BLOCK), 1)
    body = terms[: half // 2]
    body = jnp.concatenate([body[:, :BLOCK], body[:, BLOCK:]], axis=0)
    spine = jnp.broadcast_to(terms[half // 2 : half // 2 + 1, :BLOCK], (half, BLOCK))
    above = jnp.where(cols - half > rows, body, 0.0)
    top = jnp.concatenate([above, jnp.zeros_like(above)], axis=0).T[half:]
    top = top + jnp.where(rows == cols, spine, 0.0)
    return top, jnp.where(cols - half <= rows, body, 0.0)


def nt(a, b, **kw):
    return lax.dot_general(a, b, (((1,), (1,)), ((), ())), preferred_element_type=f32, **kw)


def nn(a, b):
    return jnp.dot(a, b, preferred_element_type=f32)


def call(body, outs, scalars=False, cold=(), free=()):
    def run(*args):
        specs, operands = [], []
        for at, array in enumerate(args):
            if scalars and at == 0:
                specs.append(pl.BlockSpec(memory_space=pltpu.SMEM))
            elif at in free:
                specs.append(pl.BlockSpec())
            elif at in cold:
                specs.append(pl.BlockSpec())
                array = pltpu.with_memory_space_constraint(array, pltpu.HBM)
            else:
                specs.append(pl.BlockSpec(memory_space=pltpu.VMEM))
                array = pltpu.with_memory_space_constraint(array, pltpu.VMEM)
            operands.append(array)
        limit = pltpu.CompilerParams(vmem_limit_bytes=20 * 1024 * 1024)
        made = pl.pallas_call(body, out_shape=outs, in_specs=specs, compiler_params=limit)
        return made(*operands)

    return run


def like(shape, dtype):
    return pltpu.VMEM(shape, dtype)


def stored(shape, dtype):
    return pltpu.HBM(shape, dtype)


def outside(shape, dtype):
    return jax.ShapeDtypeStruct(shape, dtype)


def project_body(hidden, weight, mixing, gain, grad, pre_out, sums_out):
    n_x, n_z, rows, both = weight.shape
    slab = n_x * rows
    pre = None
    for z in range(n_z):
        term = nn(hidden[:, z * slab : (z + 1) * slab], weight[:, z].reshape(slab, both))
        pre = term if pre is None else pre + term
    pre = pre.astype(bf16)
    pre_out[...] = pre
    flipped = causal(mixing[0].astype(f32)).T.astype(bf16)
    gating, _, back, _ = branches(pre, grad[...], flipped, gain[...])
    lane = lax.broadcasted_iota(jnp.int32, gating.shape, 1)
    sums = jnp.zeros_like(gating)
    for at, values in enumerate((gating, gating * gating, back, back * gating)):
        sums = jnp.where(lane == at, jnp.sum(values, axis=1, keepdims=True), sums)
    sums = sums.T
    for peer in range(sums_out.shape[0]):
        sums_out[peer] = sums[:4]


def branches(pre, grad, flipped, gain):
    width = grad.shape[1]
    pre_content = pre[:, :width].astype(f32)
    pre_gating = pre[:, width:].astype(f32)
    gating = pre_gating * normal_below(pre_gating)
    content = pre_content * normal_below(pre_content)
    mixed_grad = (grad.astype(f32) * content).astype(bf16)
    pieces = []
    for at in range(0, mixed_grad.shape[0], BLOCK):
        pieces.append(nn(flipped, mixed_grad[at : at + BLOCK]) * gain)
    return gating, mixed_grad, jnp.concatenate(pieces, axis=0), (pre_content, pre_gating)


def join_body(content, gating, out, done):
    width = content.shape[1]
    moves = []
    for peer in range(out.shape[0]):
        for side, array in enumerate((content, gating)):
            slot = out.at[peer, :, pl.ds(side * width, width)]
            moves.append(pltpu.make_async_copy(array, slot, done.at[peer, side]))
    for move in moves:
        move.start()
    for move in moves:
        move.wait()


def join(content, gating, n_z):
    rows, width = content.shape
    far = pl.BlockSpec(memory_space=pl.ANY)
    return pl.pallas_call(
        join_body,
        out_shape=stored((n_z, rows, 2 * width), bf16),
        in_specs=[far, far],
        out_specs=far,
        scratch_shapes=[pltpu.SemaphoreType.DMA((n_z, 2))],
        compiler_params=pltpu.CompilerParams(vmem_limit_bytes=20 * 1024 * 1024),
        name="join",
    )(*[pltpu.with_memory_space_constraint(a, pltpu.HBM) for a in (content, gating)])


def spread_body(arrived, out):
    for peer in range(out.shape[0]):
        out[peer] = arrived[...]


def flip_body(array, top, bottom):
    step, half = 256, top.shape[0]
    for at in range(0, half, step):
        top[at : at + step] = array[:, at : at + step].T
        bottom[at : at + step] = array[:, half + at : half + at + step].T


def norm_terms_body(full_width, rows, sums, pre, grad, table, flipped, bias, gain, top, bottom, joined_out, out, held, come):
    n_x, tall, _ = out.shape
    n_z = (tall - PACKED) // rows
    later, chunk, _ = held.shape
    loads = [
        pltpu.make_async_copy(bottom.at[pl.ds(i * chunk, chunk)], held.at[i], come.at[i])
        for i in range(later)
    ]
    for load in loads:
        load.start()
    gating, mixed_grad, back, (pre_content, pre_gating) = branches(
        pre[...], grad[...], flipped[...], gain[...]
    )
    content_slope = grad[...].astype(f32) * gelu_slope(pre_content)
    total = jnp.sum(sums[...], axis=0) * (1.0 / full_width)
    row_mean = total[0:1]
    row_var = total[1:2] - row_mean * row_mean
    inv_std = lax.rsqrt(row_var + norm_eps)
    first = total[2:3]
    second = inv_std * (total[3:4] - row_mean * first)
    columns = jnp.concatenate([row_mean, inv_std, first, second] * 2, axis=0).T
    row_mean, inv_std, first, second = [columns[:, i : i + 1] for i in range(4)]
    centred = (gating - row_mean) * inv_std
    normed = (centred * gain[...]).astype(bf16)
    shift = jnp.broadcast_to(bias[...], (8, BLOCK)).T[:, 0:1]
    width = normed.shape[1]
    mixing_grad = None
    for at in range(0, normed.shape[0], BLOCK):
        block = slice(at, at + BLOCK)
        mixed = nn(table[...], normed[block]) + shift
        joined_out[block, :width] = (mixed * content_slope[block]).astype(bf16)
        term = nt(mixed_grad[block], normed[block])
        mixing_grad = term if mixing_grad is None else mixing_grad + term
    gating_back = inv_std * (back - first - centred * second)
    joined_out[:, width:] = (gating_back * gelu_slope(pre_gating)).astype(bf16)
    mixing_term = packed(causal(mixing_grad)).astype(bf16)
    for x in range(n_x):
        out[x, n_z * rows :] = mixing_term
    slab = n_x * rows
    ready = top.shape[0] // slab
    for z in range(n_z):
        if z < ready:
            part = top[z * slab : (z + 1) * slab]
        else:
            at = (z - ready) * slab
            if at % chunk == 0:
                loads[at // chunk].wait()
            part = held[at // chunk, at % chunk : at % chunk + slab]
        term = nn(part, joined_out[...]).astype(bf16)
        for x in range(n_x):
            out[x, z * rows : (z + 1) * rows] = term[x * rows : (x + 1) * rows]


def norm_terms(full_width, small, top, bottom, n_x, n_z):
    width, tokens = 2 * top.shape[0], top.shape[1]
    both = 2 * small[2].shape[1]
    rows = width // (n_x * n_z)
    near, far = pl.BlockSpec(memory_space=pltpu.VMEM), pl.BlockSpec(memory_space=pl.ANY)
    return pl.pallas_call(
        functools.partial(norm_terms_body, full_width, rows),
        out_shape=(like((tokens, both), bf16), stored((n_x, n_z * rows + PACKED, both), bf16)),
        in_specs=[near] * (len(small) + 1) + [far],
        out_specs=(near, pl.BlockSpec()),
        scratch_shapes=[
            pltpu.VMEM((1, bottom.shape[0], tokens), bf16),
            pltpu.SemaphoreType.DMA((1,)),
        ],
        compiler_params=pltpu.CompilerParams(vmem_limit_bytes=20 * 1024 * 1024),
        name="norm_terms",
    )(
        *[pltpu.with_memory_space_constraint(a, pltpu.VMEM) for a in (*small, top)],
        pltpu.with_memory_space_constraint(bottom, pltpu.HBM),
    )


def pick_body(where, weight, mixing, mine_out, theirs_out, table_out, flipped_out):
    table = causal(mixing[0].astype(f32))
    table_out[...] = table.astype(bf16)
    flipped_out[...] = table.T.astype(bf16)
    n_x, _, rows, both = weight.shape
    half = n_x // 2
    for out, base, core in ((mine_out, 0, where[10]), (theirs_out, 5, 1 - where[10])):
        at = 0
        for step in (3, 1, 2):
            block = weight[:, pl.ds(where[base + step], 1)].reshape(n_x * rows, both)
            out[at : at + n_x * rows] = block
            at += n_x * rows
        for step in (4, 0):
            block = weight[pl.ds(core * half, half), pl.ds(where[base + step], 1)]
            out[at : at + half * rows] = block.reshape(half * rows, both)
            at += half * rows


def input_terms_body(joined, joined_far, mine, far, odd, two, four, own):
    def term(at, n):
        rows = slice(at, at + n)
        return nt(joined[...], mine[rows]) + nt(joined_far[...], far[rows])

    single, pair = own.shape[1], two.shape[1]
    odd[...] = term(0, 2 * pair).astype(bf16)
    four[...] = term(3 * pair, single).astype(bf16)
    two[...] = term(2 * pair, pair)
    own[...] = term(3 * pair + single, single)


def merge_body(where, two, odd, four, same_out, other_out, keep_out, send_out):
    half = four.shape[1]
    first = where[10] == 0
    both = two[...] + odd[:, : 2 * half].astype(f32)
    left, right = both[:, :half], both[:, half:]
    same_out[...] = (jnp.where(first, left, right) + four[...].astype(f32)).astype(bf16)
    other_out[...] = jnp.where(first, right, left).astype(bf16)
    left, right = odd[:, 2 * half : 3 * half], odd[:, 3 * half :]
    left, right = left.astype(f32), right.astype(f32)
    keep_out[...] = jnp.where(first, left, right).astype(bf16)
    send_out[...] = jnp.where(first, right, left).astype(bf16)


def total_body(own, same, other, keep, sent, out):
    total = own[...]
    for part in (same, other, keep, sent):
        total = total + part[...].astype(f32)
    out[...] = total.astype(bf16)


def regroup_body(arrived, out, made, done):
    n_z, tall, _ = made.shape
    rows = tall - PACKED

    def summed(at, n):
        total = arrived[0, at : at + n].astype(f32)
        for x in range(1, arrived.shape[0]):
            total = total + arrived[x, at : at + n].astype(f32)
        return total.astype(bf16)

    stores = [pltpu.make_async_copy(made.at[z], out.at[z], done.at[z]) for z in range(n_z)]
    shared = summed(n_z * rows, PACKED)
    for z in range(n_z):
        made[z, :rows] = summed(z * rows, rows)
        made[z, rows:] = shared
        stores[z].start()
    for store in stores:
        store.wait()


def regroup(arrived, n_z, rows):
    shape = (n_z, rows + PACKED, arrived.shape[2])
    return pl.pallas_call(
        regroup_body,
        out_shape=stored(shape, bf16),
        in_specs=[pl.BlockSpec(memory_space=pltpu.VMEM)],
        out_specs=pl.BlockSpec(memory_space=pl.ANY),
        scratch_shapes=[pltpu.VMEM(shape, bf16), pltpu.SemaphoreType.DMA((n_z,))],
        compiler_params=pltpu.CompilerParams(vmem_limit_bytes=20 * 1024 * 1024),
        name="regroup",
    )(pltpu.with_memory_space_constraint(arrived, pltpu.VMEM))


def finish_body(scale, arrived, content_out, gating_out, mixing_out):
    total = arrived[0].astype(f32)
    for z in range(1, arrived.shape[0]):
        total = total + arrived[z].astype(f32)
    total = total * scale
    rows, half = content_out.shape
    content_out[...] = total[:rows, :half]
    gating_out[...] = total[:rows, half:]
    top, bottom = unpacked(total[rows:])
    mixing_out[0, : BLOCK // 2] = top
    mixing_out[0, BLOCK // 2 :] = bottom


def step(
    hidden_in, content_weight, gating_weight, norm_gain, mixing_weight, mixing_bias, out_grad
):
    tok_rows, width = hidden_in.shape
    shard_rows, local_width = content_weight.shape
    both = 2 * local_width
    n_z, n_x = lax.axis_size("sp_0"), lax.axis_size("sp_1")
    n_sp, n_dp = n_z * n_x, lax.axis_size(DP)
    ring = lax.axis_size("dp_0")
    full_width = local_width * n_dp
    out_cols = width // n_dp
    grad_scale = 1.0 / math.sqrt(tok_rows * n_sp)
    here, core = lax.axis_index("dp_0"), lax.axis_index("dp_1")
    side = 1 - 2 * core
    ahead = [(here + side * k + ring) % ring for k in range(5)]
    behind = [(here - side * k + ring) % ring for k in range(5)]
    where = jnp.stack(ahead + behind + [core]).astype(jnp.int32)
    gain = norm_gain[None, :]

    half = (width // 2, tok_rows)
    top, bottom = call(flip_body, (like(half, bf16), stored(half, bf16)))(hidden_in)
    shards = join(content_weight, gating_weight, n_z)
    along_z = exchange(shards, "sp_0")
    spread = call(spread_body, like((n_x, n_z, shard_rows, both), bf16))(along_z)
    weight = exchange(spread, "sp_1")
    single, pair = (tok_rows, out_cols), (tok_rows, 2 * out_cols)
    wide_pair, picked = (tok_rows, 4 * out_cols), (width // 2, both)
    square = like((BLOCK, BLOCK), bf16)
    mine, theirs, table, flipped = call(
        pick_body,
        (stored(picked, bf16), stored(picked, bf16), square, square),
        scalars=True,
        cold=(2,),
    )(where, weight, mixing_weight)
    far = swapped(theirs)

    wide = (tok_rows, both)
    pre, sums = call(
        project_body, (like(wide, bf16), stored((n_dp, 4, tok_rows), f32))
    )(hidden_in, weight, mixing_weight, gain, out_grad)
    sums = exchange(sums, DP)
    small = (sums, pre, out_grad, table, flipped, mixing_bias, gain)
    joined, terms = norm_terms(full_width, small, top, bottom, n_x, n_z)

    joined_far = swapped(joined)
    along_x = exchange(terms, "sp_1")

    odd, two, four, own = call(
        input_terms_body,
        (like(wide_pair, bf16), like(pair, f32), like(single, bf16), like(single, f32)),
        cold=(2,),
    )(joined, joined_far, mine, far)
    four = sent_apart(four, 2)
    odd = sent_apart(odd, 1)
    same, other, keep, send = call(merge_body, (like(single, bf16),) * 4, scalars=True)(
        where, two, odd, four
    )
    same = sent_apart(same, 2)
    other = sent_apart(other, 2, True)
    sent = swapped(send)

    regrouped = regroup(along_x, n_z, shard_rows)
    arrived = exchange(regrouped, "sp_0")

    input_grad = call(total_body, outside(single, bf16))(own, same, other, keep, sent)

    content_grad, gating_grad, mixing_grad = call(
        functools.partial(finish_body, grad_scale),
        (
            outside((shard_rows, local_width), f32),
            outside((shard_rows, local_width), f32),
            outside(mixing_weight.shape, f32),
        ),
    )(arrived)
    return (input_grad, content_grad, gating_grad, mixing_grad)


def solution(mesh):
    split = Mesh(mesh.devices.reshape(8, 4, 8, 2), (*SP, *DP))
    in_specs = (
        P(SP, None),
        P(SP, DP),
        P(SP, DP),
        P(DP),
        P(DP, None, None),
        P(DP, None),
        P(SP, DP),
    )
    out_specs = (P(SP, DP), P(SP, DP), P(SP, DP), P(DP, None, None))
    return jax.shard_map(step, mesh=split, in_specs=in_specs, out_specs=out_specs, check_vma=False)
```

```python
import functools
import math

import jax
import jax.numpy as jnp
from jax import lax
from jax.experimental import pallas as pl
from jax.experimental.pallas import tpu as pltpu
from jax.sharding import Mesh
from jax.sharding import PartitionSpec as P


BLOCK = 128
Z = ("z_far", "z_near")
SP = (*Z, "x")
DP = ("dp_0", "dp_1")


norm_eps = 1e-05
f32, bf16 = jnp.float32, jnp.bfloat16


def exchange(array, axis):
    return lax.all_to_all(array, axis, split_axis=0, concat_axis=0, tiled=True)


def swapped(array):
    return lax.ppermute(array, "dp_1", [(0, 1), (1, 0)])


def sent_apart(array, step, cross=False):
    ring = lax.axis_size("dp_0")
    moves = []
    for y in range(ring):
        for core, there in ((0, (y + step) % ring), (1, (y - step) % ring)):
            moves.append((2 * y + core, 2 * there + (1 - core if cross else core)))
    return lax.ppermute(array, DP, moves)


def normal_below(values):
    return 0.5 * (1.0 + lax.erf(values * (1.0 / math.sqrt(2.0))))


def gelu_slope(values):
    density = jnp.exp(-0.5 * values * values) * (1.0 / math.sqrt(2.0 * math.pi))
    return normal_below(values) + values * density


def causal(weights):
    rows = lax.broadcasted_iota(jnp.int32, (BLOCK, BLOCK), 0)
    cols = lax.broadcasted_iota(jnp.int32, (BLOCK, BLOCK), 1)
    return jnp.where(cols <= rows, weights, jnp.zeros_like(weights))


PACKED = BLOCK // 4 + 8


def packed(grad):
    half = BLOCK // 2
    rows = lax.broadcasted_iota(jnp.int32, (half, BLOCK), 0)
    cols = lax.broadcasted_iota(jnp.int32, (half, BLOCK), 1)
    turned = pltpu.roll(grad.T, half, 1)[:half]
    body = grad[half:] + jnp.where(cols - half > rows, turned, 0.0)
    spine = jnp.sum(jnp.where(rows == cols, grad[:half], 0.0), axis=0, keepdims=True)
    spine = jnp.broadcast_to(spine, (8, BLOCK))
    body = jnp.concatenate([body[: half // 2], body[half // 2 :]], axis=1)
    return jnp.concatenate([body, jnp.concatenate([spine, spine], axis=1)], axis=0)


def unpacked(terms):
    half = BLOCK // 2
    rows = lax.broadcasted_iota(jnp.int32, (half, BLOCK), 0)
    cols = lax.broadcasted_iota(jnp.int32, (half, BLOCK), 1)
    body = terms[: half // 2]
    body = jnp.concatenate([body[:, :BLOCK], body[:, BLOCK:]], axis=0)
    spine = jnp.broadcast_to(terms[half // 2 : half // 2 + 1, :BLOCK], (half, BLOCK))
    above = jnp.where(cols - half > rows, body, 0.0)
    top = jnp.concatenate([above, jnp.zeros_like(above)], axis=0).T[half:]
    top = top + jnp.where(rows == cols, spine, 0.0)
    return top, jnp.where(cols - half <= rows, body, 0.0)


def nt(a, b, **kw):
    return lax.dot_general(a, b, (((1,), (1,)), ((), ())), preferred_element_type=f32, **kw)


def nn(a, b):
    return jnp.dot(a, b, preferred_element_type=f32)


def call(body, outs, scalars=False, cold=(), free=()):
    def run(*args):
        specs, operands = [], []
        for at, array in enumerate(args):
            if scalars and at == 0:
                specs.append(pl.BlockSpec(memory_space=pltpu.SMEM))
            elif at in free:
                specs.append(pl.BlockSpec())
            elif at in cold:
                specs.append(pl.BlockSpec())
                array = pltpu.with_memory_space_constraint(array, pltpu.HBM)
            else:
                specs.append(pl.BlockSpec(memory_space=pltpu.VMEM))
                array = pltpu.with_memory_space_constraint(array, pltpu.VMEM)
            operands.append(array)
        limit = pltpu.CompilerParams(vmem_limit_bytes=20 * 1024 * 1024)
        made = pl.pallas_call(body, out_shape=outs, in_specs=specs, compiler_params=limit)
        return made(*operands)

    return run


def like(shape, dtype):
    return pltpu.VMEM(shape, dtype)


def stored(shape, dtype):
    return pltpu.HBM(shape, dtype)


def outside(shape, dtype):
    return jax.ShapeDtypeStruct(shape, dtype)


def project_body(hidden, weight, mixing, gain, grad, pre_out, sums_out):
    n_x, n_z, rows, both = weight.shape
    slab = n_x * rows
    pre = None
    for z in range(n_z):
        term = nn(hidden[:, z * slab : (z + 1) * slab], weight[:, z].reshape(slab, both))
        pre = term if pre is None else pre + term
    pre = pre.astype(bf16)
    pre_out[...] = pre
    flipped = causal(mixing[0].astype(f32)).T.astype(bf16)
    gating, _, back, _ = branches(pre, grad[...], flipped, gain[...])
    lane = lax.broadcasted_iota(jnp.int32, gating.shape, 1)
    sums = jnp.zeros_like(gating)
    for at, values in enumerate((gating, gating * gating, back, back * gating)):
        sums = jnp.where(lane == at, jnp.sum(values, axis=1, keepdims=True), sums)
    sums = sums.T
    for peer in range(sums_out.shape[0]):
        sums_out[peer] = sums[:4]


def branches(pre, grad, flipped, gain):
    width = grad.shape[1]
    pre_content = pre[:, :width].astype(f32)
    pre_gating = pre[:, width:].astype(f32)
    gating = pre_gating * normal_below(pre_gating)
    content = pre_content * normal_below(pre_content)
    mixed_grad = (grad.astype(f32) * content).astype(bf16)
    pieces = []
    for at in range(0, mixed_grad.shape[0], BLOCK):
        pieces.append(nn(flipped, mixed_grad[at : at + BLOCK]) * gain)
    return gating, mixed_grad, jnp.concatenate(pieces, axis=0), (pre_content, pre_gating)


def join_body(content, gating, out):
    both = jnp.concatenate([content[...], gating[...]], axis=1)
    for peer in range(out.shape[0]):
        out[peer] = both


def spread_body(arrived, out):
    for peer in range(out.shape[0]):
        out[peer] = arrived[...]


def flip_body(array, top, bottom):
    step, half = 256, top.shape[0]
    for at in range(0, half, step):
        top[at : at + step] = array[:, at : at + step].T
        bottom[at : at + step] = array[:, half + at : half + at + step].T


def norm_terms_body(full_width, rows, n_x, sums, pre, grad, table, flipped, bias, gain, top, bottom, joined_out, out, held, come):
    n_first, tall, _ = out.shape
    n_far, n_near = (tall - PACKED) // rows, n_first // n_x
    later, chunk, _ = held.shape
    loads = [
        pltpu.make_async_copy(bottom.at[pl.ds(i * chunk, chunk)], held.at[i], come.at[i])
        for i in range(later)
    ]
    for load in loads:
        load.start()
    gating, mixed_grad, back, (pre_content, pre_gating) = branches(
        pre[...], grad[...], flipped[...], gain[...]
    )
    content_slope = grad[...].astype(f32) * gelu_slope(pre_content)
    total = jnp.sum(sums[...], axis=0) * (1.0 / full_width)
    row_mean = total[0:1]
    row_var = total[1:2] - row_mean * row_mean
    inv_std = lax.rsqrt(row_var + norm_eps)
    first = total[2:3]
    second = inv_std * (total[3:4] - row_mean * first)
    columns = jnp.concatenate([row_mean, inv_std, first, second] * 2, axis=0).T
    row_mean, inv_std, first, second = [columns[:, i : i + 1] for i in range(4)]
    centred = (gating - row_mean) * inv_std
    normed = (centred * gain[...]).astype(bf16)
    shift = jnp.broadcast_to(bias[...], (8, BLOCK)).T[:, 0:1]
    width = normed.shape[1]
    mixing_grad = None
    for at in range(0, normed.shape[0], BLOCK):
        block = slice(at, at + BLOCK)
        mixed = nn(table[...], normed[block]) + shift
        joined_out[block, :width] = (mixed * content_slope[block]).astype(bf16)
        term = nt(mixed_grad[block], normed[block])
        mixing_grad = term if mixing_grad is None else mixing_grad + term
    gating_back = inv_std * (back - first - centred * second)
    joined_out[:, width:] = (gating_back * gelu_slope(pre_gating)).astype(bf16)
    mixing_term = packed(causal(mixing_grad)).astype(bf16)
    for peer in range(n_first):
        out[peer, n_far * rows :] = mixing_term
    slab = n_x * rows
    ready = top.shape[0] // slab
    for z in range(n_far * n_near):
        if z < ready:
            part = top[z * slab : (z + 1) * slab]
        else:
            at = (z - ready) * slab
            if at % chunk == 0:
                loads[at // chunk].wait()
            part = held[at // chunk, at % chunk : at % chunk + slab]
        term = nn(part, joined_out[...]).astype(bf16)
        at = z // n_near * rows
        for x in range(n_x):
            out[z % n_near * n_x + x, at : at + rows] = term[x * rows : (x + 1) * rows]


def norm_terms(full_width, small, top, bottom, n_x, n_near, n_far):
    width, tokens = 2 * top.shape[0], top.shape[1]
    both = 2 * small[2].shape[1]
    rows = width // (n_x * n_near * n_far)
    near, far = pl.BlockSpec(memory_space=pltpu.VMEM), pl.BlockSpec(memory_space=pl.ANY)
    return pl.pallas_call(
        functools.partial(norm_terms_body, full_width, rows, n_x),
        out_shape=(like((tokens, both), bf16), stored((n_near * n_x, n_far * rows + PACKED, both), bf16)),
        in_specs=[near] * (len(small) + 1) + [far],
        out_specs=(near, pl.BlockSpec()),
        scratch_shapes=[
            pltpu.VMEM((1, bottom.shape[0], tokens), bf16),
            pltpu.SemaphoreType.DMA((1,)),
        ],
        compiler_params=pltpu.CompilerParams(vmem_limit_bytes=20 * 1024 * 1024),
        name="norm_terms",
    )(
        *[pltpu.with_memory_space_constraint(a, pltpu.VMEM) for a in (*small, top)],
        pltpu.with_memory_space_constraint(bottom, pltpu.HBM),
    )


def pick_body(where, weight, mixing, mine_out, theirs_out, table_out, flipped_out):
    table = causal(mixing[0].astype(f32))
    table_out[...] = table.astype(bf16)
    flipped_out[...] = table.T.astype(bf16)
    n_x, _, rows, both = weight.shape
    half = n_x // 2
    for out, base, core in ((mine_out, 0, where[10]), (theirs_out, 5, 1 - where[10])):
        at = 0
        for step in (3, 1, 2):
            block = weight[:, pl.ds(where[base + step], 1)].reshape(n_x * rows, both)
            out[at : at + n_x * rows] = block
            at += n_x * rows
        for step in (4, 0):
            block = weight[pl.ds(core * half, half), pl.ds(where[base + step], 1)]
            out[at : at + half * rows] = block.reshape(half * rows, both)
            at += half * rows


def input_terms_body(joined, joined_far, mine, far, odd, two, four, own):
    def term(at, n):
        rows = slice(at, at + n)
        return nt(joined[...], mine[rows]) + nt(joined_far[...], far[rows])

    single, pair = own.shape[1], two.shape[1]
    odd[...] = term(0, 2 * pair).astype(bf16)
    four[...] = term(3 * pair, single).astype(bf16)
    two[...] = term(2 * pair, pair)
    own[...] = term(3 * pair + single, single)


def merge_body(where, two, odd, four, same_out, other_out, keep_out, send_out):
    half = four.shape[1]
    first = where[10] == 0
    both = two[...] + odd[:, : 2 * half].astype(f32)
    left, right = both[:, :half], both[:, half:]
    same_out[...] = (jnp.where(first, left, right) + four[...].astype(f32)).astype(bf16)
    other_out[...] = jnp.where(first, right, left).astype(bf16)
    left, right = odd[:, 2 * half : 3 * half], odd[:, 3 * half :]
    left, right = left.astype(f32), right.astype(f32)
    keep_out[...] = jnp.where(first, left, right).astype(bf16)
    send_out[...] = jnp.where(first, right, left).astype(bf16)


def total_body(own, same, other, keep, sent, out):
    total = own[...]
    for part in (same, other, keep, sent):
        total = total + part[...].astype(f32)
    out[...] = total.astype(bf16)


def regroup_body(arrived, out):
    n_z = out.shape[0]
    rows = out.shape[1] - PACKED
    total = arrived[0].astype(f32)
    for x in range(1, arrived.shape[0]):
        total = total + arrived[x].astype(f32)
    total = total.astype(bf16)
    for z in range(n_z):
        out[z, :rows] = total[z * rows : (z + 1) * rows]
        out[z, rows:] = total[n_z * rows :]


def finish_body(scale, arrived, content_out, gating_out, mixing_out):
    total = arrived[0].astype(f32)
    for z in range(1, arrived.shape[0]):
        total = total + arrived[z].astype(f32)
    total = total * scale
    rows, half = content_out.shape
    content_out[...] = total[:rows, :half]
    gating_out[...] = total[:rows, half:]
    top, bottom = unpacked(total[rows:])
    mixing_out[0, : BLOCK // 2] = top
    mixing_out[0, BLOCK // 2 :] = bottom


def step(
    hidden_in, content_weight, gating_weight, norm_gain, mixing_weight, mixing_bias, out_grad
):
    tok_rows, width = hidden_in.shape
    shard_rows, local_width = content_weight.shape
    both = 2 * local_width
    n_z, n_x = lax.axis_size(Z), lax.axis_size("x")
    n_sp, n_dp = n_z * n_x, lax.axis_size(DP)
    n_near, n_far = lax.axis_size("z_near"), lax.axis_size("z_far")
    ring = lax.axis_size("dp_0")
    full_width = local_width * n_dp
    out_cols = width // n_dp
    grad_scale = 1.0 / math.sqrt(tok_rows * n_sp)
    here, core = lax.axis_index("dp_0"), lax.axis_index("dp_1")
    side = 1 - 2 * core
    ahead = [(here + side * k + ring) % ring for k in range(5)]
    behind = [(here - side * k + ring) % ring for k in range(5)]
    where = jnp.stack(ahead + behind + [core]).astype(jnp.int32)
    gain = norm_gain[None, :]

    half = (width // 2, tok_rows)
    top, bottom = call(flip_body, (like(half, bf16), stored(half, bf16)))(hidden_in)
    shards = call(join_body, stored((n_z, shard_rows, both), bf16), cold=(0, 1))(
        content_weight, gating_weight
    )
    along_z = exchange(shards, Z)
    spread = call(spread_body, like((n_x, n_z, shard_rows, both), bf16))(along_z)
    weight = exchange(spread, "x")
    single, pair = (tok_rows, out_cols), (tok_rows, 2 * out_cols)
    wide_pair, picked = (tok_rows, 4 * out_cols), (width // 2, both)
    square = like((BLOCK, BLOCK), bf16)
    mine, theirs, table, flipped = call(
        pick_body,
        (stored(picked, bf16), stored(picked, bf16), square, square),
        scalars=True,
        cold=(2,),
    )(where, weight, mixing_weight)
    far = swapped(theirs)

    wide = (tok_rows, both)
    pre, sums = call(
        project_body, (like(wide, bf16), stored((n_dp, 4, tok_rows), f32))
    )(hidden_in, weight, mixing_weight, gain, out_grad)
    sums = exchange(sums, DP)
    small = (sums, pre, out_grad, table, flipped, mixing_bias, gain)
    joined, terms = norm_terms(full_width, small, top, bottom, n_x, n_near, n_far)

    joined_far = swapped(joined)
    along_x = exchange(terms, ("z_near", "x"))

    odd, two, four, own = call(
        input_terms_body,
        (like(wide_pair, bf16), like(pair, f32), like(single, bf16), like(single, f32)),
        cold=(2,),
    )(joined, joined_far, mine, far)
    four = sent_apart(four, 2)
    odd = sent_apart(odd, 1)
    same, other, keep, send = call(merge_body, (like(single, bf16),) * 4, scalars=True)(
        where, two, odd, four
    )
    same = sent_apart(same, 2)
    other = sent_apart(other, 2, True)
    sent = swapped(send)

    regrouped = call(regroup_body, stored((n_far, shard_rows + PACKED, both), bf16))(along_x)
    arrived = exchange(regrouped, "z_far")

    input_grad = call(total_body, outside(single, bf16))(own, same, other, keep, sent)

    content_grad, gating_grad, mixing_grad = call(
        functools.partial(finish_body, grad_scale),
        (
            outside((shard_rows, local_width), f32),
            outside((shard_rows, local_width), f32),
            outside(mixing_weight.shape, f32),
        ),
    )(arrived)
    return (input_grad, content_grad, gating_grad, mixing_grad)


def solution(mesh):
    split = Mesh(mesh.devices.reshape(4, 2, 4, 8, 2), (*SP, *DP))
    in_specs = (
        P(SP, None),
        P(SP, DP),
        P(SP, DP),
        P(DP),
        P(DP, None, None),
        P(DP, None),
        P(SP, DP),
    )
    out_specs = (P(SP, DP), P(SP, DP), P(SP, DP), P(DP, None, None))
    return jax.shard_map(step, mesh=split, in_specs=in_specs, out_specs=out_specs, check_vma=False)
```

```python
import functools
import math

import jax
import jax.numpy as jnp
from jax import lax
from jax.experimental import pallas as pl
from jax.experimental.pallas import tpu as pltpu
from jax.sharding import Mesh
from jax.sharding import PartitionSpec as P


BLOCK = 128
Z = ("z_far", "z_near")
SP = (*Z, "x")
DP = ("dp_0", "dp_1")


norm_eps = 1e-05
f32, bf16 = jnp.float32, jnp.bfloat16


def exchange(array, axis):
    return lax.all_to_all(array, axis, split_axis=0, concat_axis=0, tiled=True)


def swapped(array):
    return lax.ppermute(array, "dp_1", [(0, 1), (1, 0)])


def sent_apart(array, step, cross=False):
    ring = lax.axis_size("dp_0")
    moves = []
    for y in range(ring):
        for core, there in ((0, (y + step) % ring), (1, (y - step) % ring)):
            moves.append((2 * y + core, 2 * there + (1 - core if cross else core)))
    return lax.ppermute(array, DP, moves)


def normal_below(values):
    return 0.5 * (1.0 + lax.erf(values * (1.0 / math.sqrt(2.0))))


def gelu_slope(values):
    density = jnp.exp(-0.5 * values * values) * (1.0 / math.sqrt(2.0 * math.pi))
    return normal_below(values) + values * density


def causal(weights):
    rows = lax.broadcasted_iota(jnp.int32, (BLOCK, BLOCK), 0)
    cols = lax.broadcasted_iota(jnp.int32, (BLOCK, BLOCK), 1)
    return jnp.where(cols <= rows, weights, jnp.zeros_like(weights))


PACKED = BLOCK // 4 + 8


def packed(grad):
    half = BLOCK // 2
    rows = lax.broadcasted_iota(jnp.int32, (half, BLOCK), 0)
    cols = lax.broadcasted_iota(jnp.int32, (half, BLOCK), 1)
    turned = pltpu.roll(grad.T, half, 1)[:half]
    body = grad[half:] + jnp.where(cols - half > rows, turned, 0.0)
    spine = jnp.sum(jnp.where(rows == cols, grad[:half], 0.0), axis=0, keepdims=True)
    spine = jnp.broadcast_to(spine, (8, BLOCK))
    body = jnp.concatenate([body[: half // 2], body[half // 2 :]], axis=1)
    return jnp.concatenate([body, jnp.concatenate([spine, spine], axis=1)], axis=0)


def unpacked(terms):
    half = BLOCK // 2
    rows = lax.broadcasted_iota(jnp.int32, (half, BLOCK), 0)
    cols = lax.broadcasted_iota(jnp.int32, (half, BLOCK), 1)
    body = terms[: half // 2]
    body = jnp.concatenate([body[:, :BLOCK], body[:, BLOCK:]], axis=0)
    spine = jnp.broadcast_to(terms[half // 2 : half // 2 + 1, :BLOCK], (half, BLOCK))
    above = jnp.where(cols - half > rows, body, 0.0)
    top = jnp.concatenate([above, jnp.zeros_like(above)], axis=0).T[half:]
    top = top + jnp.where(rows == cols, spine, 0.0)
    return top, jnp.where(cols - half <= rows, body, 0.0)


def nt(a, b, **kw):
    return lax.dot_general(a, b, (((1,), (1,)), ((), ())), preferred_element_type=f32, **kw)


def nn(a, b):
    return jnp.dot(a, b, preferred_element_type=f32)


def call(body, outs, scalars=False, cold=(), free=()):
    def run(*args):
        specs, operands = [], []
        for at, array in enumerate(args):
            if scalars and at == 0:
                specs.append(pl.BlockSpec(memory_space=pltpu.SMEM))
            elif at in free:
                specs.append(pl.BlockSpec())
            elif at in cold:
                specs.append(pl.BlockSpec())
                array = pltpu.with_memory_space_constraint(array, pltpu.HBM)
            else:
                specs.append(pl.BlockSpec(memory_space=pltpu.VMEM))
                array = pltpu.with_memory_space_constraint(array, pltpu.VMEM)
            operands.append(array)
        limit = pltpu.CompilerParams(vmem_limit_bytes=20 * 1024 * 1024)
        made = pl.pallas_call(body, out_shape=outs, in_specs=specs, compiler_params=limit)
        return made(*operands)

    return run


def like(shape, dtype):
    return pltpu.VMEM(shape, dtype)


def stored(shape, dtype):
    return pltpu.HBM(shape, dtype)


def outside(shape, dtype):
    return jax.ShapeDtypeStruct(shape, dtype)


def project_body(n_x, hidden, weight, mixing, gain, grad, pre_out, sums_out):
    n_first, n_far, rows, both = weight.shape
    slab = n_x * rows
    n_near = n_first // n_x
    pre = None
    for z in range(n_far * n_near):
        near = z % n_near * n_x
        block = weight[near : near + n_x, z // n_near].reshape(slab, both)
        term = nn(hidden[:, z * slab : (z + 1) * slab], block)
        pre = term if pre is None else pre + term
    pre = pre.astype(bf16)
    pre_out[...] = pre
    flipped = causal(mixing[0].astype(f32)).T.astype(bf16)
    gating, _, back, _ = branches(pre, grad[...], flipped, gain[...])
    lane = lax.broadcasted_iota(jnp.int32, gating.shape, 1)
    sums = jnp.zeros_like(gating)
    for at, values in enumerate((gating, gating * gating, back, back * gating)):
        sums = jnp.where(lane == at, jnp.sum(values, axis=1, keepdims=True), sums)
    sums = sums.T
    for peer in range(sums_out.shape[0]):
        sums_out[peer] = sums[:4]


def branches(pre, grad, flipped, gain):
    width = grad.shape[1]
    pre_content = pre[:, :width].astype(f32)
    pre_gating = pre[:, width:].astype(f32)
    gating = pre_gating * normal_below(pre_gating)
    content = pre_content * normal_below(pre_content)
    mixed_grad = (grad.astype(f32) * content).astype(bf16)
    pieces = []
    for at in range(0, mixed_grad.shape[0], BLOCK):
        pieces.append(nn(flipped, mixed_grad[at : at + BLOCK]) * gain)
    return gating, mixed_grad, jnp.concatenate(pieces, axis=0), (pre_content, pre_gating)


def join_body(content, gating, out):
    both = jnp.concatenate([content[...], gating[...]], axis=1)
    for peer in range(out.shape[0]):
        out[peer] = both


def spread_body(arrived, out):
    for peer in range(out.shape[0]):
        out[peer] = arrived[...]


def flip_body(array, top, bottom):
    step, half = 256, top.shape[0]
    for at in range(0, half, step):
        top[at : at + step] = array[:, at : at + step].T
        bottom[at : at + step] = array[:, half + at : half + at + step].T


def norm_terms_body(full_width, rows, n_x, sums, pre, grad, table, flipped, bias, gain, top, bottom, joined_out, out, held, come):
    n_first, tall, _ = out.shape
    n_far, n_near = (tall - PACKED) // rows, n_first // n_x
    later, chunk, _ = held.shape
    loads = [
        pltpu.make_async_copy(bottom.at[pl.ds(i * chunk, chunk)], held.at[i], come.at[i])
        for i in range(later)
    ]
    for load in loads:
        load.start()
    gating, mixed_grad, back, (pre_content, pre_gating) = branches(
        pre[...], grad[...], flipped[...], gain[...]
    )
    content_slope = grad[...].astype(f32) * gelu_slope(pre_content)
    total = jnp.sum(sums[...], axis=0) * (1.0 / full_width)
    row_mean = total[0:1]
    row_var = total[1:2] - row_mean * row_mean
    inv_std = lax.rsqrt(row_var + norm_eps)
    first = total[2:3]
    second = inv_std * (total[3:4] - row_mean * first)
    columns = jnp.concatenate([row_mean, inv_std, first, second] * 2, axis=0).T
    row_mean, inv_std, first, second = [columns[:, i : i + 1] for i in range(4)]
    centred = (gating - row_mean) * inv_std
    normed = (centred * gain[...]).astype(bf16)
    shift = jnp.broadcast_to(bias[...], (8, BLOCK)).T[:, 0:1]
    width = normed.shape[1]
    mixing_grad = None
    for at in range(0, normed.shape[0], BLOCK):
        block = slice(at, at + BLOCK)
        mixed = nn(table[...], normed[block]) + shift
        joined_out[block, :width] = (mixed * content_slope[block]).astype(bf16)
        term = nt(mixed_grad[block], normed[block])
        mixing_grad = term if mixing_grad is None else mixing_grad + term
    gating_back = inv_std * (back - first - centred * second)
    joined_out[:, width:] = (gating_back * gelu_slope(pre_gating)).astype(bf16)
    mixing_term = packed(causal(mixing_grad)).astype(bf16)
    for peer in range(n_first):
        out[peer, n_far * rows :] = mixing_term
    slab = n_x * rows
    ready = top.shape[0] // slab
    for z in range(n_far * n_near):
        if z < ready:
            part = top[z * slab : (z + 1) * slab]
        else:
            at = (z - ready) * slab
            if at % chunk == 0:
                loads[at // chunk].wait()
            part = held[at // chunk, at % chunk : at % chunk + slab]
        term = nn(part, joined_out[...]).astype(bf16)
        at = z // n_near * rows
        for x in range(n_x):
            out[z % n_near * n_x + x, at : at + rows] = term[x * rows : (x + 1) * rows]


def norm_terms(full_width, small, top, bottom, n_x, n_near, n_far):
    width, tokens = 2 * top.shape[0], top.shape[1]
    both = 2 * small[2].shape[1]
    rows = width // (n_x * n_near * n_far)
    near, far = pl.BlockSpec(memory_space=pltpu.VMEM), pl.BlockSpec(memory_space=pl.ANY)
    return pl.pallas_call(
        functools.partial(norm_terms_body, full_width, rows, n_x),
        out_shape=(like((tokens, both), bf16), stored((n_near * n_x, n_far * rows + PACKED, both), bf16)),
        in_specs=[near] * (len(small) + 1) + [far],
        out_specs=(near, pl.BlockSpec()),
        scratch_shapes=[
            pltpu.VMEM((1, bottom.shape[0], tokens), bf16),
            pltpu.SemaphoreType.DMA((1,)),
        ],
        compiler_params=pltpu.CompilerParams(vmem_limit_bytes=20 * 1024 * 1024),
        name="norm_terms",
    )(
        *[pltpu.with_memory_space_constraint(a, pltpu.VMEM) for a in (*small, top)],
        pltpu.with_memory_space_constraint(bottom, pltpu.HBM),
    )


def pick_body(n_x, where, weight, mixing, mine_out, theirs_out, table_out, flipped_out):
    table = causal(mixing[0].astype(f32))
    table_out[...] = table.astype(bf16)
    flipped_out[...] = table.T.astype(bf16)
    n_first, _, rows, both = weight.shape
    n_near = n_first // n_x
    half = n_x // 2
    for out, base, core in ((mine_out, 0, where[10]), (theirs_out, 5, 1 - where[10])):
        at = 0
        for step in (3, 1, 2):
            z = where[base + step]
            block = weight[pl.ds(z % n_near * n_x, n_x), pl.ds(z // n_near, 1)]
            block = block.reshape(n_x * rows, both)
            out[at : at + n_x * rows] = block
            at += n_x * rows
        for step in (4, 0):
            z = where[base + step]
            block = weight[pl.ds(z % n_near * n_x + core * half, half), pl.ds(z // n_near, 1)]
            out[at : at + half * rows] = block.reshape(half * rows, both)
            at += half * rows


def input_terms_body(joined, joined_far, mine, far, odd, two, four, own):
    def term(at, n):
        rows = slice(at, at + n)
        return nt(joined[...], mine[rows]) + nt(joined_far[...], far[rows])

    single, pair = own.shape[1], two.shape[1]
    odd[...] = term(0, 2 * pair).astype(bf16)
    four[...] = term(3 * pair, single).astype(bf16)
    two[...] = term(2 * pair, pair)
    own[...] = term(3 * pair + single, single)


def merge_body(where, two, odd, four, same_out, other_out, keep_out, send_out):
    half = four.shape[1]
    first = where[10] == 0
    both = two[...] + odd[:, : 2 * half].astype(f32)
    left, right = both[:, :half], both[:, half:]
    same_out[...] = (jnp.where(first, left, right) + four[...].astype(f32)).astype(bf16)
    other_out[...] = jnp.where(first, right, left).astype(bf16)
    left, right = odd[:, 2 * half : 3 * half], odd[:, 3 * half :]
    left, right = left.astype(f32), right.astype(f32)
    keep_out[...] = jnp.where(first, left, right).astype(bf16)
    send_out[...] = jnp.where(first, right, left).astype(bf16)


def total_body(own, same, other, keep, sent, out):
    total = own[...]
    for part in (same, other, keep, sent):
        total = total + part[...].astype(f32)
    out[...] = total.astype(bf16)


def regroup_body(arrived, out):
    n_z = out.shape[0]
    rows = out.shape[1] - PACKED
    total = arrived[0].astype(f32)
    for x in range(1, arrived.shape[0]):
        total = total + arrived[x].astype(f32)
    total = total.astype(bf16)
    for z in range(n_z):
        out[z, :rows] = total[z * rows : (z + 1) * rows]
        out[z, rows:] = total[n_z * rows :]


def finish_body(scale, arrived, content_out, gating_out, mixing_out):
    total = arrived[0].astype(f32)
    for z in range(1, arrived.shape[0]):
        total = total + arrived[z].astype(f32)
    total = total * scale
    rows, half = content_out.shape
    content_out[...] = total[:rows, :half]
    gating_out[...] = total[:rows, half:]
    top, bottom = unpacked(total[rows:])
    mixing_out[0, : BLOCK // 2] = top
    mixing_out[0, BLOCK // 2 :] = bottom


def step(
    hidden_in, content_weight, gating_weight, norm_gain, mixing_weight, mixing_bias, out_grad
):
    tok_rows, width = hidden_in.shape
    shard_rows, local_width = content_weight.shape
    both = 2 * local_width
    n_z, n_x = lax.axis_size(Z), lax.axis_size("x")
    n_sp, n_dp = n_z * n_x, lax.axis_size(DP)
    n_near, n_far = lax.axis_size("z_near"), lax.axis_size("z_far")
    ring = lax.axis_size("dp_0")
    full_width = local_width * n_dp
    out_cols = width // n_dp
    grad_scale = 1.0 / math.sqrt(tok_rows * n_sp)
    here, core = lax.axis_index("dp_0"), lax.axis_index("dp_1")
    side = 1 - 2 * core
    ahead = [(here + side * k + ring) % ring for k in range(5)]
    behind = [(here - side * k + ring) % ring for k in range(5)]
    where = jnp.stack(ahead + behind + [core]).astype(jnp.int32)
    gain = norm_gain[None, :]

    half = (width // 2, tok_rows)
    top, bottom = call(flip_body, (like(half, bf16), stored(half, bf16)))(hidden_in)
    shards = call(join_body, stored((n_far, shard_rows, both), bf16), cold=(0, 1))(
        content_weight, gating_weight
    )
    along_z = exchange(shards, "z_far")
    spread = call(spread_body, like((n_near * n_x, n_far, shard_rows, both), bf16))(along_z)
    weight = exchange(spread, ("z_near", "x"))
    single, pair = (tok_rows, out_cols), (tok_rows, 2 * out_cols)
    wide_pair, picked = (tok_rows, 4 * out_cols), (width // 2, both)
    square = like((BLOCK, BLOCK), bf16)
    mine, theirs, table, flipped = call(
        functools.partial(pick_body, n_x),
        (stored(picked, bf16), stored(picked, bf16), square, square),
        scalars=True,
        cold=(2,),
    )(where, weight, mixing_weight)
    far = swapped(theirs)

    wide = (tok_rows, both)
    pre, sums = call(
        functools.partial(project_body, n_x), (like(wide, bf16), stored((n_dp, 4, tok_rows), f32))
    )(hidden_in, weight, mixing_weight, gain, out_grad)
    sums = exchange(sums, DP)
    small = (sums, pre, out_grad, table, flipped, mixing_bias, gain)
    joined, terms = norm_terms(full_width, small, top, bottom, n_x, n_near, n_far)

    joined_far = swapped(joined)
    along_x = exchange(terms, ("z_near", "x"))

    odd, two, four, own = call(
        input_terms_body,
        (like(wide_pair, bf16), like(pair, f32), like(single, bf16), like(single, f32)),
        cold=(2,),
    )(joined, joined_far, mine, far)
    four = sent_apart(four, 2)
    odd = sent_apart(odd, 1)
    same, other, keep, send = call(merge_body, (like(single, bf16),) * 4, scalars=True)(
        where, two, odd, four
    )
    same = sent_apart(same, 2)
    other = sent_apart(other, 2, True)
    sent = swapped(send)

    regrouped = call(regroup_body, stored((n_far, shard_rows + PACKED, both), bf16))(along_x)
    arrived = exchange(regrouped, "z_far")

    input_grad = call(total_body, outside(single, bf16))(own, same, other, keep, sent)

    content_grad, gating_grad, mixing_grad = call(
        functools.partial(finish_body, grad_scale),
        (
            outside((shard_rows, local_width), f32),
            outside((shard_rows, local_width), f32),
            outside(mixing_weight.shape, f32),
        ),
    )(arrived)
    return (input_grad, content_grad, gating_grad, mixing_grad)


def solution(mesh):
    split = Mesh(mesh.devices.reshape(4, 2, 4, 8, 2), (*SP, *DP))
    in_specs = (
        P(SP, None),
        P(SP, DP),
        P(SP, DP),
        P(DP),
        P(DP, None, None),
        P(DP, None),
        P(SP, DP),
    )
    out_specs = (P(SP, DP), P(SP, DP), P(SP, DP), P(DP, None, None))
    return jax.shard_map(step, mesh=split, in_specs=in_specs, out_specs=out_specs, check_vma=False)
```
